256 devices in a mesh: ep: 64 (over z, x, core), tp: 4 (over y).
Axes of the slice: x: 4, y: 4, z: 8, core: 2. Of those that a mesh axis runs over, the one named last changes fastest.
Arguments:
- layer_in: bfloat16 [1024, 2048], P('ep'), may hold values from -6 to 6
- state_in: float32 [1024, 32, 4096], P('ep', 'tp'), may hold values from -6 to 6
- mix_gain: float32 [2048], replicated, may hold values from 0.1 to 1.9
- rec_weight: bfloat16 [2048, 2048], P('ep', 'tp'), may hold values from -0.125 to 0.125
- key_weight: bfloat16 [2048, 2048], P('ep', 'tp'), may hold values from -0.125 to 0.125
- val_weight: bfloat16 [2048, 2048], P('ep', 'tp'), may hold values from -0.125 to 0.125
- decay_down: bfloat16 [2048, 64], replicated, may hold values from -0.125 to 0.125
- decay_up: bfloat16 [64, 2048], P(None, 'tp'), may hold values from -0.75 to 0.75
- decay_base: float32 [2048], P('tp'), may hold values from -6 to 6
- rate_down: bfloat16 [2048, 64], replicated, may hold values from -0.125 to 0.125
- rate_up: bfloat16 [64, 2048], P(None, 'tp'), may hold values from -0.75 to 0.75
- rate_base: float32 [2048], P('tp'), may hold values from -6 to 6
- key_scale: float32 [2048], P('tp'), may hold values from 0.25 to 4
- group_gain: float32 [2048], P('tp'), may hold values from 0.1 to 1.9
- out_weight: bfloat16 [2048, 2048], P('tp', 'ep'), may hold values from -0.125 to 0.125
- post_gain: float32 [2048], replicated, may hold values from 0.1 to 1.9
- ffn_gain: float32 [2048], replicated, may hold values from 0.1 to 1.9
- routes: int32 [1024, 4], P('ep'), may hold values from 0 to 63, all different within a row; in each aligned block of 16 rows (0 to 15, 16 to 31, ...) at most 2 rows name the same one
- route_gates: float32 [1024, 4], P('ep'), may hold values from 0.05 to 1
- expert_gate: bfloat16 [64, 2048, 2048], P('ep', None, 'tp'), may hold values from -0.375 to 0.375
- expert_up: bfloat16 [64, 2048, 2048], P('ep', None, 'tp'), may hold values from -0.375 to 0.375
- expert_down: bfloat16 [64, 2048, 2048], P('ep', 'tp'), may hold values from -0.125 to 0.125
- out_gain: float32 [2048], replicated, may hold values from 0.1 to 1.9
Outputs:
- layer_out: bfloat16 [1024, 2048], P('ep')
- new_state: float32 [1024, 32, 4096], P('ep', 'tp')
The draws below stay inside these ranges and needn't reach their ends.
Inputs may be any that keep to these rules, and one draw needn't show every extreme that they name: `routes`: each row names 4 different experts. Within the rows of one device (aligned blocks of 16 rows) no expert is named by more than 2 rows, and in every draw some block names some expert exactly 2 times.
All inputs are finite; a program needn't handle non-finite values.
Results may differ from the reference program's by a relative error of at most 0.017.
Values may be sent and summed in bfloat16 or wider, within the bound.
No kernel may reach another device: no remote copies, remote signals or barrier semaphores. Data moves between devices by JAX's collectives and lax.ppermute only.
A program may use at most 128 MiB of HBM per device.

```python
import math
import jax
import jax.numpy as jnp
import numpy as np
from jax import lax

D = 2048
HEADS = 32
HEAD_DIM = 64
LOW = 64
FF = 2048
TOPK = 4
SEQ_DEV = 16
SEQS = 1024
EXPERTS = 64
CAP = 2
N_EP = 64
N_TP = 4


def shard_levels(stream_key, shape, pieces, smallest, largest):
    def one(position, blocks):
        steps = jax.random.uniform(jax.random.fold_in(jax.random.fold_in(stream_key, 6), position), (blocks,), jnp.float32, smallest / len(pieces), largest / len(pieces))
        return jnp.repeat(jnp.exp(steps), shape[position] // blocks).reshape((-1,) + (1,) * (len(shape) - position - 1))

    factor_of = one(*pieces[0])
    for cut in pieces[1:]:
        factor_of = factor_of * one(*cut)
    return factor_of


def routed_block(own_key, own, number, rows, amount, top, limit, slope):
    ranking = jax.random.permutation(own_key, amount)
    packed, common = shares(amount, rows * top, limit, slope, True), shares(amount, rows * top, limit, slope, False)
    places = jnp.arange(amount)

    def named(sizes, turn):
        used = int((sizes > 0).sum())
        fixed = max(1, used // 4)
        moved = fixed + (places - fixed + turn * (used - fixed)) % max(1, amount - fixed)
        return jnp.zeros((amount,), jnp.int32).at[ranking[jnp.where(places < fixed, places, moved)]].set(jnp.asarray(sizes, jnp.int32))

    sizes = jnp.where(number % 4 == 0, named(packed, number // 4), named(common, number - number // 4 - 1))
    mixed = jax.random.permutation(jax.random.fold_in(own, 3), amount)
    donor, taker = mixed[0:amount // 2 * 2:2], mixed[1:amount // 2 * 2:2]
    margin = jnp.minimum(sizes[donor] - 1, limit - sizes[taker]) // 2
    margin = jnp.where((donor == ranking[0]) | (taker == ranking[0]) | (sizes[taker] == 0), 0, jnp.maximum(margin, 0))
    moved = jax.random.randint(jax.random.fold_in(own, 4), (amount // 2,), 0, 1 << 20) % (margin + 1)
    sizes = sizes.at[donor].add(-moved).at[taker].add(moved)
    items = jnp.searchsorted(jnp.cumsum(sizes), jnp.arange(rows * top), side="right").astype(jnp.int32)
    grid = items.reshape(top, rows).T
    grid = grid[jax.random.permutation(jax.random.fold_in(own, 1), rows)]
    turn = jax.random.randint(jax.random.fold_in(own, 2), (rows, 1), 0, top)
    return jnp.take_along_axis(grid, (jnp.arange(top)[None, :] + turn) % top, axis=1)


def shares(number_of, total, most, slope, full):
    loads = [(1 << 20) // math.isqrt(grade ** slope) + 1 for grade in range(1, number_of + 1)]
    largest = most if full else min(most, max(-(-total // number_of), total * loads[0] // sum(loads)))
    least = 1 if total - largest >= number_of - 1 else 0
    counts, rest = [largest] + [least] * (number_of - 1), total - largest - least * (number_of - 1)
    while rest > 0:
        candidates = [i for i in range(1, number_of) if counts[i] < largest] or [i for i in range(1, number_of) if counts[i] < most]
        mass, budget = sum([loads[i] for i in candidates]), rest
        for i in candidates:
            extra = min(most - counts[i], max(1, budget * loads[i] // mass), rest)
            counts[i] = counts[i] + extra
            rest = rest - extra
    return np.array(counts)


def bell_draw(stream_key, extent, spread, limit, shards=(), kind=jnp.bfloat16):
    entries = jax.random.normal(stream_key, extent, jnp.float32) * spread
    if len(shards) > 0:
        entries = shard_levels(stream_key, extent, shards, -0.22, 0.18) * entries
    return jnp.clip(entries, min=-limit, max=limit).astype(kind)


def setup_inputs(seed: int = 0) -> dict:
    seeds = jax.random.split(jax.random.key(seed), 24)
    layer_in = bell_draw(seeds[0], (SEQS, D), 1.0, 6.0, ((0, 64),))
    state_in = bell_draw(seeds[1], (SEQS, HEADS, HEAD_DIM * HEAD_DIM), 1.0, 6.0, ((0, 64), (1, 4)), jnp.float32)
    mix_gain = jnp.clip(1.0 + 0.18 * jax.random.normal(seeds[2], (D,), jnp.float32), 0.1, 1.9)
    rec_weight = bell_draw(seeds[3], (D, D), D ** -0.5, 0.125, ((0, 64), (1, 4)))
    key_weight = bell_draw(seeds[4], (D, D), D ** -0.5, 0.125, ((0, 64), (1, 4)))
    val_weight = bell_draw(seeds[5], (D, D), D ** -0.5, 0.125, ((0, 64), (1, 4)))
    decay_down = bell_draw(seeds[6], (D, LOW), D ** -0.5, 0.125)
    decay_up = bell_draw(seeds[7], (LOW, D), LOW ** -0.5, 0.75, ((1, 4),))
    decay_base = bell_draw(seeds[8], (D,), 1.5, 6.0, ((0, 4),), jnp.float32)
    rate_down = bell_draw(seeds[9], (D, LOW), D ** -0.5, 0.125)
    rate_up = bell_draw(seeds[10], (LOW, D), LOW ** -0.5, 0.75, ((1, 4),))
    rate_base = bell_draw(seeds[11], (D,), 1.0, 6.0, ((0, 4),), jnp.float32)
    key_scale = jnp.clip(jnp.exp(math.log(4.0) - 2.7725887 * jax.random.uniform(seeds[12], (D,), jnp.float32) ** shard_levels(seeds[12], (D,), ((0, 4),), -0.2, 0.2)), 0.25, 4.0)
    group_gain = jnp.clip(1.0 + 0.18 * jax.random.normal(seeds[13], (D,), jnp.float32), 0.1, 1.9)
    out_weight = bell_draw(seeds[14], (D, D), D ** -0.5, 0.125, ((0, 4), (1, 64)))
    post_gain = jnp.clip(1.0 + 0.18 * jax.random.normal(seeds[15], (D,), jnp.float32), 0.1, 1.9)
    ffn_gain = jnp.clip(1.0 + 0.18 * jax.random.normal(seeds[16], (D,), jnp.float32), 0.1, 1.9)
    routes_keys = jax.random.split(jax.random.fold_in(seeds[17], 1), SEQS // SEQ_DEV)
    routes_turns = jax.random.permutation(jax.random.fold_in(seeds[17], 3), SEQS // SEQ_DEV)
    routes = jax.vmap(lambda own, number: routed_block(jax.random.fold_in(seeds[17], 2), own, number, SEQ_DEV, EXPERTS, TOPK, CAP, 2))(routes_keys, routes_turns).reshape((SEQS, TOPK))
    route_gates = jnp.clip(jnp.exp(math.log(1.0) - 2.9957323 * jax.random.uniform(seeds[18], (SEQS, TOPK), jnp.float32) ** shard_levels(seeds[18], (SEQS, TOPK), ((0, 64),), -0.2, 0.2)), 0.05, 1.0)
    expert_gate = bell_draw(seeds[19], (EXPERTS, D, FF), (D // 9) ** -0.5, 0.375, ((0, 64), (2, 4)))
    expert_up = bell_draw(seeds[20], (EXPERTS, D, FF), (D // 9) ** -0.5, 0.375, ((0, 64), (2, 4)))
    expert_down = bell_draw(seeds[21], (EXPERTS, FF, D), FF ** -0.5, 0.125, ((0, 64), (1, 4)))
    out_gain = jnp.clip(1.0 + 0.18 * jax.random.normal(seeds[22], (D,), jnp.float32), 0.1, 1.9)
    return {"layer_in": layer_in, "state_in": state_in, "mix_gain": mix_gain, "rec_weight": rec_weight, "key_weight": key_weight, "val_weight": val_weight, "decay_down": decay_down, "decay_up": decay_up, "decay_base": decay_base, "rate_down": rate_down, "rate_up": rate_up, "rate_base": rate_base, "key_scale": key_scale, "group_gain": group_gain, "out_weight": out_weight, "post_gain": post_gain, "ffn_gain": ffn_gain, "routes": routes, "route_gates": route_gates, "expert_gate": expert_gate, "expert_up": expert_up, "expert_down": expert_down, "out_gain": out_gain}


norm_eps = 1e-06
group_eps = 0.00064
clamp_limit = 7.0
gate_alpha = 1.702

def rms_scale(values, scales):
    return values * lax.rsqrt(lax.optimization_barrier(jnp.mean(values * values, axis=-1, keepdims=True)) + norm_eps) * scales

def rounded(values):
    return lax.optimization_barrier(values.astype(jnp.bfloat16)).astype(jnp.float32)

def update_block(inputs):
    old_state, unit_key, decay_factor, learn_rate, val_rows, key_rows, rec_rows = inputs
    along_key = lax.optimization_barrier(jnp.sum(old_state * unit_key[:, :, None, :], axis=-1))
    new_state = old_state * decay_factor[:, :, None, :] - along_key[..., None] * (unit_key * learn_rate)[:, :, None, :] + val_rows[..., None] * (key_rows * learn_rate)[:, :, None, :]
    readout = lax.optimization_barrier(jnp.sum(new_state * rec_rows[:, :, None, :], axis=-1))
    return (new_state, readout)

def reference(layer_in, state_in, mix_gain, rec_weight, key_weight, val_weight, decay_down, decay_up, decay_base, rate_down, rate_up, rate_base, key_scale, group_gain, out_weight, post_gain, ffn_gain, routes, route_gates, expert_gate, expert_up, expert_down, out_gain):
    normed_in = rms_scale(layer_in.astype(jnp.float32), mix_gain).astype(jnp.bfloat16)
    rec_full = rounded(jnp.dot(normed_in, rec_weight, preferred_element_type=jnp.float32))
    key_full = rounded(jnp.dot(normed_in, key_weight, preferred_element_type=jnp.float32))
    val_full = rounded(jnp.dot(normed_in, val_weight, preferred_element_type=jnp.float32))
    decay_hidden = jnp.tanh(jnp.dot(normed_in, decay_down, preferred_element_type=jnp.float32)).astype(jnp.bfloat16)
    rate_hidden = jnp.dot(normed_in, rate_down, preferred_element_type=jnp.float32).astype(jnp.bfloat16)
    decay_pre = decay_base + jnp.dot(decay_hidden, decay_up, preferred_element_type=jnp.float32)
    decay_factor = jnp.exp(-jnp.exp(-jax.nn.softplus(-decay_pre) - 0.5))
    learn_rate = jax.nn.sigmoid(rate_base + jnp.dot(rate_hidden, rate_up, preferred_element_type=jnp.float32))
    head_shape = (N_EP, SEQ_DEV, HEADS, HEAD_DIM)
    key_heads = key_full.reshape(head_shape)
    scaled_key = key_heads * key_scale.reshape(HEADS, HEAD_DIM)
    unit_key = scaled_key * lax.rsqrt(lax.optimization_barrier(jnp.sum(scaled_key * scaled_key, axis=-1, keepdims=True)) + norm_eps)
    old_state = state_in.reshape(N_EP, SEQ_DEV, HEADS, HEAD_DIM, HEAD_DIM)
    new_state, readout = lax.map(update_block, (old_state, unit_key, decay_factor.reshape(head_shape), learn_rate.reshape(head_shape), val_full.reshape(head_shape), key_heads, rec_full.reshape(head_shape)))
    readout = readout.reshape(SEQS, HEADS, HEAD_DIM)
    centred = readout - lax.optimization_barrier(jnp.mean(readout, axis=-1, keepdims=True))
    normed_out = centred * lax.rsqrt(lax.optimization_barrier(jnp.mean(centred * centred, axis=-1, keepdims=True)) + group_eps)
    normed_out = (normed_out * group_gain.reshape(HEADS, HEAD_DIM)).reshape(SEQS, D).astype(jnp.bfloat16)
    grouped_out = normed_out.astype(jnp.float32).reshape(SEQS, N_TP, D // N_TP)
    grouped_weight = out_weight.astype(jnp.float32).reshape(N_TP, D // N_TP, D)
    partials = jnp.einsum('sgc,gcd->gsd', grouped_out, grouped_weight)
    mix_sum = lax.optimization_barrier(jnp.sum(rounded(partials), axis=0))
    middle = (layer_in.astype(jnp.float32) + rms_scale(mix_sum, post_gain)).astype(jnp.bfloat16)
    ffn_in = rms_scale(middle.astype(jnp.float32), ffn_gain).astype(jnp.bfloat16)
    flat_routes = routes.reshape(N_EP, SEQ_DEV * TOPK)
    onehot = (flat_routes[:, :, None] == jnp.arange(EXPERTS, dtype=jnp.int32)[None, None, :]).astype(jnp.int32)
    slot_rank = lax.optimization_barrier(jnp.sum((jnp.cumsum(onehot, axis=1) - 1) * onehot, axis=2))
    source = jnp.arange(N_EP, dtype=jnp.int32)[:, None]
    slot_index = (flat_routes * (N_EP * CAP) + source * CAP + slot_rank).reshape(-1).astype(jnp.int32)
    token_index = jnp.arange(SEQS * TOPK, dtype=jnp.int32) // TOPK
    slot_token = jnp.full((EXPERTS * N_EP * CAP,), SEQS, jnp.int32).at[slot_index].set(token_index)
    padded_in = jnp.concatenate([ffn_in, jnp.zeros((1, D), jnp.bfloat16)], axis=0)

    def run_expert(inputs):
        tokens, w_gate, w_up, w_down = inputs
        taken_rows = padded_in[tokens]
        gate_cut = jnp.minimum(jnp.dot(taken_rows, w_gate, preferred_element_type=jnp.float32), clamp_limit)
        up_cut = jnp.clip(jnp.dot(taken_rows, w_up, preferred_element_type=jnp.float32), -clamp_limit, clamp_limit)
        hidden = ((up_cut + 1.0) * gate_cut * jax.nn.sigmoid(gate_alpha * gate_cut)).astype(jnp.bfloat16)
        grouped = hidden.astype(jnp.float32).reshape(tokens.shape[0], N_TP, FF // N_TP)
        down_groups = w_down.astype(jnp.float32).reshape(N_TP, FF // N_TP, D)
        parts = jnp.einsum('rgf,gfd->grd', grouped, down_groups)
        return lax.optimization_barrier(jnp.sum(rounded(parts), axis=0)).astype(jnp.bfloat16)
    expert_rows = lax.map(run_expert, (slot_token.reshape(EXPERTS, N_EP * CAP), expert_gate, expert_up, expert_down))
    picked = expert_rows.reshape(-1, D)[slot_index].reshape(SEQS, TOPK, D)
    moe_sum = lax.optimization_barrier(jnp.sum(route_gates[:, :, None] * picked.astype(jnp.float32), axis=1))
    layer_out = (middle.astype(jnp.float32) + rms_scale(moe_sum, out_gain)).astype(jnp.bfloat16)
    return (layer_out, new_state.reshape(SEQS, HEADS, HEAD_DIM * HEAD_DIM))
```

```python
import math

import jax
import jax.numpy as jnp
from jax import lax
from jax.experimental import pallas as pl
from jax.experimental.pallas import tpu as pltpu
from jax.sharding import Mesh
from jax.sharding import PartitionSpec as P

HEAD_DIM = 64
LANES = 128
norm_eps = 1e-06
group_eps = 0.00064
clamp_limit = 7.0
gate_alpha = 1.702
f32 = jnp.float32
bf16 = jnp.bfloat16


EP = ("z", "x", "c")
HBM = pl.BlockSpec(memory_space=pl.ANY)
SMEM = pl.BlockSpec(memory_space=pltpu.SMEM)


def dot(a, b):
    return jnp.dot(a, b, preferred_element_type=f32)


def rms_scale(values, scales):
    return values * lax.rsqrt(jnp.mean(values * values, axis=-1, keepdims=True) + norm_eps) * scales


def prep_kernel(x_ref, gain_ref, dd_ref, du_ref, db_ref, rd_ref, ru_ref, rb_ref, ow_ref, send_ref, decay_ref, rate_ref):
    normed = rms_scale(x_ref[...].astype(f32), gain_ref[...]).astype(bf16)
    nz, width = send_ref.shape[0], send_ref.shape[2]
    seqs = normed.shape[0]
    turned = ow_ref[...].astype(f32).T.astype(bf16)
    cols, rows = turned.shape
    for z in range(nz):
        send_ref[z, 0:seqs, :] = normed[:, z * width : (z + 1) * width]
        for part in range(rows // width):
            at = seqs + part * cols
            send_ref[z, at : at + cols, :] = turned[:, part * width : (part + 1) * width]
    decay_hidden = jnp.tanh(dot(normed, dd_ref[...])).astype(bf16)
    rate_hidden = dot(normed, rd_ref[...]).astype(bf16)
    decay_pre = db_ref[...] + dot(decay_hidden, du_ref[...])
    decay_ref[...] = jnp.exp(-math.exp(-0.5) * jax.nn.sigmoid(decay_pre))
    rate_ref[...] = jax.nn.sigmoid(rb_ref[...] + dot(rate_hidden, ru_ref[...]))


def proj_kernel(place_ref, recv_ref, *refs):
    pieces, (out_ref, w_ref, sem_ref) = refs[:8], refs[8:]
    nx = 4
    copies = []
    for n, piece in enumerate(pieces):
        shift, swap = n % nx, n // nx
        x_from = lax.rem(place_ref[0] + (nx - shift), nx)
        c_from = place_ref[1] if swap == 0 else 1 - place_ref[1]
        start = pl.multiple_of((x_from * 2 + c_from) * 32, 32)
        for m in range(3):
            copies.append(
                pltpu.make_async_copy(
                    piece.at[pl.ds(m * 32, 32), :], w_ref.at[m, pl.ds(start, 32), :], sem_ref.at[n, m]
                )
            )
    for copy in copies:
        copy.start()
    nz, seqs, width = recv_ref.shape[0], out_ref.shape[1], recv_ref.shape[2]
    tokens = recv_ref[:, 0:seqs, :].reshape(nz * seqs, width)
    for copy in copies:
        copy.wait()
    for m in range(3):
        part = dot(tokens, w_ref[m]).astype(bf16)
        out_ref[:, :, m * 512 : (m + 1) * 512] = part.reshape(nz, seqs, 512)


def paired(a):
    return jnp.concatenate([a, a], axis=-1)


def state_kernel(parts_ref, decay_ref, rate_ref, scale_ref, gain_ref, state_ref, normed_ref, new_ref,
                 s_ref, p_ref, a_ref, v_ref, head_ref, in_sem, out_sem):
    rows_total = state_ref.shape[0]
    chunk = 32
    chunks = rows_total // chunk
    blocks = state_ref.shape[1] // LANES
    heads = scale_ref.shape[0]
    seqs = rows_total // heads

    def fetch(c):
        span = pl.ds(c * chunk, chunk)
        return pltpu.make_async_copy(state_ref.at[span, :], s_ref.at[span, :], in_sem.at[c])

    def put_back(c):
        span = pl.ds(c * chunk, chunk)
        return pltpu.make_async_copy(s_ref.at[span, :], new_ref.at[span, :], out_sem.at[c])

    for c in range(chunks):
        fetch(c).start()

    total = parts_ref[0].astype(f32)
    for n in range(1, parts_ref.shape[0]):
        total = total + parts_ref[n].astype(f32)
    total = total.astype(bf16).astype(f32)
    local = heads * HEAD_DIM

    def by_head(slot, wide):
        for h in range(heads):
            head_ref[slot, pl.ds(h, seqs, stride=heads), :] = paired(wide[:, h * HEAD_DIM : (h + 1) * HEAD_DIM])

    def per_head(small):
        wide = paired(small)
        return jnp.broadcast_to(wide[None], (seqs, heads, LANES)).reshape(rows_total, LANES)

    by_head(0, total[:, 0:local])
    by_head(1, total[:, local : 2 * local])
    by_head(2, total[:, 2 * local : 3 * local])
    by_head(3, decay_ref[...])
    by_head(4, rate_ref[...])
    keys = head_ref[1]
    rates = head_ref[4]
    scaled = keys * per_head(scale_ref[...])
    squares = jnp.sum((scaled * scaled)[:, 0:HEAD_DIM], axis=-1, keepdims=True)
    unit = scaled * lax.rsqrt(squares + norm_eps)
    head_ref[1] = unit
    head_ref[4] = unit * rates
    head_ref[5] = keys * rates

    def iota(shape, dim):
        return lax.broadcasted_iota(jnp.int32, shape, dim)

    shape = (2 * LANES, LANES)
    half_in = (iota(shape, 0) % LANES) // HEAD_DIM
    spread = (half_in == iota(shape, 1) // HEAD_DIM).astype(f32).astype(bf16)
    gathered = (half_in == iota(shape, 1) % 2).astype(f32).astype(bf16)
    square = (LANES, LANES)
    widen = (iota(square, 0) % 2 == iota(square, 1) // HEAD_DIM).astype(f32).astype(bf16)
    pair_of_lane = iota((chunk, LANES), 1) // 2

    def split(k, values):
        high = values.astype(bf16)
        p_ref[k * chunk : (k + 1) * chunk, 0:LANES] = high
        p_ref[k * chunk : (k + 1) * chunk, LANES : 2 * LANES] = (values - high.astype(f32)).astype(bf16)

    for c in range(chunks):
        rows = pl.ds(c * chunk, chunk)
        fetch(c).wait()
        unit_c = head_ref[1, rows, :]
        val_c = head_ref[2, rows, :]
        for k in range(blocks):
            split(k, s_ref[rows, k * LANES : (k + 1) * LANES] * unit_c)
            v_ref[k * chunk : (k + 1) * chunk, :] = jnp.where(pair_of_lane == k, val_c, 0.0).astype(bf16)
        a_ref[0] = dot(p_ref[...], spread)
        a_ref[1] = dot(v_ref[...], widen)
        rec_c = head_ref[0, rows, :]
        dec_c = head_ref[3, rows, :]
        corr_c = head_ref[4, rows, :]
        add_c = head_ref[5, rows, :]
        for k in range(blocks):
            lanes = slice(k * LANES, (k + 1) * LANES)
            here = slice(k * chunk, (k + 1) * chunk)
            new = s_ref[rows, lanes] * dec_c - a_ref[0, here, :] * corr_c + a_ref[1, here, :] * add_c
            s_ref[rows, lanes] = new
            split(k, new * rec_c)
        put_back(c).start()
        a_ref[0] = dot(p_ref[...], gathered)
        read = jnp.zeros((chunk, LANES), f32)
        for k in range(blocks):
            read = jnp.where(pair_of_lane == k, a_ref[0, k * chunk : (k + 1) * chunk, :], read)
        head_ref[2, rows, :] = read

    read = head_ref[2][:, 0:HEAD_DIM]
    centred = read - jnp.mean(read, axis=-1, keepdims=True)
    normed = centred * lax.rsqrt(jnp.mean(centred * centred, axis=-1, keepdims=True) + group_eps)
    head_ref[2] = paired(normed) * per_head(gain_ref[...])
    for h in range(0, heads, 2):
        low = head_ref[2, pl.ds(h, seqs, stride=heads), :]
        high = head_ref[2, pl.ds(h + 1, seqs, stride=heads), :]
        both = jnp.concatenate([low[:, 0:HEAD_DIM], high[:, 0:HEAD_DIM]], axis=-1).astype(bf16)
        for n in range(normed_ref.shape[0]):
            normed_ref[n, :, h * HEAD_DIM : (h + 2) * HEAD_DIM] = both
    for c in range(chunks):
        put_back(c).wait()


def out_kernel(tok_ref, recv_ref, out_ref):
    groups, seqs, local = tok_ref.shape
    nz, width = recv_ref.shape[0], recv_ref.shape[2]
    cols = width // nz
    tokens = tok_ref[...].reshape(groups * seqs, local)
    weight = jnp.concatenate(
        [recv_ref[:, seqs + p * cols : seqs + (p + 1) * cols, :].reshape(nz * cols, width) for p in range(local // width)],
        axis=-1,
    )
    part = lax.dot_general(tokens, weight, (((1,), (1,)), ((), ())), preferred_element_type=f32)
    part = part.astype(bf16).reshape(groups, seqs, width)
    for t in range(out_ref.shape[1]):
        out_ref[:, t] = part


def mid_kernel(parts_ref, x_ref, post_ref, ffn_ref, table_ref, middle_ref, rows_ref, mix_ref):
    groups, tps, seqs, width = parts_ref.shape
    cols = width // groups
    sums = []
    for g in range(groups):
        total = parts_ref[g, 0].astype(f32)
        for t in range(1, tps):
            total = total + parts_ref[g, t].astype(f32)
        sums.append(total)
    for z in range(groups):
        mix_ref[:, z * width : (z + 1) * width] = jnp.concatenate(
            [sums[g][:, z * cols : (z + 1) * cols] for g in range(groups)], axis=-1
        )
    middle = (x_ref[...].astype(f32) + rms_scale(mix_ref[...], post_ref[...])).astype(bf16)
    middle_ref[...] = middle
    ffn_in = rms_scale(middle.astype(f32), ffn_ref[...]).astype(bf16)
    rows_ref[...] = dot(table_ref[...], ffn_in).astype(bf16)


def local(
    layer_in,
    state_in,
    mix_gain,
    rec_weight,
    key_weight,
    val_weight,
    decay_down,
    decay_up,
    decay_base,
    rate_down,
    rate_up,
    rate_base,
    key_scale,
    group_gain,
    out_weight,
    post_gain,
    ffn_gain,
    routes,
    route_gates,
    expert_gate,
    expert_up,
    expert_down,
    out_gain,
):
    seqs, width = layer_in.shape
    heads = state_in.shape[1]
    local_cols = heads * HEAD_DIM
    nz, nx, nc, ny = (lax.axis_size(a) for a in ("z", "x", "c", "y"))
    nxc = nx * nc
    share = width // nz
    shape = jax.ShapeDtypeStruct

    own = jnp.concatenate([rec_weight, key_weight, val_weight], axis=0)
    pieces = [own] + [lax.ppermute(own, "x", [(i, (i + s) % nx) for i in range(nx)]) for s in range(1, nx)]
    pieces = pieces + [lax.ppermute(p, "c", [(0, 1), (1, 0)]) for p in pieces]
    place = jnp.stack([lax.axis_index("x"), lax.axis_index("c")]).astype(jnp.int32)

    ow_rows = out_weight.shape[0] * out_weight.shape[1] // share
    send, decay_factor, learn_rate = pl.pallas_call(
        prep_kernel,
        out_shape=(
            shape((nz, seqs + ow_rows, share), bf16),
            shape((seqs, local_cols), f32),
            shape((seqs, local_cols), f32),
        ),
        name="prep",
    )(layer_in, mix_gain[None], decay_down, decay_up, decay_base[None], rate_down, rate_up, rate_base[None], out_weight)
    recv = lax.all_to_all(send, "z", split_axis=0, concat_axis=0, tiled=True)

    part = pl.pallas_call(
        proj_kernel,
        out_shape=shape((nz, seqs, 3 * local_cols), bf16),
        in_specs=[SMEM, pl.BlockSpec()] + [HBM] * 8,
        scratch_shapes=[pltpu.VMEM((3, nxc * 32, local_cols), bf16), pltpu.SemaphoreType.DMA((8, 3))],
        name="proj",
    )(place, recv, *pieces)
    parts = lax.all_to_all(part, "z", split_axis=0, concat_axis=0, tiled=True)

    rows = seqs * heads
    lanes_total = state_in.shape[2]
    normed_out, new_state = pl.pallas_call(
        state_kernel,
        out_shape=(shape((nxc, seqs, local_cols), bf16), shape((rows, lanes_total), f32)),
        in_specs=[pl.BlockSpec()] * 5 + [HBM],
        out_specs=(pl.BlockSpec(), HBM),
        scratch_shapes=[
            pltpu.VMEM((rows, lanes_total), f32),
            pltpu.VMEM((32 * (lanes_total // LANES), 2 * LANES), bf16),
            pltpu.VMEM((2, 32 * (lanes_total // LANES), LANES), f32),
            pltpu.VMEM((32 * (lanes_total // LANES), LANES), bf16),
            pltpu.VMEM((6, rows, LANES), f32),
            pltpu.SemaphoreType.DMA((rows // 32,)),
            pltpu.SemaphoreType.DMA((rows // 32,)),
        ],
        name="state",
    )(
        parts,
        decay_factor,
        learn_rate,
        key_scale.reshape(heads, HEAD_DIM),
        group_gain.reshape(heads, HEAD_DIM),
        state_in.reshape(rows, lanes_total),
    )
    tokens = lax.all_to_all(normed_out, ("x", "c"), split_axis=0, concat_axis=0, tiled=True)
    mix_part = pl.pallas_call(
        out_kernel,
        out_shape=shape((nxc, ny, seqs, share), bf16),
        name="outproj",
    )(tokens, recv)
    mix_parts = lax.all_to_all(
        mix_part.reshape(nxc * ny, seqs, share), ("x", "c", "y"), split_axis=0, concat_axis=0, tiled=True
    )

    top_count = routes.shape[1]
    expert_total = nz * nxc
    capacity = max(2, 2 * seqs * top_count // expert_total)
    slot_total = expert_total * capacity
    flat_routes = routes.reshape(-1)
    onehot = (flat_routes[:, None] == jnp.arange(expert_total, dtype=jnp.int32)[None, :]).astype(jnp.int32)
    slot_rank = jnp.sum((jnp.cumsum(onehot, axis=0) - 1) * onehot, axis=1)
    slot_index = flat_routes * capacity + slot_rank
    slot_range = jnp.arange(slot_total, dtype=jnp.int32)
    dispatch_table = jnp.sum(
        (slot_range[:, None] == slot_index[None, :]).astype(bf16).reshape(slot_total, seqs, top_count), axis=2
    )

    middle, send_rows = pl.pallas_call(
        mid_kernel,
        out_shape=(shape((seqs, width), bf16), shape((slot_total, width), bf16)),
        scratch_shapes=[pltpu.VMEM((seqs, width), f32)],
        name="mid",
    )(mix_parts.reshape(nxc, ny, seqs, share), layer_in, post_gain[None], ffn_gain[None], dispatch_table)

    arrived = lax.all_to_all(
        send_rows.reshape(expert_total, capacity, width), EP, split_axis=0, concat_axis=0, tiled=True
    ).reshape(slot_total, width)
    gate_cut = jnp.minimum(dot(arrived, expert_gate[0]), clamp_limit)
    up_cut = jnp.clip(dot(arrived, expert_up[0]), -clamp_limit, clamp_limit)
    hidden = ((up_cut + 1.0) * gate_cut * jax.nn.sigmoid(gate_alpha * gate_cut)).astype(bf16)
    partial_value = dot(hidden, expert_down[0]).astype(bf16)
    back_rows = lax.all_to_all(
        partial_value.reshape(expert_total, capacity, width), EP, split_axis=0, concat_axis=0, tiled=True
    ).reshape(slot_total, width)
    combine_table = (slot_index[:, None] == slot_range[None, :]).astype(bf16)
    picked = dot(combine_table, back_rows)
    moe_part = jnp.sum(route_gates[:, :, None] * picked.reshape(seqs, top_count, width), axis=1)
    copies = jnp.broadcast_to(moe_part.astype(bf16), (ny, seqs, width))
    moe_sum = lax.all_to_all(copies, "y", split_axis=0, concat_axis=0, tiled=True).astype(f32).sum(axis=0)
    layer_out = (middle.astype(f32) + rms_scale(moe_sum, out_gain)).astype(bf16)
    return layer_out, new_state.reshape(seqs, heads, lanes_total)


def solution(mesh):
    mesh = Mesh(mesh.devices.reshape(8, 4, 2, 4), ("z", "x", "c", "y"))
    in_specs = (
        P(EP, None),
        P(EP, "y", None),
        P(),
        P(EP, "y"),
        P(EP, "y"),
        P(EP, "y"),
        P(),
        P(None, "y"),
        P("y"),
        P(),
        P(None, "y"),
        P("y"),
        P("y"),
        P("y"),
        P("y", EP),
        P(),
        P(),
        P(EP, None),
        P(EP, None),
        P(EP, None, "y"),
        P(EP, None, "y"),
        P(EP, "y", None),
        P(),
    )
    out_specs = (P(EP, None), P(EP, "y", None))
    return jax.shard_map(local, mesh=mesh, in_specs=in_specs, out_specs=out_specs, check_vma=False)
```

```python
import math

import jax
import jax.numpy as jnp
from jax import lax
from jax.experimental import pallas as pl
from jax.experimental.pallas import tpu as pltpu
from jax.sharding import Mesh
from jax.sharding import PartitionSpec as P

HEAD_DIM = 64
LANES = 128
norm_eps = 1e-06
group_eps = 0.00064
clamp_limit = 7.0
gate_alpha = 1.702
f32 = jnp.float32
bf16 = jnp.bfloat16


EP = ("z", "x", "c")
HBM = pl.BlockSpec(memory_space=pl.ANY)
SMEM = pl.BlockSpec(memory_space=pltpu.SMEM)
ON_CHIP = pl.BlockSpec(memory_space=pltpu.VMEM)


def dot(a, b):
    return jnp.dot(a, b, preferred_element_type=f32)


def dot_t(a, b):
    return lax.dot_general(a, b, (((1,), (1,)), ((), ())), preferred_element_type=f32)


def on_chip(a):
    return pltpu.with_memory_space_constraint(a, pltpu.VMEM)


def from_others(own, axis):
    size = lax.axis_size(axis)
    return [lax.ppermute(own, axis, [(i, (i + s) % size) for i in range(size)]) for s in range(1, size)]


def rms_scale(values, scales):
    return values * lax.rsqrt(jnp.mean(values * values, axis=-1, keepdims=True) + norm_eps) * scales


def prep_kernel(x_ref, gain_ref, dd_ref, du_ref, db_ref, rd_ref, ru_ref, rb_ref, ow_ref, send_ref, decay_ref, rate_ref):
    normed = rms_scale(x_ref[...].astype(f32), gain_ref[...]).astype(bf16)
    nz, wide = send_ref.shape[0], send_ref.shape[2]
    width, half = wide // 2, normed.shape[0] // 2
    for z in range(nz):
        lanes = slice(z * width, (z + 1) * width)
        send_ref[z, 0:half, 0:width] = normed[0:half, lanes]
        send_ref[z, 0:half, width:wide] = normed[half : 2 * half, lanes]
        send_ref[z, half:, :] = ow_ref[...]
    decay_hidden = jnp.tanh(dot_t(normed, dd_ref[...])).astype(bf16)
    rate_hidden = dot_t(normed, rd_ref[...]).astype(bf16)
    decay_pre = db_ref[...] + dot(decay_hidden, du_ref[...])
    decay_ref[...] = jnp.exp(-math.exp(-0.5) * jax.nn.sigmoid(decay_pre))
    rate_ref[...] = jax.nn.sigmoid(rb_ref[...] + dot(rate_hidden, ru_ref[...]))


def source_of(place_ref, n):
    shift, swap = n % 4, n // 4
    x_from = lax.rem(place_ref[0] + (4 - shift), 4)
    return x_from * 2 + (place_ref[1] if swap == 0 else 1 - place_ref[1])


def proj_kernel(place_ref, recv_ref, *refs):
    pieces, (out_ref, w_ref, tok_ref, sem_ref) = refs[:8], refs[8:]
    copies = []
    for n, piece in enumerate(pieces):
        start = pl.multiple_of(source_of(place_ref, n) * 32, 32)
        for m in range(3):
            copies.append(
                pltpu.make_async_copy(
                    piece.at[pl.ds(m * 32, 32), :], w_ref.at[m, pl.ds(start, 32), :], sem_ref.at[n, m]
                )
            )
    for copy in copies:
        copy.start()
    nz, seqs, width = recv_ref.shape[0], out_ref.shape[1], recv_ref.shape[2] // 2
    half = seqs // 2
    for z in range(nz):
        tok_ref[z, 0:half, :] = recv_ref[z, 0:half, 0:width].astype(f32)
        tok_ref[z, half:, :] = recv_ref[z, 0:half, width:].astype(f32)
    tokens = tok_ref[...].reshape(nz * seqs, width).astype(bf16)
    for copy in copies:
        copy.wait()
    for m in range(3):
        part = dot(tokens, w_ref[m]).astype(bf16)
        out_ref[:, :, m * 512 : (m + 1) * 512] = part.reshape(nz, seqs, 512)


def paired(a):
    return jnp.concatenate([a, a], axis=-1)


def state_kernel(parts_ref, decay_ref, rate_ref, scale_ref, gain_ref, state_ref, normed_ref, new_ref,
                 s_ref, p_ref, a_ref, v_ref, head_ref, in_sem, out_sem):
    rows_total = state_ref.shape[0]
    chunk = 32
    chunks = rows_total // chunk
    blocks = state_ref.shape[1] // LANES
    heads = scale_ref.shape[0]
    seqs = rows_total // heads

    def fetch(c):
        span = pl.ds(c * chunk, chunk)
        return pltpu.make_async_copy(state_ref.at[span, :], s_ref.at[span, :], in_sem.at[c])

    def put_back(c):
        span = pl.ds(c * chunk, chunk)
        return pltpu.make_async_copy(s_ref.at[span, :], new_ref.at[span, :], out_sem.at[c])

    for c in range(chunks):
        fetch(c).start()

    total = parts_ref[0].astype(f32)
    for n in range(1, parts_ref.shape[0]):
        total = total + parts_ref[n].astype(f32)
    total = total.astype(bf16).astype(f32)
    local = heads * HEAD_DIM

    def by_head(slot, wide):
        for h in range(heads):
            head_ref[slot, pl.ds(h, seqs, stride=heads), :] = paired(wide[:, h * HEAD_DIM : (h + 1) * HEAD_DIM])

    def per_head(small):
        wide = paired(small)
        return jnp.broadcast_to(wide[None], (seqs, heads, LANES)).reshape(rows_total, LANES)

    by_head(0, total[:, 0:local])
    by_head(1, total[:, local : 2 * local])
    by_head(2, total[:, 2 * local : 3 * local])
    by_head(3, decay_ref[...])
    by_head(4, rate_ref[...])
    keys = head_ref[1]
    rates = head_ref[4]
    scaled = keys * per_head(scale_ref[...])
    squares = jnp.sum((scaled * scaled)[:, 0:HEAD_DIM], axis=-1, keepdims=True)
    unit = scaled * lax.rsqrt(squares + norm_eps)
    head_ref[1] = unit
    head_ref[4] = unit * rates
    head_ref[5] = keys * rates

    def iota(shape, dim):
        return lax.broadcasted_iota(jnp.int32, shape, dim)

    shape = (2 * LANES, LANES)
    half_in = (iota(shape, 0) % LANES) // HEAD_DIM
    spread = (half_in == iota(shape, 1) // HEAD_DIM).astype(f32).astype(bf16)
    gathered = (half_in == iota(shape, 1) % 2).astype(f32).astype(bf16)
    square = (LANES, LANES)
    widen = (iota(square, 0) % 2 == iota(square, 1) // HEAD_DIM).astype(f32).astype(bf16)
    pair_of_lane = iota((chunk, LANES), 1) // 2

    def split(k, values):
        high = values.astype(bf16)
        p_ref[k * chunk : (k + 1) * chunk, 0:LANES] = high
        p_ref[k * chunk : (k + 1) * chunk, LANES : 2 * LANES] = (values - high.astype(f32)).astype(bf16)

    for c in range(chunks):
        rows = pl.ds(c * chunk, chunk)
        fetch(c).wait()
        unit_c = head_ref[1, rows, :]
        val_c = head_ref[2, rows, :]
        for k in range(blocks):
            split(k, s_ref[rows, k * LANES : (k + 1) * LANES] * unit_c)
            v_ref[k * chunk : (k + 1) * chunk, :] = jnp.where(pair_of_lane == k, val_c, 0.0).astype(bf16)
        a_ref[0] = dot(p_ref[...], spread)
        a_ref[1] = dot(v_ref[...], widen)
        rec_c = head_ref[0, rows, :]
        dec_c = head_ref[3, rows, :]
        corr_c = head_ref[4, rows, :]
        add_c = head_ref[5, rows, :]
        for k in range(blocks):
            lanes = slice(k * LANES, (k + 1) * LANES)
            here = slice(k * chunk, (k + 1) * chunk)
            new = s_ref[rows, lanes] * dec_c - a_ref[0, here, :] * corr_c + a_ref[1, here, :] * add_c
            s_ref[rows, lanes] = new
            split(k, new * rec_c)
        put_back(c).start()
        a_ref[0] = dot(p_ref[...], gathered)
        read = jnp.zeros((chunk, LANES), f32)
        for k in range(blocks):
            read = jnp.where(pair_of_lane == k, a_ref[0, k * chunk : (k + 1) * chunk, :], read)
        head_ref[2, rows, :] = read

    read = head_ref[2][:, 0:HEAD_DIM]
    centred = read - jnp.mean(read, axis=-1, keepdims=True)
    normed = centred * lax.rsqrt(jnp.mean(centred * centred, axis=-1, keepdims=True) + group_eps)
    head_ref[2] = paired(normed) * per_head(gain_ref[...])
    for h in range(0, heads, 2):
        low = head_ref[2, pl.ds(h, seqs, stride=heads), :]
        high = head_ref[2, pl.ds(h + 1, seqs, stride=heads), :]
        both = jnp.concatenate([low[:, 0:HEAD_DIM], high[:, 0:HEAD_DIM]], axis=-1).astype(bf16)
        normed_ref[:, h * HEAD_DIM : (h + 2) * HEAD_DIM] = both
    for c in range(chunks):
        put_back(c).wait()


def out_kernel(place_ref, tok_ref, *refs):
    pieces, (out_ref, part_ref) = refs[:8], refs[8:]
    tokens = tok_ref[...]
    for n, piece in enumerate(pieces):
        part_ref[source_of(place_ref, n)] = dot_t(tokens, piece[...])
    groups, _, width = part_ref.shape
    cols = width // groups
    for z in range(groups):
        out_ref[:, z * width : (z + 1) * width] = jnp.concatenate(
            [part_ref[g, :, z * cols : (z + 1) * cols] for g in range(groups)], axis=-1
        ).astype(bf16)


def sum_in_order(place_ref, piece_refs, line_ref):
    count = len(piece_refs)
    for shift, piece in enumerate(piece_refs):
        line_ref[lax.rem(place_ref[2] + (count - shift), count)] = piece[...].astype(f32)
    total = line_ref[0]
    for n in range(1, count):
        total = total + line_ref[n]
    return total


def mid_kernel(place_ref, p0, p1, p2, p3, x_ref, post_ref, ffn_ref, table_ref, middle_ref, rows_ref, line_ref):
    mix_sum = sum_in_order(place_ref, (p0, p1, p2, p3), line_ref)
    middle = (x_ref[...].astype(f32) + rms_scale(mix_sum, post_ref[...])).astype(bf16)
    middle_ref[...] = middle
    ffn_in = rms_scale(middle.astype(f32), ffn_ref[...]).astype(bf16)
    rows_ref[...] = dot(table_ref[...], ffn_in).astype(bf16)


def last_kernel(place_ref, p0, p1, p2, p3, middle_ref, gain_ref, out_ref, line_ref):
    moe_sum = sum_in_order(place_ref, (p0, p1, p2, p3), line_ref)
    out_ref[...] = (middle_ref[...].astype(f32) + rms_scale(moe_sum, gain_ref[...])).astype(bf16)


def local(
    layer_in,
    state_in,
    mix_gain,
    rec_weight,
    key_weight,
    val_weight,
    decay_down,
    decay_up,
    decay_base,
    rate_down,
    rate_up,
    rate_base,
    key_scale,
    group_gain,
    out_weight,
    post_gain,
    ffn_gain,
    routes,
    route_gates,
    expert_gate,
    expert_up,
    expert_down,
    out_gain,
):
    seqs, width = layer_in.shape
    heads = state_in.shape[1]
    local_cols = heads * HEAD_DIM
    nz, nx, nc, ny = (lax.axis_size(a) for a in ("z", "x", "c", "y"))
    nxc = nx * nc
    share = width // nz
    shape = jax.ShapeDtypeStruct

    own = jnp.concatenate([rec_weight, key_weight, val_weight], axis=0)

    def along_x_and_core(own):
        pieces = [own] + from_others(own, "x")
        return pieces + [p for q in pieces for p in from_others(q, "c")]

    pieces = along_x_and_core(own)
    place = jnp.stack([lax.axis_index("x"), lax.axis_index("c"), lax.axis_index("y")]).astype(jnp.int32)

    send, decay_factor, learn_rate = pl.pallas_call(
        prep_kernel,
        out_shape=(
            pltpu.VMEM((nz, seqs // 2 + out_weight.shape[1], 2 * share), bf16),
            pltpu.VMEM((seqs, local_cols), f32),
            pltpu.VMEM((seqs, local_cols), f32),
        ),
        name="prep",
    )(
        layer_in,
        mix_gain[None],
        decay_down.T,
        decay_up,
        decay_base[None],
        rate_down.T,
        rate_up,
        rate_base[None],
        out_weight.T,
    )
    recv = lax.all_to_all(send, "z", split_axis=0, concat_axis=0, tiled=True)
    ow_pieces = along_x_and_core(recv[:, seqs // 2 :, :].reshape(nz * out_weight.shape[1], local_cols))

    part = pl.pallas_call(
        proj_kernel,
        out_shape=pltpu.VMEM((nz, seqs, 3 * local_cols), bf16),
        in_specs=[SMEM, ON_CHIP] + [ON_CHIP] * 8,
        scratch_shapes=[
            pltpu.VMEM((3, nxc * 32, local_cols), bf16),
            pltpu.VMEM((nz, seqs, share), f32),
            pltpu.SemaphoreType.DMA((8, 3)),
        ],
        name="proj",
    )(place, on_chip(recv), *[on_chip(p) for p in pieces])
    parts = lax.all_to_all(part, "z", split_axis=0, concat_axis=0, tiled=True)

    rows = seqs * heads
    lanes_total = state_in.shape[2]
    normed_out, new_state = pl.pallas_call(
        state_kernel,
        out_shape=(pltpu.VMEM((seqs, local_cols), bf16), shape((rows, lanes_total), f32)),
        in_specs=[ON_CHIP] * 5 + [HBM],
        out_specs=(ON_CHIP, HBM),
        scratch_shapes=[
            pltpu.VMEM((rows, lanes_total), f32),
            pltpu.VMEM((32 * (lanes_total // LANES), 2 * LANES), bf16),
            pltpu.VMEM((2, 32 * (lanes_total // LANES), LANES), f32),
            pltpu.VMEM((32 * (lanes_total // LANES), LANES), bf16),
            pltpu.VMEM((6, rows, LANES), f32),
            pltpu.SemaphoreType.DMA((rows // 32,)),
            pltpu.SemaphoreType.DMA((rows // 32,)),
        ],
        name="state",
    )(
        on_chip(parts),
        on_chip(decay_factor),
        on_chip(learn_rate),
        key_scale.reshape(heads, HEAD_DIM),
        group_gain.reshape(heads, HEAD_DIM),
        state_in.reshape(rows, lanes_total),
    )
    mix_part = pl.pallas_call(
        out_kernel,
        out_shape=pltpu.VMEM((seqs, width), bf16),
        in_specs=[SMEM] + [ON_CHIP] * 9,
        scratch_shapes=[pltpu.VMEM((nxc, seqs, share), f32)],
        name="outproj",
    )(place, on_chip(normed_out), *[on_chip(p) for p in ow_pieces])
    mix_parts = [mix_part] + from_others(mix_part, "y")

    top_count = routes.shape[1]
    expert_total = nz * nxc
    capacity = max(2, 2 * seqs * top_count // expert_total)
    slot_total = expert_total * capacity
    flat_routes = routes.reshape(-1)
    onehot = (flat_routes[:, None] == jnp.arange(expert_total, dtype=jnp.int32)[None, :]).astype(jnp.int32)
    slot_rank = jnp.sum((jnp.cumsum(onehot, axis=0) - 1) * onehot, axis=1)
    slot_index = flat_routes * capacity + slot_rank
    slot_range = jnp.arange(slot_total, dtype=jnp.int32)
    dispatch_table = jnp.sum(
        (slot_range[:, None] == slot_index[None, :]).astype(bf16).reshape(slot_total, seqs, top_count), axis=2
    )

    middle, send_rows = pl.pallas_call(
        mid_kernel,
        out_shape=(pltpu.VMEM((seqs, width), bf16), pltpu.VMEM((slot_total, width), bf16)),
        in_specs=[SMEM] + [ON_CHIP] * 8,
        scratch_shapes=[pltpu.VMEM((ny, seqs, width), f32)],
        name="mid",
    )(
        place,
        *[on_chip(p) for p in mix_parts],
        on_chip(layer_in),
        on_chip(post_gain[None]),
        on_chip(ffn_gain[None]),
        on_chip(dispatch_table),
    )

    arrived = lax.all_to_all(
        send_rows.reshape(expert_total, capacity, width), EP, split_axis=0, concat_axis=0, tiled=True
    ).reshape(slot_total, width)
    gate_cut = jnp.minimum(dot(arrived, expert_gate[0]), clamp_limit)
    up_cut = jnp.clip(dot(arrived, expert_up[0]), -clamp_limit, clamp_limit)
    hidden = ((up_cut + 1.0) * gate_cut * jax.nn.sigmoid(gate_alpha * gate_cut)).astype(bf16)
    partial_value = dot(hidden, expert_down[0]).astype(bf16)
    back_rows = lax.all_to_all(
        partial_value.reshape(expert_total, capacity, width), EP, split_axis=0, concat_axis=0, tiled=True
    ).reshape(slot_total, width)
    combine_table = (slot_index[:, None] == slot_range[None, :]).astype(bf16)
    picked = dot(combine_table, back_rows)
    moe_part = jnp.sum(route_gates[:, :, None] * picked.reshape(seqs, top_count, width), axis=1)
    moe_part = moe_part.astype(bf16)
    layer_out = pl.pallas_call(
        last_kernel,
        out_shape=shape((seqs, width), bf16),
        in_specs=[SMEM] + [ON_CHIP] * 6,
        scratch_shapes=[pltpu.VMEM((ny, seqs, width), f32)],
        name="last",
    )(
        place,
        *[on_chip(p) for p in [moe_part] + from_others(moe_part, "y")],
        on_chip(middle),
        on_chip(out_gain[None]),
    )
    return layer_out, new_state.reshape(seqs, heads, lanes_total)


def solution(mesh):
    mesh = Mesh(mesh.devices.reshape(8, 4, 2, 4), ("z", "x", "c", "y"))
    in_specs = (
        P(EP, None),
        P(EP, "y", None),
        P(),
        P(EP, "y"),
        P(EP, "y"),
        P(EP, "y"),
        P(),
        P(None, "y"),
        P("y"),
        P(),
        P(None, "y"),
        P("y"),
        P("y"),
        P("y"),
        P("y", EP),
        P(),
        P(),
        P(EP, None),
        P(EP, None),
        P(EP, None, "y"),
        P(EP, None, "y"),
        P(EP, "y", None),
        P(),
    )
    out_specs = (P(EP, None), P(EP, "y", None))
    return jax.shard_map(local, mesh=mesh, in_specs=in_specs, out_specs=out_specs, check_vma=False)
```

```python
import math

import jax
import jax.numpy as jnp
from jax import lax
from jax.experimental import pallas as pl
from jax.experimental.pallas import tpu as pltpu
from jax.sharding import Mesh
from jax.sharding import PartitionSpec as P

HEAD_DIM = 64
LANES = 128
norm_eps = 1e-06
group_eps = 0.00064
clamp_limit = 7.0
gate_alpha = 1.702
f32 = jnp.float32
bf16 = jnp.bfloat16


EP = ("z", "x", "c")
HBM = pl.BlockSpec(memory_space=pl.ANY)
SMALL = pltpu.CompilerParams(vmem_limit_bytes=12 * 2**20)
ON_CHIP = pl.BlockSpec(memory_space=pltpu.VMEM)


def dot(a, b):
    return jnp.dot(a, b, preferred_element_type=f32)


def dot_t(a, b):
    return lax.dot_general(a, b, (((1,), (1,)), ((), ())), preferred_element_type=f32)


def on_chip(a):
    return pltpu.with_memory_space_constraint(a, pltpu.VMEM)


def from_others(own, axis):
    size = lax.axis_size(axis)
    return [lax.ppermute(own, axis, [(i, (i + s) % size) for i in range(size)]) for s in range(1, size)]


def rms_scale(values, scales):
    return values * lax.rsqrt(jnp.mean(values * values, axis=-1, keepdims=True) + norm_eps) * scales


def source_of(n):
    x_from = (lax.axis_index("x") + 4 - n % 4) % 4
    return x_from * 2 + (lax.axis_index("c") + n // 4) % 2


def prep_kernel(x_ref, gain_ref, ow_ref, rec_ref, key_ref, val_ref, send_ref, own_ref, normed_ref):
    for m, weight in enumerate((rec_ref, key_ref, val_ref)):
        own_ref[m * 32 : (m + 1) * 32, :] = weight[...]
    normed = rms_scale(x_ref[...].astype(f32), gain_ref[...]).astype(bf16)
    normed_ref[...] = normed
    nz, wide = send_ref.shape[0], send_ref.shape[2]
    seqs = normed.shape[0]
    width, half = wide // 2, seqs // 2
    at = lax.broadcasted_iota(jnp.int32, (width, width), 1)
    piece = at // 32
    x_from = (lax.axis_index("x") + 4 - piece % 4) % 4
    feature = (x_from * 2 + (lax.axis_index("c") + piece // 4) % 2) * 32 + at % 32
    order = (lax.broadcasted_iota(jnp.int32, (width, width), 0) == feature).astype(f32).astype(bf16)
    slices = jnp.concatenate([normed[:, z * width : (z + 1) * width] for z in range(nz)], axis=0)
    slices = dot(slices, order)
    for z in range(nz):
        send_ref[z, 0:half, 0:width] = slices[z * seqs : z * seqs + half].astype(bf16)
        send_ref[z, 0:half, width:wide] = slices[z * seqs + half : (z + 1) * seqs].astype(bf16)
        send_ref[z, half:, :] = ow_ref[...]


def rates_kernel(normed_ref, dd_ref, du_ref, db_ref, rd_ref, ru_ref, rb_ref, decay_ref, rate_ref):
    normed = normed_ref[...]
    decay_hidden = jnp.tanh(dot_t(normed, dd_ref[...])).astype(bf16)
    rate_hidden = dot_t(normed, rd_ref[...]).astype(bf16)
    decay_pre = db_ref[...] + dot(decay_hidden, du_ref[...])
    decay_ref[...] = jnp.exp(-math.exp(-0.5) * jax.nn.sigmoid(decay_pre))
    rate_ref[...] = jax.nn.sigmoid(rb_ref[...] + dot(rate_hidden, ru_ref[...]))


def proj_kernel(recv_ref, *refs):
    pieces, (out_ref, tok_ref) = refs[:8], refs[8:]
    nz, seqs, width = recv_ref.shape[0], out_ref.shape[1], recv_ref.shape[2] // 2
    half = seqs // 2
    for z in range(nz):
        tok_ref[z, 0:half, :] = recv_ref[z, 0:half, 0:width].astype(f32)
        tok_ref[z, half:, :] = recv_ref[z, 0:half, width:].astype(f32)
    tokens = tok_ref[...].reshape(nz * seqs, width).astype(bf16)
    for m in range(3):
        weight = jnp.concatenate([piece[m * 32 : (m + 1) * 32, :] for piece in pieces], axis=0)
        part = dot(tokens, weight).astype(bf16)
        out_ref[:, :, m * 512 : (m + 1) * 512] = part.reshape(nz, seqs, 512)


def paired(a):
    return jnp.concatenate([a, a], axis=-1)


def state_kernel(parts_ref, decay_ref, rate_ref, scale_ref, gain_ref, state_ref, normed_ref, new_ref,
                 s_ref, p_ref, a_ref, v_ref, head_ref, in_sem, out_sem):
    rows_total = state_ref.shape[0]
    chunk = 32
    chunks = rows_total // chunk
    blocks = state_ref.shape[1] // LANES
    heads = scale_ref.shape[0]
    seqs = rows_total // heads

    def fetch(c):
        span = pl.ds(c * chunk, chunk)
        return pltpu.make_async_copy(state_ref.at[span, :], s_ref.at[span, :], in_sem.at[c])

    def put_back(c):
        span = pl.ds(c * chunk, chunk)
        return pltpu.make_async_copy(s_ref.at[span, :], new_ref.at[span, :], out_sem.at[c])

    for c in range(chunks):
        fetch(c).start()

    total = parts_ref[0].astype(f32)
    for n in range(1, parts_ref.shape[0]):
        total = total + parts_ref[n].astype(f32)
    total = total.astype(bf16).astype(f32)
    local = heads * HEAD_DIM

    def by_head(slot, wide):
        for h in range(heads):
            head_ref[slot, pl.ds(h, seqs, stride=heads), :] = paired(wide[:, h * HEAD_DIM : (h + 1) * HEAD_DIM])

    def per_head(small):
        wide = paired(small)
        return jnp.broadcast_to(wide[None], (seqs, heads, LANES)).reshape(rows_total, LANES)

    by_head(0, total[:, 0:local])
    by_head(1, total[:, local : 2 * local])
    by_head(2, total[:, 2 * local : 3 * local])
    by_head(3, decay_ref[...])
    by_head(4, rate_ref[...])
    keys = head_ref[1]
    rates = head_ref[4]
    scaled = keys * per_head(scale_ref[...])
    squares = jnp.sum((scaled * scaled)[:, 0:HEAD_DIM], axis=-1, keepdims=True)
    unit = scaled * lax.rsqrt(squares + norm_eps)
    head_ref[1] = unit
    head_ref[4] = unit * rates
    head_ref[5] = keys * rates

    def iota(shape, dim):
        return lax.broadcasted_iota(jnp.int32, shape, dim)

    shape = (2 * LANES, LANES)
    half_in = (iota(shape, 0) % LANES) // HEAD_DIM
    spread = (half_in == iota(shape, 1) // HEAD_DIM).astype(f32).astype(bf16)
    gathered = (half_in == iota(shape, 1) % 2).astype(f32).astype(bf16)
    square = (LANES, LANES)
    widen = (iota(square, 0) % 2 == iota(square, 1) // HEAD_DIM).astype(f32).astype(bf16)
    pair_of_lane = iota((chunk, LANES), 1) // 2

    def split(k, values):
        high = values.astype(bf16)
        p_ref[k * chunk : (k + 1) * chunk, 0:LANES] = high
        p_ref[k * chunk : (k + 1) * chunk, LANES : 2 * LANES] = (values - high.astype(f32)).astype(bf16)

    for c in range(chunks):
        rows = pl.ds(c * chunk, chunk)
        fetch(c).wait()
        unit_c = head_ref[1, rows, :]
        val_c = head_ref[2, rows, :]
        for k in range(blocks):
            split(k, s_ref[rows, k * LANES : (k + 1) * LANES] * unit_c)
            v_ref[k * chunk : (k + 1) * chunk, :] = jnp.where(pair_of_lane == k, val_c, 0.0).astype(bf16)
        a_ref[0] = dot(p_ref[...], spread)
        a_ref[1] = dot(v_ref[...], widen)
        rec_c = head_ref[0, rows, :]
        dec_c = head_ref[3, rows, :]
        corr_c = head_ref[4, rows, :]
        add_c = head_ref[5, rows, :]
        for k in range(blocks):
            lanes = slice(k * LANES, (k + 1) * LANES)
            here = slice(k * chunk, (k + 1) * chunk)
            new = s_ref[rows, lanes] * dec_c - a_ref[0, here, :] * corr_c + a_ref[1, here, :] * add_c
            s_ref[rows, lanes] = new
            split(k, new * rec_c)
        put_back(c).start()
        a_ref[0] = dot(p_ref[...], gathered)
        read = jnp.zeros((chunk, LANES), f32)
        for k in range(blocks):
            read = jnp.where(pair_of_lane == k, a_ref[0, k * chunk : (k + 1) * chunk, :], read)
        head_ref[2, rows, :] = read

    read = head_ref[2][:, 0:HEAD_DIM]
    centred = read - jnp.mean(read, axis=-1, keepdims=True)
    normed = centred * lax.rsqrt(jnp.mean(centred * centred, axis=-1, keepdims=True) + group_eps)
    head_ref[2] = paired(normed) * per_head(gain_ref[...])
    for h in range(0, heads, 2):
        low = head_ref[2, pl.ds(h, seqs, stride=heads), :]
        high = head_ref[2, pl.ds(h + 1, seqs, stride=heads), :]
        both = jnp.concatenate([low[:, 0:HEAD_DIM], high[:, 0:HEAD_DIM]], axis=-1).astype(bf16)
        normed_ref[:, h * HEAD_DIM : (h + 2) * HEAD_DIM] = both
    for c in range(chunks):
        put_back(c).wait()


def out_kernel(tok_ref, *refs):
    pieces, (out_ref, part_ref) = refs[:8], refs[8:]
    tokens = tok_ref[...]
    for n, piece in enumerate(pieces):
        part_ref[source_of(n)] = dot_t(tokens, piece[...])
    groups, _, width = part_ref.shape
    cols = width // groups
    for z in range(groups):
        out_ref[:, z * width : (z + 1) * width] = jnp.concatenate(
            [part_ref[g, :, z * cols : (z + 1) * cols] for g in range(groups)], axis=-1
        ).astype(bf16)


def sum_in_order(piece_refs, line_ref):
    count = len(piece_refs)
    for shift, piece in enumerate(piece_refs):
        line_ref[(lax.axis_index("y") + count - shift) % count] = piece[...].astype(f32)
    total = line_ref[0]
    for n in range(1, count):
        total = total + line_ref[n]
    return total


def mid_kernel(p0, p1, p2, p3, x_ref, post_ref, ffn_ref, table_ref, middle_ref, rows_ref, line_ref):
    mix_sum = sum_in_order((p0, p1, p2, p3), line_ref)
    middle = (x_ref[...].astype(f32) + rms_scale(mix_sum, post_ref[...])).astype(bf16)
    middle_ref[...] = middle
    ffn_in = rms_scale(middle.astype(f32), ffn_ref[...]).astype(bf16)
    rows_ref[...] = dot(table_ref[...], ffn_in).reshape(rows_ref.shape).astype(bf16)


def expert_kernel(rows_ref, gate_ref, up_ref, down_ref, out_ref, gate_in, up_in, down_in, sem_ref):
    copies = []
    for n, (source, target) in enumerate(((gate_ref, gate_in), (up_ref, up_in), (down_ref, down_in))):
        half = target.shape[0] // 2
        for p in range(2):
            span = pl.ds(p * half, half)
            copies.append(pltpu.make_async_copy(source.at[0, span, :], target.at[span, :], sem_ref.at[n, p]))
            copies[-1].start()

    def product(values, n, target):
        half = target.shape[0] // 2
        copies[2 * n].wait()
        low = dot(values[:, 0:half], target[0:half, :])
        copies[2 * n + 1].wait()
        return low + dot(values[:, half:], target[half:, :])

    rows = rows_ref[...]
    gate_cut = jnp.minimum(product(rows, 0, gate_in), clamp_limit)
    up_cut = jnp.clip(product(rows, 1, up_in), -clamp_limit, clamp_limit)
    hidden = ((up_cut + 1.0) * gate_cut * jax.nn.sigmoid(gate_alpha * gate_cut)).astype(bf16)
    out_ref[...] = product(hidden, 2, down_in).reshape(out_ref.shape).astype(bf16)


def last_kernel(p0, p1, p2, p3, middle_ref, gain_ref, out_ref, line_ref):
    moe_sum = sum_in_order((p0, p1, p2, p3), line_ref)
    out_ref[...] = (middle_ref[...].astype(f32) + rms_scale(moe_sum, gain_ref[...])).astype(bf16)


def local(
    layer_in,
    state_in,
    mix_gain,
    rec_weight,
    key_weight,
    val_weight,
    decay_down,
    decay_up,
    decay_base,
    rate_down,
    rate_up,
    rate_base,
    key_scale,
    group_gain,
    out_weight,
    post_gain,
    ffn_gain,
    routes,
    route_gates,
    expert_gate,
    expert_up,
    expert_down,
    out_gain,
):
    seqs, width = layer_in.shape
    heads = state_in.shape[1]
    local_cols = heads * HEAD_DIM
    nz, nx, nc, ny = (lax.axis_size(a) for a in ("z", "x", "c", "y"))
    nxc = nx * nc
    share = width // nz
    shape = jax.ShapeDtypeStruct

    send, own, normed = pl.pallas_call(
        prep_kernel,
        out_shape=(
            pltpu.VMEM((nz, seqs // 2 + out_weight.shape[1], 2 * share), bf16),
            pltpu.VMEM((3 * rec_weight.shape[0], local_cols), bf16),
            pltpu.VMEM((seqs, width), bf16),
        ),
        name="prep",
    )(layer_in, mix_gain[None], out_weight.T, rec_weight, key_weight, val_weight)
    recv = lax.all_to_all(send, "z", split_axis=0, concat_axis=0, tiled=True)
    along_x = [own] + from_others(own, "x")
    pieces = along_x + [p for q in along_x for p in from_others(q, "c")]
    ow_along_x = recv[:, seqs // 2 :, :].reshape(nz * out_weight.shape[1], local_cols)
    ow_along_x = [ow_along_x] + from_others(ow_along_x, "x")

    decay_factor, learn_rate = pl.pallas_call(
        rates_kernel,
        out_shape=(pltpu.VMEM((seqs, local_cols), f32), pltpu.VMEM((seqs, local_cols), f32)),
        name="rates",
        compiler_params=SMALL,
    )(on_chip(normed), decay_down.T, decay_up, decay_base[None], rate_down.T, rate_up, rate_base[None])

    part = pl.pallas_call(
        proj_kernel,
        out_shape=pltpu.VMEM((nz, seqs, 3 * local_cols), bf16),
        in_specs=[ON_CHIP] * 9,
        scratch_shapes=[
            pltpu.VMEM((nz, seqs, share), f32),
        ],
        name="proj",
        compiler_params=SMALL,
    )(on_chip(recv), *[on_chip(p) for p in pieces])
    parts = lax.all_to_all(part, "z", split_axis=0, concat_axis=0, tiled=True)

    rows = seqs * heads
    lanes_total = state_in.shape[2]
    normed_out, new_state = pl.pallas_call(
        state_kernel,
        out_shape=(pltpu.VMEM((seqs, local_cols), bf16), shape((rows, lanes_total), f32)),
        in_specs=[ON_CHIP] * 5 + [HBM],
        out_specs=(ON_CHIP, HBM),
        scratch_shapes=[
            pltpu.VMEM((rows, lanes_total), f32),
            pltpu.VMEM((32 * (lanes_total // LANES), 2 * LANES), bf16),
            pltpu.VMEM((2, 32 * (lanes_total // LANES), LANES), f32),
            pltpu.VMEM((32 * (lanes_total // LANES), LANES), bf16),
            pltpu.VMEM((6, rows, LANES), f32),
            pltpu.SemaphoreType.DMA((rows // 32,)),
            pltpu.SemaphoreType.DMA((rows // 32,)),
        ],
        name="state",
        compiler_params=SMALL,
    )(
        on_chip(parts),
        on_chip(decay_factor),
        on_chip(learn_rate),
        key_scale.reshape(heads, HEAD_DIM),
        group_gain.reshape(heads, HEAD_DIM),
        state_in.reshape(rows, lanes_total),
    )
    normed_out, *ow_along_x = lax.optimization_barrier((normed_out, *ow_along_x))
    ow_pieces = ow_along_x + [p for q in ow_along_x for p in from_others(q, "c")]
    mix_part = pl.pallas_call(
        out_kernel,
        out_shape=pltpu.VMEM((seqs, width), bf16),
        in_specs=[ON_CHIP] * 9,
        scratch_shapes=[pltpu.VMEM((nxc, seqs, share), f32)],
        name="outproj",
        compiler_params=SMALL,
    )(on_chip(normed_out), *[on_chip(p) for p in ow_pieces])
    mix_parts = [mix_part] + from_others(mix_part, "y")

    top_count = routes.shape[1]
    expert_total = nz * nxc
    capacity = max(2, 2 * seqs * top_count // expert_total)
    slot_total = expert_total * capacity
    flat_routes = routes.reshape(-1)
    onehot = (flat_routes[:, None] == jnp.arange(expert_total, dtype=jnp.int32)[None, :]).astype(jnp.int32)
    slot_rank = jnp.sum((jnp.cumsum(onehot, axis=0) - 1) * onehot, axis=1)
    slot_index = flat_routes * capacity + slot_rank
    slot_range = jnp.arange(slot_total, dtype=jnp.int32)
    dispatch_table = jnp.sum(
        (slot_range[:, None] == slot_index[None, :]).astype(bf16).reshape(slot_total, seqs, top_count), axis=2
    )

    middle, send_rows = pl.pallas_call(
        mid_kernel,
        out_shape=(pltpu.VMEM((seqs, width), bf16), pltpu.VMEM((expert_total, capacity, width), bf16)),
        in_specs=[ON_CHIP] * 8,
        scratch_shapes=[pltpu.VMEM((ny, seqs, width), f32)],
        name="mid",
        compiler_params=SMALL,
    )(
        *[on_chip(p) for p in mix_parts],
        layer_in,
        post_gain[None],
        ffn_gain[None],
        on_chip(dispatch_table),
    )

    arrived = lax.all_to_all(send_rows, EP, split_axis=0, concat_axis=0, tiled=True).reshape(slot_total, width)
    partial_value = pl.pallas_call(
        expert_kernel,
        out_shape=pltpu.VMEM((expert_total, capacity, width), bf16),
        in_specs=[ON_CHIP] + [HBM] * 3,
        scratch_shapes=[pltpu.VMEM(w.shape[1:], bf16) for w in (expert_gate, expert_up, expert_down)]
        + [pltpu.SemaphoreType.DMA((3, 2))],
        name="expert",
    )(on_chip(arrived), expert_gate, expert_up, expert_down)
    back_rows = lax.all_to_all(partial_value, EP, split_axis=0, concat_axis=0, tiled=True).reshape(slot_total, width)
    combine_table = (slot_index[:, None] == slot_range[None, :]).astype(bf16)
    picked = dot(combine_table, back_rows)
    moe_part = jnp.sum(route_gates[:, :, None] * picked.reshape(seqs, top_count, width), axis=1)
    moe_part = moe_part.astype(bf16)
    layer_out = pl.pallas_call(
        last_kernel,
        out_shape=shape((seqs, width), bf16),
        in_specs=[ON_CHIP] * 6,
        scratch_shapes=[pltpu.VMEM((ny, seqs, width), f32)],
        name="last",
        compiler_params=SMALL,
    )(
        *[on_chip(p) for p in [moe_part] + from_others(moe_part, "y")],
        on_chip(middle),
        out_gain[None],
    )
    return layer_out, new_state.reshape(seqs, heads, lanes_total)


def solution(mesh):
    mesh = Mesh(mesh.devices.reshape(8, 4, 2, 4), ("z", "x", "c", "y"))
    in_specs = (
        P(EP, None),
        P(EP, "y", None),
        P(),
        P(EP, "y"),
        P(EP, "y"),
        P(EP, "y"),
        P(),
        P(None, "y"),
        P("y"),
        P(),
        P(None, "y"),
        P("y"),
        P("y"),
        P("y"),
        P("y", EP),
        P(),
        P(),
        P(EP, None),
        P(EP, None),
        P(EP, None, "y"),
        P(EP, None, "y"),
        P(EP, "y", None),
        P(),
    )
    out_specs = (P(EP, None), P(EP, "y", None))
    return jax.shard_map(local, mesh=mesh, in_specs=in_specs, out_specs=out_specs, check_vma=False)
```

```python
import math

import jax
import jax.numpy as jnp
from jax import lax
from jax.experimental import pallas as pl
from jax.experimental.pallas import tpu as pltpu
from jax.sharding import Mesh
from jax.sharding import PartitionSpec as P

HEAD_DIM = 64
CAPACITY = 2
LANES = 128
norm_eps = 1e-06
group_eps = 0.00064
clamp_limit = 7.0
gate_alpha = 1.702
f32 = jnp.float32
bf16 = jnp.bfloat16


EP = ("z", "x", "c")
HBM = pl.BlockSpec(memory_space=pl.ANY)
SMALL = pltpu.CompilerParams(vmem_limit_bytes=12 * 2**20)
ON_CHIP = pl.BlockSpec(memory_space=pltpu.VMEM)


def dot(a, b):
    return jnp.dot(a, b, preferred_element_type=f32)


def dot_t(a, b):
    return lax.dot_general(a, b, (((1,), (1,)), ((), ())), preferred_element_type=f32)


def on_chip(a):
    return pltpu.with_memory_space_constraint(a, pltpu.VMEM)


def from_others(own, axis):
    size = lax.axis_size(axis)
    return [lax.ppermute(own, axis, [(i, (i + s) % size) for i in range(size)]) for s in range(1, size)]


def rms_scale(values, scales):
    return values * lax.rsqrt(jnp.mean(values * values, axis=-1, keepdims=True) + norm_eps) * scales


def source_of(n):
    x_from = (lax.axis_index("x") + 4 - n % 4) % 4
    return x_from * 2 + (lax.axis_index("c") + n // 4) % 2


def prep_kernel(x_ref, gain_ref, ow_ref, rec_ref, key_ref, val_ref, send_ref, own_ref, normed_ref):
    for m, weight in enumerate((rec_ref, key_ref, val_ref)):
        own_ref[m * 32 : (m + 1) * 32, :] = weight[...]
    normed = rms_scale(x_ref[...].astype(f32), gain_ref[...]).astype(bf16)
    normed_ref[...] = normed
    nz, wide = send_ref.shape[0], send_ref.shape[2]
    seqs = normed.shape[0]
    width, half = wide // 2, seqs // 2
    at = lax.broadcasted_iota(jnp.int32, (width, width), 1)
    piece = at // 32
    x_from = (lax.axis_index("x") + 4 - piece % 4) % 4
    feature = (x_from * 2 + (lax.axis_index("c") + piece // 4) % 2) * 32 + at % 32
    order = (lax.broadcasted_iota(jnp.int32, (width, width), 0) == feature).astype(f32).astype(bf16)
    slices = jnp.concatenate([normed[:, z * width : (z + 1) * width] for z in range(nz)], axis=0)
    slices = dot(slices, order)
    for z in range(nz):
        send_ref[z, 0:half, 0:width] = slices[z * seqs : z * seqs + half].astype(bf16)
        send_ref[z, 0:half, width:wide] = slices[z * seqs + half : (z + 1) * seqs].astype(bf16)
        send_ref[z, half:, :] = ow_ref[...]


def rates_kernel(normed_ref, dd_ref, du_ref, db_ref, rd_ref, ru_ref, rb_ref, route_ref, gate_ref,
                 decay_ref, rate_ref, table_ref, mixing_ref):
    normed = normed_ref[...]
    decay_hidden = jnp.tanh(dot_t(normed, dd_ref[...])).astype(bf16)
    rate_hidden = dot_t(normed, rd_ref[...]).astype(bf16)
    decay_pre = db_ref[...] + dot(decay_hidden, du_ref[...])
    decay_ref[...] = jnp.exp(-math.exp(-0.5) * jax.nn.sigmoid(decay_pre))
    rate_ref[...] = jax.nn.sigmoid(rb_ref[...] + dot(rate_hidden, ru_ref[...]))

    seqs = normed.shape[0]
    top_count = route_ref.shape[0]
    slots = table_ref.shape[0]
    square = (seqs, seqs)
    row, col = (lax.broadcasted_iota(jnp.int32, square, d) for d in (0, 1))
    own, earlier = row == col, col < row

    def total(where, values, dim):
        return jnp.sum(jnp.where(where, values, 0.0), axis=dim, keepdims=True)

    along = [jnp.broadcast_to(route_ref[k : k + 1, :].astype(f32), square) for k in range(top_count)]
    down = [total(own, a, 1) for a in along]
    slot_of_row = lax.broadcasted_iota(jnp.int32, (slots, seqs), 0).astype(f32)
    slot_of_lane = lax.broadcasted_iota(jnp.int32, (seqs, slots), 1).astype(f32)
    table = jnp.zeros((slots, seqs), f32)
    mixing = jnp.zeros((seqs, slots), f32)
    for k in range(top_count):
        slot = down[k] * CAPACITY
        for other in along:
            slot = slot + total(earlier & (other == down[k]), 1.0, 1)
        table = table + (slot_of_row == total(own, slot, 0)).astype(f32)
        gate = total(own, jnp.broadcast_to(gate_ref[k : k + 1, :], square), 1)
        mixing = mixing + jnp.where(slot_of_lane == slot, gate, 0.0)
    table_ref[...] = table.astype(bf16)
    high = mixing.astype(bf16)
    mixing_ref[0:seqs, :] = high
    mixing_ref[seqs:, :] = (mixing - high.astype(f32)).astype(bf16)


def proj_kernel(recv_ref, *refs):
    pieces, (out_ref, tok_ref) = refs[:8], refs[8:]
    nz, seqs, width = recv_ref.shape[0], out_ref.shape[1], recv_ref.shape[2] // 2
    half = seqs // 2
    for z in range(nz):
        tok_ref[z, 0:half, :] = recv_ref[z, 0:half, 0:width].astype(f32)
        tok_ref[z, half:, :] = recv_ref[z, 0:half, width:].astype(f32)
    tokens = tok_ref[...].reshape(nz * seqs, width).astype(bf16)
    for m in range(3):
        weight = jnp.concatenate([piece[m * 32 : (m + 1) * 32, :] for piece in pieces], axis=0)
        part = dot(tokens, weight).astype(bf16)
        out_ref[:, :, m * 512 : (m + 1) * 512] = part.reshape(nz, seqs, 512)


def paired(a):
    return jnp.concatenate([a, a], axis=-1)


def state_kernel(parts_ref, decay_ref, rate_ref, scale_ref, gain_ref, state_ref, normed_ref, new_ref,
                 s_ref, p_ref, a_ref, v_ref, head_ref, in_sem, out_sem):
    rows_total = state_ref.shape[0]
    chunk = 32
    chunks = rows_total // chunk
    blocks = state_ref.shape[1] // LANES
    heads = scale_ref.shape[0]
    seqs = rows_total // heads

    def fetch(c):
        span = pl.ds(c * chunk, chunk)
        return pltpu.make_async_copy(state_ref.at[span, :], s_ref.at[span, :], in_sem.at[c])

    def put_back(c):
        span = pl.ds(c * chunk, chunk)
        return pltpu.make_async_copy(s_ref.at[span, :], new_ref.at[span, :], out_sem.at[c])

    for c in range(chunks):
        fetch(c).start()

    total = parts_ref[0].astype(f32)
    for n in range(1, parts_ref.shape[0]):
        total = total + parts_ref[n].astype(f32)
    total = total.astype(bf16).astype(f32)
    local = heads * HEAD_DIM

    def by_head(slot, wide):
        for h in range(heads):
            head_ref[slot, pl.ds(h, seqs, stride=heads), :] = paired(wide[:, h * HEAD_DIM : (h + 1) * HEAD_DIM])

    def per_head(small):
        wide = paired(small)
        return jnp.broadcast_to(wide[None], (seqs, heads, LANES)).reshape(rows_total, LANES)

    by_head(0, total[:, 0:local])
    by_head(1, total[:, local : 2 * local])
    by_head(2, total[:, 2 * local : 3 * local])
    by_head(3, decay_ref[...])
    by_head(4, rate_ref[...])
    keys = head_ref[1]
    rates = head_ref[4]
    scaled = keys * per_head(scale_ref[...])
    squares = jnp.sum((scaled * scaled)[:, 0:HEAD_DIM], axis=-1, keepdims=True)
    unit = scaled * lax.rsqrt(squares + norm_eps)
    head_ref[1] = unit
    head_ref[4] = unit * rates
    head_ref[5] = keys * rates

    def iota(shape, dim):
        return lax.broadcasted_iota(jnp.int32, shape, dim)

    square = (LANES, LANES)
    half_in = iota(square, 0) // HEAD_DIM
    spread = (half_in == iota(square, 1) // HEAD_DIM).astype(f32).astype(bf16)
    gathered = (half_in == iota(square, 1) % 2).astype(f32).astype(bf16)
    widen = (iota(square, 0) % 2 == iota(square, 1) // HEAD_DIM).astype(f32).astype(bf16)
    pair_of_lane = iota((chunk, LANES), 1) // 2

    def keep(k, values):
        p_ref[k * chunk : (k + 1) * chunk, :] = values.astype(bf16)

    for c in range(chunks):
        rows = pl.ds(c * chunk, chunk)
        fetch(c).wait()
        unit_c = head_ref[1, rows, :]
        val_c = head_ref[2, rows, :]
        for k in range(blocks):
            keep(k, s_ref[rows, k * LANES : (k + 1) * LANES] * unit_c)
            v_ref[k * chunk : (k + 1) * chunk, :] = jnp.where(pair_of_lane == k, val_c, 0.0).astype(bf16)
        a_ref[0] = dot(p_ref[...], spread)
        a_ref[1] = dot(v_ref[...], widen)
        rec_c = head_ref[0, rows, :]
        dec_c = head_ref[3, rows, :]
        corr_c = head_ref[4, rows, :]
        add_c = head_ref[5, rows, :]
        for k in range(blocks):
            lanes = slice(k * LANES, (k + 1) * LANES)
            here = slice(k * chunk, (k + 1) * chunk)
            new = s_ref[rows, lanes] * dec_c - a_ref[0, here, :] * corr_c + a_ref[1, here, :] * add_c
            s_ref[rows, lanes] = new
            keep(k, new * rec_c)
        put_back(c).start()
        a_ref[0] = dot(p_ref[...], gathered)
        read = jnp.zeros((chunk, LANES), f32)
        for k in range(blocks):
            read = jnp.where(pair_of_lane == k, a_ref[0, k * chunk : (k + 1) * chunk, :], read)
        head_ref[2, rows, :] = read

    read = head_ref[2][:, 0:HEAD_DIM]
    centred = read - jnp.mean(read, axis=-1, keepdims=True)
    normed = centred * lax.rsqrt(jnp.mean(centred * centred, axis=-1, keepdims=True) + group_eps)
    head_ref[2] = paired(normed) * per_head(gain_ref[...])
    for h in range(0, heads, 2):
        low = head_ref[2, pl.ds(h, seqs, stride=heads), :]
        high = head_ref[2, pl.ds(h + 1, seqs, stride=heads), :]
        both = jnp.concatenate([low[:, 0:HEAD_DIM], high[:, 0:HEAD_DIM]], axis=-1).astype(bf16)
        normed_ref[:, h * HEAD_DIM : (h + 2) * HEAD_DIM] = both
    for c in range(chunks):
        put_back(c).wait()


def out_kernel(tok_ref, *refs):
    pieces, (out_ref, part_ref) = refs[:8], refs[8:]
    tokens = tok_ref[...]
    for n, piece in enumerate(pieces):
        part_ref[source_of(n)] = dot_t(tokens, piece[...])
    groups, _, width = part_ref.shape
    cols = width // groups
    for z in range(groups):
        out_ref[:, z * width : (z + 1) * width] = jnp.concatenate(
            [part_ref[g, :, z * cols : (z + 1) * cols] for g in range(groups)], axis=-1
        ).astype(bf16)


def sum_in_order(piece_refs, line_ref):
    count = len(piece_refs)
    for shift, piece in enumerate(piece_refs):
        line_ref[(lax.axis_index("y") + count - shift) % count] = piece[...].astype(f32)
    total = line_ref[0]
    for n in range(1, count):
        total = total + line_ref[n]
    return total


def mid_kernel(p0, p1, p2, p3, x_ref, post_ref, ffn_ref, table_ref, middle_ref, rows_ref, line_ref):
    mix_sum = sum_in_order((p0, p1, p2, p3), line_ref)
    middle = (x_ref[...].astype(f32) + rms_scale(mix_sum, post_ref[...])).astype(bf16)
    middle_ref[...] = middle
    ffn_in = rms_scale(middle.astype(f32), ffn_ref[...]).astype(bf16)
    rows_ref[...] = dot(table_ref[...], ffn_in).reshape(rows_ref.shape).astype(bf16)


def fetch_kernel(gate_ref, up_ref, down_ref, gate_out, up_out, down_out, sem_ref):
    pairs = ((gate_ref, gate_out), (up_ref, up_out), (down_ref, down_out))
    copies = [pltpu.make_async_copy(a, b, sem_ref.at[n]) for n, (a, b) in enumerate(pairs)]
    for copy in copies:
        copy.start()
    for copy in copies:
        copy.wait()


def combine_kernel(back_ref, mixing_ref, out_ref):
    rows = back_ref[...].astype(f32).reshape(-1, back_ref.shape[2]).astype(bf16)
    both = dot(mixing_ref[...], rows)
    seqs = out_ref.shape[0]
    out_ref[...] = (both[0:seqs] + both[seqs:]).astype(bf16)


def expert_kernel(rows_ref, gate_ref, up_ref, down_ref, out_ref):
    rows = rows_ref[...].astype(f32).reshape(-1, rows_ref.shape[2]).astype(bf16)
    gate_cut = jnp.minimum(dot(rows, gate_ref[0]), clamp_limit)
    up_cut = jnp.clip(dot(rows, up_ref[0]), -clamp_limit, clamp_limit)
    hidden = ((up_cut + 1.0) * gate_cut * jax.nn.sigmoid(gate_alpha * gate_cut)).astype(bf16)
    out_ref[...] = dot(hidden, down_ref[0]).reshape(out_ref.shape).astype(bf16)


def last_kernel(p0, p1, p2, p3, middle_ref, gain_ref, out_ref, line_ref):
    moe_sum = sum_in_order((p0, p1, p2, p3), line_ref)
    out_ref[...] = (middle_ref[...].astype(f32) + rms_scale(moe_sum, gain_ref[...])).astype(bf16)


def local(
    layer_in,
    state_in,
    mix_gain,
    rec_weight,
    key_weight,
    val_weight,
    decay_down,
    decay_up,
    decay_base,
    rate_down,
    rate_up,
    rate_base,
    key_scale,
    group_gain,
    out_weight,
    post_gain,
    ffn_gain,
    routes,
    route_gates,
    expert_gate,
    expert_up,
    expert_down,
    out_gain,
):
    seqs, width = layer_in.shape
    heads = state_in.shape[1]
    local_cols = heads * HEAD_DIM
    nz, nx, nc, ny = (lax.axis_size(a) for a in ("z", "x", "c", "y"))
    nxc = nx * nc
    share = width // nz
    expert_total = nz * nxc
    slot_total = expert_total * CAPACITY
    shape = jax.ShapeDtypeStruct

    send, own, normed = pl.pallas_call(
        prep_kernel,
        out_shape=(
            pltpu.VMEM((nz, seqs // 2 + out_weight.shape[1], 2 * share), bf16),
            pltpu.VMEM((3 * rec_weight.shape[0], local_cols), bf16),
            pltpu.VMEM((seqs, width), bf16),
        ),
        name="prep",
    )(layer_in, mix_gain[None], out_weight.T, rec_weight, key_weight, val_weight)
    recv = lax.all_to_all(send, "z", split_axis=0, concat_axis=0, tiled=True)
    along_x = [own] + from_others(own, "x")
    pieces = along_x + [p for q in along_x for p in from_others(q, "c")]
    ow_along_x = recv[:, seqs // 2 :, :].reshape(nz * out_weight.shape[1], local_cols)
    ow_along_x = [ow_along_x] + from_others(ow_along_x, "x")

    decay_factor, learn_rate, dispatch_table, mixing = pl.pallas_call(
        rates_kernel,
        out_shape=(
            pltpu.VMEM((seqs, local_cols), f32),
            pltpu.VMEM((seqs, local_cols), f32),
            pltpu.VMEM((slot_total, seqs), bf16),
            pltpu.VMEM((2 * seqs, slot_total), bf16),
        ),
        name="rates",
        compiler_params=SMALL,
    )(
        on_chip(normed),
        decay_down.T,
        decay_up,
        decay_base[None],
        rate_down.T,
        rate_up,
        rate_base[None],
        routes.T,
        route_gates.T,
    )

    part = pl.pallas_call(
        proj_kernel,
        out_shape=pltpu.VMEM((nz, seqs, 3 * local_cols), bf16),
        in_specs=[ON_CHIP] * 9,
        scratch_shapes=[
            pltpu.VMEM((nz, seqs, share), f32),
        ],
        name="proj",
        compiler_params=SMALL,
    )(on_chip(recv), *[on_chip(p) for p in pieces])
    parts = lax.all_to_all(part, "z", split_axis=0, concat_axis=0, tiled=True)

    rows = seqs * heads
    lanes_total = state_in.shape[2]
    normed_out, new_state = pl.pallas_call(
        state_kernel,
        out_shape=(pltpu.VMEM((seqs, local_cols), bf16), shape((rows, lanes_total), f32)),
        in_specs=[ON_CHIP] * 5 + [HBM],
        out_specs=(ON_CHIP, HBM),
        scratch_shapes=[
            pltpu.VMEM((rows, lanes_total), f32),
            pltpu.VMEM((32 * (lanes_total // LANES), LANES), bf16),
            pltpu.VMEM((2, 32 * (lanes_total // LANES), LANES), f32),
            pltpu.VMEM((32 * (lanes_total // LANES), LANES), bf16),
            pltpu.VMEM((6, rows, LANES), f32),
            pltpu.SemaphoreType.DMA((rows // 32,)),
            pltpu.SemaphoreType.DMA((rows // 32,)),
        ],
        name="state",
        compiler_params=SMALL,
    )(
        on_chip(parts),
        on_chip(decay_factor),
        on_chip(learn_rate),
        key_scale.reshape(heads, HEAD_DIM),
        group_gain.reshape(heads, HEAD_DIM),
        state_in.reshape(rows, lanes_total),
    )
    ow_others = from_others(ow_along_x[0], "c")
    normed_out, *ow_far = lax.optimization_barrier((normed_out, *ow_along_x[1:]))
    ow_pieces = [ow_along_x[0], *ow_far, *ow_others] + [p for q in ow_far for p in from_others(q, "c")]
    mix_part = pl.pallas_call(
        out_kernel,
        out_shape=pltpu.VMEM((seqs, width), bf16),
        in_specs=[ON_CHIP] * 9,
        scratch_shapes=[pltpu.VMEM((nxc, seqs, share), f32)],
        name="outproj",
        compiler_params=SMALL,
    )(on_chip(normed_out), *[on_chip(p) for p in ow_pieces])
    mix_part, *weights = lax.optimization_barrier((mix_part, expert_gate, expert_up, expert_down))
    mix_parts = [mix_part] + from_others(mix_part, "y")
    weights = pl.pallas_call(
        fetch_kernel,
        out_shape=[pltpu.VMEM(w.shape, bf16) for w in weights],
        in_specs=[HBM] * 3,
        out_specs=[ON_CHIP] * 3,
        scratch_shapes=[pltpu.SemaphoreType.DMA((3,))],
        name="fetch",
        compiler_params=SMALL,
    )(*[pltpu.with_memory_space_constraint(w, pltpu.HBM) for w in weights])
    dispatch_table, *weights = lax.optimization_barrier((dispatch_table, *weights))

    middle, send_rows = pl.pallas_call(
        mid_kernel,
        out_shape=(pltpu.VMEM((seqs, width), bf16), pltpu.VMEM((expert_total, CAPACITY, width), bf16)),
        in_specs=[ON_CHIP] * 8,
        scratch_shapes=[pltpu.VMEM((ny, seqs, width), f32)],
        name="mid",
        compiler_params=SMALL,
    )(
        *[on_chip(p) for p in mix_parts],
        layer_in,
        post_gain[None],
        ffn_gain[None],
        on_chip(dispatch_table),
    )

    arrived = lax.all_to_all(send_rows, EP, split_axis=0, concat_axis=0, tiled=True)
    partial_value = pl.pallas_call(
        expert_kernel,
        out_shape=pltpu.VMEM((expert_total, CAPACITY, width), bf16),
        in_specs=[ON_CHIP] * 4,
        name="expert",
        compiler_params=SMALL,
    )(on_chip(arrived), *[on_chip(w) for w in weights])
    back_rows = lax.all_to_all(partial_value, EP, split_axis=0, concat_axis=0, tiled=True)
    moe_part = pl.pallas_call(
        combine_kernel,
        out_shape=pltpu.VMEM((seqs, width), bf16),
        in_specs=[ON_CHIP] * 2,
        name="combine",
        compiler_params=SMALL,
    )(on_chip(back_rows), on_chip(mixing))
    layer_out = pl.pallas_call(
        last_kernel,
        out_shape=shape((seqs, width), bf16),
        in_specs=[ON_CHIP] * 6,
        scratch_shapes=[pltpu.VMEM((ny, seqs, width), f32)],
        name="last",
        compiler_params=SMALL,
    )(
        *[on_chip(p) for p in [moe_part] + from_others(moe_part, "y")],
        on_chip(middle),
        out_gain[None],
    )
    return layer_out, new_state.reshape(seqs, heads, lanes_total)


def solution(mesh):
    mesh = Mesh(mesh.devices.reshape(8, 4, 2, 4), ("z", "x", "c", "y"))
    in_specs = (
        P(EP, None),
        P(EP, "y", None),
        P(),
        P(EP, "y"),
        P(EP, "y"),
        P(EP, "y"),
        P(),
        P(None, "y"),
        P("y"),
        P(),
        P(None, "y"),
        P("y"),
        P("y"),
        P("y"),
        P("y", EP),
        P(),
        P(),
        P(EP, None),
        P(EP, None),
        P(EP, None, "y"),
        P(EP, None, "y"),
        P(EP, "y", None),
        P(),
    )
    out_specs = (P(EP, None), P(EP, "y", None))
    return jax.shard_map(local, mesh=mesh, in_specs=in_specs, out_specs=out_specs, check_vma=False)
```

```python
import math

import jax
import jax.numpy as jnp
from jax import lax
from jax.experimental import pallas as pl
from jax.experimental.pallas import tpu as pltpu
from jax.sharding import Mesh
from jax.sharding import PartitionSpec as P

HEAD_DIM = 64
CAPACITY = 2
LANES = 128
norm_eps = 1e-06
group_eps = 0.00064
clamp_limit = 7.0
gate_alpha = 1.702
f32 = jnp.float32
bf16 = jnp.bfloat16


EP = ("z", "x", "c")
HBM = pl.BlockSpec(memory_space=pl.ANY)
SMALL = pltpu.CompilerParams(vmem_limit_bytes=12 * 2**20)
ON_CHIP = pl.BlockSpec(memory_space=pltpu.VMEM)


def dot(a, b):
    return jnp.dot(a, b, preferred_element_type=f32)


def dot_t(a, b):
    return lax.dot_general(a, b, (((1,), (1,)), ((), ())), preferred_element_type=f32)


def on_chip(a):
    return pltpu.with_memory_space_constraint(a, pltpu.VMEM)


def from_others(own, axis):
    size = lax.axis_size(axis)
    return [lax.ppermute(own, axis, [(i, (i + s) % size) for i in range(size)]) for s in range(1, size)]


def rms_scale(values, scales):
    return values * lax.rsqrt(jnp.mean(values * values, axis=-1, keepdims=True) + norm_eps) * scales


def source_of(n):
    x_from = (lax.axis_index("x") + 4 - n % 4) % 4
    return x_from * 2 + (lax.axis_index("c") + n // 4) % 2


def prep_kernel(x_ref, gain_ref, ow_ref, rec_ref, key_ref, val_ref, send_ref, own_ref, normed_ref):
    for m, weight in enumerate((rec_ref, key_ref, val_ref)):
        own_ref[m * 32 : (m + 1) * 32, :] = weight[...]
    normed = rms_scale(x_ref[...].astype(f32), gain_ref[...]).astype(bf16)
    normed_ref[...] = normed
    nz, wide = send_ref.shape[0], send_ref.shape[2]
    seqs = normed.shape[0]
    width, half = wide // 2, seqs // 2
    at = lax.broadcasted_iota(jnp.int32, (width, width), 1)
    piece = at // 32
    x_from = (lax.axis_index("x") + 4 - piece % 4) % 4
    feature = (x_from * 2 + (lax.axis_index("c") + piece // 4) % 2) * 32 + at % 32
    order = (lax.broadcasted_iota(jnp.int32, (width, width), 0) == feature).astype(f32).astype(bf16)
    slices = jnp.concatenate([normed[:, z * width : (z + 1) * width] for z in range(nz)], axis=0)
    slices = dot(slices, order)
    for z in range(nz):
        send_ref[z, 0:half, 0:width] = slices[z * seqs : z * seqs + half].astype(bf16)
        send_ref[z, 0:half, width:wide] = slices[z * seqs + half : (z + 1) * seqs].astype(bf16)
        send_ref[z, half:, :] = ow_ref[...]


def rates_kernel(normed_ref, dd_ref, du_ref, db_ref, rd_ref, ru_ref, rb_ref, route_ref, gate_ref,
                 decay_ref, rate_ref, table_ref, mixing_ref):
    normed = normed_ref[...]
    decay_hidden = jnp.tanh(dot_t(normed, dd_ref[...])).astype(bf16)
    rate_hidden = dot_t(normed, rd_ref[...]).astype(bf16)
    decay_pre = db_ref[...] + dot(decay_hidden, du_ref[...])
    decay_ref[...] = jnp.exp(-math.exp(-0.5) * jax.nn.sigmoid(decay_pre))
    rate_ref[...] = jax.nn.sigmoid(rb_ref[...] + dot(rate_hidden, ru_ref[...]))

    seqs = normed.shape[0]
    top_count = route_ref.shape[0]
    slots = table_ref.shape[0]
    square = (seqs, seqs)
    row, col = (lax.broadcasted_iota(jnp.int32, square, d) for d in (0, 1))
    own, earlier = row == col, col < row

    def total(where, values, dim):
        return jnp.sum(jnp.where(where, values, 0.0), axis=dim, keepdims=True)

    along = [jnp.broadcast_to(route_ref[k : k + 1, :].astype(f32), square) for k in range(top_count)]
    down = [total(own, a, 1) for a in along]
    slot_of_row = lax.broadcasted_iota(jnp.int32, (slots, seqs), 0).astype(f32)
    slot_of_lane = lax.broadcasted_iota(jnp.int32, (seqs, slots), 1).astype(f32)
    table = jnp.zeros((slots, seqs), f32)
    mixing = jnp.zeros((seqs, slots), f32)
    for k in range(top_count):
        slot = down[k] * CAPACITY
        for other in along:
            slot = slot + total(earlier & (other == down[k]), 1.0, 1)
        table = table + (slot_of_row == total(own, slot, 0)).astype(f32)
        gate = total(own, jnp.broadcast_to(gate_ref[k : k + 1, :], square), 1)
        mixing = mixing + jnp.where(slot_of_lane == slot, gate, 0.0)
    table_ref[...] = table.astype(bf16)
    high = mixing.astype(bf16)
    mixing_ref[0:seqs, :] = high
    mixing_ref[seqs:, :] = (mixing - high.astype(f32)).astype(bf16)


def proj_kernel(recv_ref, *refs):
    pieces, (out_ref, tok_ref) = refs[:8], refs[8:]
    nz, seqs, width = recv_ref.shape[0], out_ref.shape[1], recv_ref.shape[2] // 2
    half = seqs // 2
    for z in range(nz):
        tok_ref[z, 0:half, :] = recv_ref[z, 0:half, 0:width].astype(f32)
        tok_ref[z, half:, :] = recv_ref[z, 0:half, width:].astype(f32)
    tokens = tok_ref[...].reshape(nz * seqs, width).astype(bf16)
    for m in range(3):
        weight = jnp.concatenate([piece[m * 32 : (m + 1) * 32, :] for piece in pieces], axis=0)
        part = dot(tokens, weight).astype(bf16)
        out_ref[:, :, m * 512 : (m + 1) * 512] = part.reshape(nz, seqs, 512)


def paired(a):
    return jnp.concatenate([a, a], axis=-1)


def state_kernel(parts_ref, decay_ref, rate_ref, scale_ref, gain_ref, state_ref, normed_ref, new_ref,
                 s_ref, p_ref, a_ref, v_ref, head_ref, in_sem, out_sem):
    rows_total = state_ref.shape[0]
    chunk = 32
    chunks = rows_total // chunk
    blocks = state_ref.shape[1] // LANES
    heads = scale_ref.shape[0]
    seqs = rows_total // heads

    def fetch(c):
        span = pl.ds(c * chunk, chunk)
        return pltpu.make_async_copy(state_ref.at[span, :], s_ref.at[span, :], in_sem.at[c])

    def put_back(c):
        span = pl.ds(c * chunk, chunk)
        return pltpu.make_async_copy(s_ref.at[span, :], new_ref.at[span, :], out_sem.at[c])

    for c in range(chunks):
        fetch(c).start()

    total = parts_ref[0].astype(f32)
    for n in range(1, parts_ref.shape[0]):
        total = total + parts_ref[n].astype(f32)
    total = total.astype(bf16).astype(f32)
    local = heads * HEAD_DIM

    def by_head(slot, wide):
        for h in range(heads):
            head_ref[slot, pl.ds(h, seqs, stride=heads), :] = paired(wide[:, h * HEAD_DIM : (h + 1) * HEAD_DIM])

    def per_head(small):
        wide = paired(small)
        return jnp.broadcast_to(wide[None], (seqs, heads, LANES)).reshape(rows_total, LANES)

    by_head(0, total[:, 0:local])
    by_head(1, total[:, local : 2 * local])
    by_head(2, total[:, 2 * local : 3 * local])
    by_head(3, decay_ref[...])
    by_head(4, rate_ref[...])
    keys = head_ref[1]
    rates = head_ref[4]
    scaled = keys * per_head(scale_ref[...])
    squares = jnp.sum((scaled * scaled)[:, 0:HEAD_DIM], axis=-1, keepdims=True)
    unit = scaled * lax.rsqrt(squares + norm_eps)
    head_ref[1] = unit
    head_ref[4] = unit * rates
    head_ref[5] = keys * rates

    def iota(shape, dim):
        return lax.broadcasted_iota(jnp.int32, shape, dim)

    square = (LANES, LANES)
    half_in = iota(square, 0) // HEAD_DIM
    spread = (half_in == iota(square, 1) // HEAD_DIM).astype(f32).astype(bf16)
    gathered = (half_in == iota(square, 1) % 2).astype(f32).astype(bf16)
    widen = (iota(square, 0) % 2 == iota(square, 1) // HEAD_DIM).astype(f32).astype(bf16)
    pair_of_lane = iota((chunk, LANES), 1) // 2

    def keep(k, values):
        p_ref[k * chunk : (k + 1) * chunk, :] = values.astype(bf16)

    for c in range(chunks):
        rows = pl.ds(c * chunk, chunk)
        fetch(c).wait()
        unit_c = head_ref[1, rows, :]
        val_c = head_ref[2, rows, :]
        for k in range(blocks):
            keep(k, s_ref[rows, k * LANES : (k + 1) * LANES] * unit_c)
            v_ref[k * chunk : (k + 1) * chunk, :] = jnp.where(pair_of_lane == k, val_c, 0.0).astype(bf16)
        a_ref[0] = dot(p_ref[...], spread)
        a_ref[1] = dot(v_ref[...], widen)
        rec_c = head_ref[0, rows, :]
        dec_c = head_ref[3, rows, :]
        corr_c = head_ref[4, rows, :]
        add_c = head_ref[5, rows, :]
        for k in range(blocks):
            lanes = slice(k * LANES, (k + 1) * LANES)
            here = slice(k * chunk, (k + 1) * chunk)
            new = s_ref[rows, lanes] * dec_c - a_ref[0, here, :] * corr_c + a_ref[1, here, :] * add_c
            s_ref[rows, lanes] = new
            keep(k, new * rec_c)
        put_back(c).start()
        a_ref[0] = dot(p_ref[...], gathered)
        read = jnp.zeros((chunk, LANES), f32)
        for k in range(blocks):
            read = jnp.where(pair_of_lane == k, a_ref[0, k * chunk : (k + 1) * chunk, :], read)
        head_ref[2, rows, :] = read

    read = head_ref[2][:, 0:HEAD_DIM]
    centred = read - jnp.mean(read, axis=-1, keepdims=True)
    normed = centred * lax.rsqrt(jnp.mean(centred * centred, axis=-1, keepdims=True) + group_eps)
    head_ref[2] = paired(normed) * per_head(gain_ref[...])
    for h in range(0, heads, 2):
        low = head_ref[2, pl.ds(h, seqs, stride=heads), :]
        high = head_ref[2, pl.ds(h + 1, seqs, stride=heads), :]
        both = jnp.concatenate([low[:, 0:HEAD_DIM], high[:, 0:HEAD_DIM]], axis=-1).astype(bf16)
        normed_ref[:, h * HEAD_DIM : (h + 2) * HEAD_DIM] = both
    for c in range(chunks):
        put_back(c).wait()


def out_kernel(tok_ref, *refs):
    pieces, (out_ref, part_ref) = refs[:8], refs[8:]
    tokens = tok_ref[...]
    groups, cols, seqs = 8, 32, tokens.shape[0]
    for n, piece in enumerate(pieces):
        turned = dot_t(piece[...], tokens)
        first = source_of(n) * cols
        for z in range(groups):
            at = pl.multiple_of(first + z * groups * cols, cols)
            part_ref[pl.ds(at, cols), :] = turned[z * cols : (z + 1) * cols, :]
    same = (lax.broadcasted_iota(jnp.int32, (seqs, seqs), 0) == lax.broadcasted_iota(jnp.int32, (seqs, seqs), 1))
    out_ref[...] = dot_t(same.astype(f32).astype(bf16), part_ref[...].astype(bf16)).astype(bf16)


def sum_in_order(piece_refs, line_ref):
    count = len(piece_refs)
    for shift, piece in enumerate(piece_refs):
        line_ref[(lax.axis_index("y") + count - shift) % count] = piece[...].astype(f32)
    total = line_ref[0]
    for n in range(1, count):
        total = total + line_ref[n]
    return total


def mid_kernel(p0, p1, p2, p3, x_ref, post_ref, ffn_ref, table_ref, middle_ref, rows_ref, line_ref):
    mix_sum = sum_in_order((p0, p1, p2, p3), line_ref)
    middle = (x_ref[...].astype(f32) + rms_scale(mix_sum, post_ref[...])).astype(bf16)
    middle_ref[...] = middle
    ffn_in = rms_scale(middle.astype(f32), ffn_ref[...]).astype(bf16)
    rows_ref[...] = dot(table_ref[...], ffn_in).reshape(rows_ref.shape).astype(bf16)


def fetch_kernel(gate_ref, up_ref, gate_out, up_out, sem_ref):
    copies = [
        pltpu.make_async_copy(gate_ref, gate_out, sem_ref.at[0]),
        pltpu.make_async_copy(up_ref, up_out, sem_ref.at[1]),
    ]
    for copy in copies:
        copy.start()
    for copy in copies:
        copy.wait()


def combine_kernel(back_ref, mixing_ref, out_ref):
    rows = back_ref[...].astype(f32).reshape(-1, back_ref.shape[2]).astype(bf16)
    both = dot(mixing_ref[...], rows)
    seqs = out_ref.shape[0]
    out_ref[...] = (both[0:seqs] + both[seqs:]).astype(bf16)


def expert_kernel(rows_ref, gate_ref, up_ref, down_ref, out_ref, down_in, sem_ref):
    copy = pltpu.make_async_copy(down_ref.at[0], down_in, sem_ref.at[0])
    copy.start()
    rows = rows_ref[...].astype(f32).reshape(-1, rows_ref.shape[2]).astype(bf16)
    gate_cut = jnp.minimum(dot(rows, gate_ref[0]), clamp_limit)
    up_cut = jnp.clip(dot(rows, up_ref[0]), -clamp_limit, clamp_limit)
    hidden = ((up_cut + 1.0) * gate_cut * jax.nn.sigmoid(gate_alpha * gate_cut)).astype(bf16)
    copy.wait()
    out_ref[...] = dot(hidden, down_in[...]).reshape(out_ref.shape).astype(bf16)


def last_kernel(p0, p1, p2, p3, middle_ref, gain_ref, out_ref, line_ref):
    moe_sum = sum_in_order((p0, p1, p2, p3), line_ref)
    out_ref[...] = (middle_ref[...].astype(f32) + rms_scale(moe_sum, gain_ref[...])).astype(bf16)


def local(
    layer_in,
    state_in,
    mix_gain,
    rec_weight,
    key_weight,
    val_weight,
    decay_down,
    decay_up,
    decay_base,
    rate_down,
    rate_up,
    rate_base,
    key_scale,
    group_gain,
    out_weight,
    post_gain,
    ffn_gain,
    routes,
    route_gates,
    expert_gate,
    expert_up,
    expert_down,
    out_gain,
):
    seqs, width = layer_in.shape
    heads = state_in.shape[1]
    local_cols = heads * HEAD_DIM
    nz, nx, nc, ny = (lax.axis_size(a) for a in ("z", "x", "c", "y"))
    nxc = nx * nc
    share = width // nz
    expert_total = nz * nxc
    slot_total = expert_total * CAPACITY
    shape = jax.ShapeDtypeStruct

    send, own, normed = pl.pallas_call(
        prep_kernel,
        out_shape=(
            pltpu.VMEM((nz, seqs // 2 + out_weight.shape[1], 2 * share), bf16),
            pltpu.VMEM((3 * rec_weight.shape[0], local_cols), bf16),
            pltpu.VMEM((seqs, width), bf16),
        ),
        name="prep",
    )(layer_in, mix_gain[None], out_weight.T, rec_weight, key_weight, val_weight)
    recv = lax.all_to_all(send, "z", split_axis=0, concat_axis=0, tiled=True)
    along_x = [own] + from_others(own, "x")
    pieces = along_x + [p for q in along_x for p in from_others(q, "c")]
    ow_along_x = recv[:, seqs // 2 :, :].reshape(nz * out_weight.shape[1], local_cols)
    ow_along_x = [ow_along_x] + from_others(ow_along_x, "x")

    decay_factor, learn_rate, dispatch_table, mixing = pl.pallas_call(
        rates_kernel,
        out_shape=(
            pltpu.VMEM((seqs, local_cols), f32),
            pltpu.VMEM((seqs, local_cols), f32),
            pltpu.VMEM((slot_total, seqs), bf16),
            pltpu.VMEM((2 * seqs, slot_total), bf16),
        ),
        name="rates",
    )(
        on_chip(normed),
        decay_down.T,
        decay_up,
        decay_base[None],
        rate_down.T,
        rate_up,
        rate_base[None],
        routes.T,
        route_gates.T,
    )

    part = pl.pallas_call(
        proj_kernel,
        out_shape=pltpu.VMEM((nz, seqs, 3 * local_cols), bf16),
        in_specs=[ON_CHIP] * 9,
        scratch_shapes=[
            pltpu.VMEM((nz, seqs, share), f32),
        ],
        name="proj",
        compiler_params=SMALL,
    )(on_chip(recv), *[on_chip(p) for p in pieces])
    parts = lax.all_to_all(part, "z", split_axis=0, concat_axis=0, tiled=True)

    rows = seqs * heads
    lanes_total = state_in.shape[2]
    normed_out, new_state = pl.pallas_call(
        state_kernel,
        out_shape=(pltpu.VMEM((seqs, local_cols), bf16), shape((rows, lanes_total), f32)),
        in_specs=[ON_CHIP] * 5 + [HBM],
        out_specs=(ON_CHIP, HBM),
        scratch_shapes=[
            pltpu.VMEM((rows, lanes_total), f32),
            pltpu.VMEM((32 * (lanes_total // LANES), LANES), bf16),
            pltpu.VMEM((2, 32 * (lanes_total // LANES), LANES), f32),
            pltpu.VMEM((32 * (lanes_total // LANES), LANES), bf16),
            pltpu.VMEM((6, rows, LANES), f32),
            pltpu.SemaphoreType.DMA((rows // 32,)),
            pltpu.SemaphoreType.DMA((rows // 32,)),
        ],
        name="state",
        compiler_params=SMALL,
    )(
        on_chip(parts),
        on_chip(decay_factor),
        on_chip(learn_rate),
        key_scale.reshape(heads, HEAD_DIM),
        group_gain.reshape(heads, HEAD_DIM),
        state_in.reshape(rows, lanes_total),
    )
    ow_others = from_others(ow_along_x[0], "c")
    normed_out, *ow_far = lax.optimization_barrier((normed_out, *ow_along_x[1:]))
    ow_pieces = [ow_along_x[0], *ow_far, *ow_others] + [p for q in ow_far for p in from_others(q, "c")]
    mix_part = pl.pallas_call(
        out_kernel,
        out_shape=pltpu.VMEM((seqs, width), bf16),
        in_specs=[ON_CHIP] * 9,
        scratch_shapes=[pltpu.VMEM((width, seqs), f32)],
        name="outproj",
        compiler_params=SMALL,
    )(on_chip(normed_out), *[on_chip(p) for p in ow_pieces])
    mix_part, *weights = lax.optimization_barrier((mix_part, expert_gate, expert_up))
    mix_parts = [mix_part] + from_others(mix_part, "y")
    weights = pl.pallas_call(
        fetch_kernel,
        out_shape=[pltpu.VMEM(w.shape, bf16) for w in weights],
        in_specs=[HBM] * 2,
        out_specs=[ON_CHIP] * 2,
        scratch_shapes=[pltpu.SemaphoreType.DMA((2,))],
        name="fetch",
        compiler_params=SMALL,
    )(*[pltpu.with_memory_space_constraint(w, pltpu.HBM) for w in weights])
    dispatch_table, *weights = lax.optimization_barrier((dispatch_table, *weights))

    middle, send_rows = pl.pallas_call(
        mid_kernel,
        out_shape=(pltpu.VMEM((seqs, width), bf16), pltpu.VMEM((expert_total, CAPACITY, width), bf16)),
        in_specs=[ON_CHIP] * 8,
        scratch_shapes=[pltpu.VMEM((ny, seqs, width), f32)],
        name="mid",
        compiler_params=SMALL,
    )(
        *[on_chip(p) for p in mix_parts],
        layer_in,
        post_gain[None],
        ffn_gain[None],
        on_chip(dispatch_table),
    )

    arrived = lax.all_to_all(send_rows, EP, split_axis=0, concat_axis=0, tiled=True)
    partial_value = pl.pallas_call(
        expert_kernel,
        out_shape=pltpu.VMEM((expert_total, CAPACITY, width), bf16),
        in_specs=[ON_CHIP] * 3 + [HBM],
        scratch_shapes=[pltpu.VMEM(expert_down.shape[1:], bf16), pltpu.SemaphoreType.DMA((1,))],
        name="expert",
        compiler_params=SMALL,
    )(
        on_chip(arrived),
        *[on_chip(w) for w in weights],
        pltpu.with_memory_space_constraint(expert_down, pltpu.HBM),
    )
    back_rows = lax.all_to_all(partial_value, EP, split_axis=0, concat_axis=0, tiled=True)
    moe_part = pl.pallas_call(
        combine_kernel,
        out_shape=pltpu.VMEM((seqs, width), bf16),
        in_specs=[ON_CHIP] * 2,
        name="combine",
        compiler_params=SMALL,
    )(on_chip(back_rows), on_chip(mixing))
    layer_out = pl.pallas_call(
        last_kernel,
        out_shape=shape((seqs, width), bf16),
        in_specs=[ON_CHIP] * 6,
        scratch_shapes=[pltpu.VMEM((ny, seqs, width), f32)],
        name="last",
        compiler_params=SMALL,
    )(
        *[on_chip(p) for p in [moe_part] + from_others(moe_part, "y")],
        on_chip(middle),
        out_gain[None],
    )
    return layer_out, new_state.reshape(seqs, heads, lanes_total)


def solution(mesh):
    mesh = Mesh(mesh.devices.reshape(8, 4, 2, 4), ("z", "x", "c", "y"))
    in_specs = (
        P(EP, None),
        P(EP, "y", None),
        P(),
        P(EP, "y"),
        P(EP, "y"),
        P(EP, "y"),
        P(),
        P(None, "y"),
        P("y"),
        P(),
        P(None, "y"),
        P("y"),
        P("y"),
        P("y"),
        P("y", EP),
        P(),
        P(),
        P(EP, None),
        P(EP, None),
        P(EP, None, "y"),
        P(EP, None, "y"),
        P(EP, "y", None),
        P(),
    )
    out_specs = (P(EP, None), P(EP, "y", None))
    return jax.shard_map(local, mesh=mesh, in_specs=in_specs, out_specs=out_specs, check_vma=False)
```

```python
import math

import jax
import jax.numpy as jnp
from jax import lax
from jax.experimental import pallas as pl
from jax.experimental.pallas import tpu as pltpu
from jax.sharding import Mesh
from jax.sharding import PartitionSpec as P

HEAD_DIM = 64
CAPACITY = 2
LANES = 128
norm_eps = 1e-06
group_eps = 0.00064
clamp_limit = 7.0
gate_alpha = 1.702
f32 = jnp.float32
bf16 = jnp.bfloat16


EP = ("z", "x", "c")
HBM = pl.BlockSpec(memory_space=pl.ANY)
SMALL = pltpu.CompilerParams(vmem_limit_bytes=12 * 2**20)
ON_CHIP = pl.BlockSpec(memory_space=pltpu.VMEM)


def dot(a, b):
    return jnp.dot(a, b, preferred_element_type=f32)


def dot_t(a, b):
    return lax.dot_general(a, b, (((1,), (1,)), ((), ())), preferred_element_type=f32)


def on_chip(a):
    return pltpu.with_memory_space_constraint(a, pltpu.VMEM)


def off_chip(a):
    return pltpu.with_memory_space_constraint(a, pltpu.HBM)


def shifted(own, axis, by):
    size = lax.axis_size(axis)
    return lax.ppermute(own, axis, [(i, (i + by) % size) for i in range(size)])


def from_others(own, axis):
    return [shifted(own, axis, s) for s in range(1, lax.axis_size(axis))]


def rms_scale(values, scales):
    return values * lax.rsqrt(jnp.mean(values * values, axis=-1, keepdims=True) + norm_eps) * scales


def source_of(n):
    x_from = (lax.axis_index("x") + 4 - n % 4) % 4
    return x_from * 2 + (lax.axis_index("c") + n // 4) % 2


def prep_kernel(x_ref, gain_ref, ow_ref, rec_ref, key_ref, val_ref, send_ref, own_ref, normed_ref):
    for m, weight in enumerate((rec_ref, key_ref, val_ref)):
        own_ref[m * 32 : (m + 1) * 32, :] = weight[...]
    normed = rms_scale(x_ref[...].astype(f32), gain_ref[...]).astype(bf16)
    normed_ref[...] = normed
    nz, wide = send_ref.shape[0], send_ref.shape[2]
    seqs = normed.shape[0]
    width, half = wide // 2, seqs // 2
    at = lax.broadcasted_iota(jnp.int32, (width, width), 1)
    piece = at // 32
    x_from = (lax.axis_index("x") + 4 - piece % 4) % 4
    feature = (x_from * 2 + (lax.axis_index("c") + piece // 4) % 2) * 32 + at % 32
    order = (lax.broadcasted_iota(jnp.int32, (width, width), 0) == feature).astype(f32).astype(bf16)
    slices = jnp.concatenate([normed[:, z * width : (z + 1) * width] for z in range(nz)], axis=0)
    slices = dot(slices, order)
    for z in range(nz):
        send_ref[z, 0:half, 0:width] = slices[z * seqs : z * seqs + half].astype(bf16)
        send_ref[z, 0:half, width:wide] = slices[z * seqs + half : (z + 1) * seqs].astype(bf16)
        send_ref[z, half:, :] = ow_ref[...]


def rates_kernel(normed_ref, dd_ref, du_ref, db_ref, rd_ref, ru_ref, rb_ref, route_ref, gate_ref,
                 decay_ref, rate_ref, table_ref, mixing_ref):
    normed = normed_ref[...]
    decay_hidden = jnp.tanh(dot_t(normed, dd_ref[...])).astype(bf16)
    rate_hidden = dot_t(normed, rd_ref[...]).astype(bf16)
    decay_pre = db_ref[...] + dot(decay_hidden, du_ref[...])
    decay_ref[...] = jnp.exp(-math.exp(-0.5) * jax.nn.sigmoid(decay_pre))
    rate_ref[...] = jax.nn.sigmoid(rb_ref[...] + dot(rate_hidden, ru_ref[...]))

    seqs = normed.shape[0]
    top_count = route_ref.shape[0]
    slots = table_ref.shape[0]
    square = (seqs, seqs)
    row, col = (lax.broadcasted_iota(jnp.int32, square, d) for d in (0, 1))
    own, earlier = row == col, col < row

    def total(where, values, dim):
        return jnp.sum(jnp.where(where, values, 0.0), axis=dim, keepdims=True)

    along = [jnp.broadcast_to(route_ref[k : k + 1, :].astype(f32), square) for k in range(top_count)]
    down = [total(own, a, 1) for a in along]
    slot_of_row = lax.broadcasted_iota(jnp.int32, (slots, seqs), 0).astype(f32)
    slot_of_lane = lax.broadcasted_iota(jnp.int32, (seqs, slots), 1).astype(f32)
    table = jnp.zeros((slots, seqs), f32)
    mixing = jnp.zeros((seqs, slots), f32)
    for k in range(top_count):
        slot = down[k] * CAPACITY
        for other in along:
            slot = slot + total(earlier & (other == down[k]), 1.0, 1)
        table = table + (slot_of_row == total(own, slot, 0)).astype(f32)
        gate = total(own, jnp.broadcast_to(gate_ref[k : k + 1, :], square), 1)
        mixing = mixing + jnp.where(slot_of_lane == slot, gate, 0.0)
    table_ref[...] = table.astype(bf16)
    high = mixing.astype(bf16)
    mixing_ref[0:seqs, :] = high
    mixing_ref[seqs:, :] = (mixing - high.astype(f32)).astype(bf16)


def proj_kernel(recv_ref, *refs):
    pieces, (out_ref, tok_ref) = refs[:8], refs[8:]
    nz, seqs, width = recv_ref.shape[0], out_ref.shape[1], recv_ref.shape[2] // 2
    half = seqs // 2
    for z in range(nz):
        tok_ref[z, 0:half, :] = recv_ref[z, 0:half, 0:width].astype(f32)
        tok_ref[z, half:, :] = recv_ref[z, 0:half, width:].astype(f32)
    tokens = tok_ref[...].reshape(nz * seqs, width).astype(bf16)
    for m in range(3):
        weight = jnp.concatenate([piece[m * 32 : (m + 1) * 32, :] for piece in pieces], axis=0)
        part = dot(tokens, weight).astype(bf16)
        out_ref[:, :, m * 512 : (m + 1) * 512] = part.reshape(nz, seqs, 512)


def paired(a):
    return jnp.concatenate([a, a], axis=-1)


def state_kernel(parts_ref, decay_ref, rate_ref, scale_ref, gain_ref, state_ref, normed_ref, new_ref,
                 s_ref, p_ref, a_ref, v_ref, head_ref, in_sem, out_sem):
    rows_total = state_ref.shape[0]
    chunk = 32
    chunks = rows_total // chunk
    blocks = state_ref.shape[1] // LANES
    heads = scale_ref.shape[1] // HEAD_DIM
    seqs = rows_total // heads

    def fetch(c):
        span = pl.ds(c * chunk, chunk)
        return pltpu.make_async_copy(state_ref.at[span, :], s_ref.at[span, :], in_sem.at[c])

    def put_back(c):
        span = pl.ds(c * chunk, chunk)
        return pltpu.make_async_copy(s_ref.at[span, :], new_ref.at[span, :], out_sem.at[c])

    for c in range(chunks):
        fetch(c).start()

    total = parts_ref[0].astype(f32)
    for n in range(1, parts_ref.shape[0]):
        total = total + parts_ref[n].astype(f32)
    total = total.astype(bf16).astype(f32)
    local = heads * HEAD_DIM

    def by_head(slot, wide):
        for h in range(heads):
            head_ref[slot, pl.ds(h, seqs, stride=heads), :] = paired(wide[:, h * HEAD_DIM : (h + 1) * HEAD_DIM])

    def per_head(slot, gain_ref):
        by_head(slot, jnp.broadcast_to(gain_ref[...], (seqs, local)))
        return head_ref[slot]

    by_head(0, total[:, 0:local])
    by_head(1, total[:, local : 2 * local])
    by_head(2, total[:, 2 * local : 3 * local])
    by_head(3, decay_ref[...])
    by_head(4, rate_ref[...])
    keys = head_ref[1]
    rates = head_ref[4]
    scaled = keys * per_head(5, scale_ref)
    squares = jnp.sum((scaled * scaled)[:, 0:HEAD_DIM], axis=-1, keepdims=True)
    unit = scaled * lax.rsqrt(squares + norm_eps)
    head_ref[1] = unit
    head_ref[4] = unit * rates
    head_ref[5] = keys * rates

    def iota(shape, dim):
        return lax.broadcasted_iota(jnp.int32, shape, dim)

    square = (LANES, LANES)
    half_in = iota(square, 0) // HEAD_DIM
    spread = (half_in == iota(square, 1) // HEAD_DIM).astype(f32).astype(bf16)
    gathered = (half_in == iota(square, 1) % 2).astype(f32).astype(bf16)
    widen = (iota(square, 0) % 2 == iota(square, 1) // HEAD_DIM).astype(f32).astype(bf16)
    pair_of_lane = iota((chunk, LANES), 1) // 2

    def keep(k, values):
        p_ref[k * chunk : (k + 1) * chunk, :] = values.astype(bf16)

    for c in range(chunks):
        rows = pl.ds(c * chunk, chunk)
        fetch(c).wait()
        unit_c = head_ref[1, rows, :]
        val_c = head_ref[2, rows, :]
        for k in range(blocks):
            keep(k, s_ref[rows, k * LANES : (k + 1) * LANES] * unit_c)
            v_ref[k * chunk : (k + 1) * chunk, :] = jnp.where(pair_of_lane == k, val_c, 0.0).astype(bf16)
        a_ref[0] = dot(p_ref[...], spread)
        a_ref[1] = dot(v_ref[...], widen)
        rec_c = head_ref[0, rows, :]
        dec_c = head_ref[3, rows, :]
        corr_c = head_ref[4, rows, :]
        add_c = head_ref[5, rows, :]
        for k in range(blocks):
            lanes = slice(k * LANES, (k + 1) * LANES)
            here = slice(k * chunk, (k + 1) * chunk)
            new = s_ref[rows, lanes] * dec_c - a_ref[0, here, :] * corr_c + a_ref[1, here, :] * add_c
            s_ref[rows, lanes] = new
            keep(k, new * rec_c)
        put_back(c).start()
        a_ref[0] = dot(p_ref[...], gathered)
        read = jnp.zeros((chunk, LANES), f32)
        for k in range(blocks):
            read = jnp.where(pair_of_lane == k, a_ref[0, k * chunk : (k + 1) * chunk, :], read)
        head_ref[2, rows, :] = read

    read = head_ref[2][:, 0:HEAD_DIM]
    centred = read - jnp.mean(read, axis=-1, keepdims=True)
    normed = centred * lax.rsqrt(jnp.mean(centred * centred, axis=-1, keepdims=True) + group_eps)
    head_ref[2] = paired(normed) * per_head(5, gain_ref)
    for h in range(0, heads, 2):
        low = head_ref[2, pl.ds(h, seqs, stride=heads), :]
        high = head_ref[2, pl.ds(h + 1, seqs, stride=heads), :]
        both = jnp.concatenate([low[:, 0:HEAD_DIM], high[:, 0:HEAD_DIM]], axis=-1).astype(bf16)
        normed_ref[:, h * HEAD_DIM : (h + 2) * HEAD_DIM] = both
    for c in range(chunks):
        put_back(c).wait()


def out_kernel(tok_ref, *refs):
    pieces, (down_ref, out_ref, down_out, part_ref, sem_ref) = refs[:10], refs[10:]
    fetch = pltpu.make_async_copy(down_ref, down_out, sem_ref.at[0])
    fetch.start()
    tokens = tok_ref[...]
    groups, cols, seqs = 8, 32, tokens.shape[0]
    for n, piece in enumerate(pieces):
        shift, first_z = ((0, 0), (1, 0), (3, 0), (2, 0), (2, groups // 2))[n % 5]
        first = source_of(shift + n // 5 * 4) * cols
        turned = dot_t(piece[...], tokens)
        for z in range(piece.shape[0] // cols):
            at = pl.multiple_of(first + (z + first_z) * groups * cols, cols)
            part_ref[pl.ds(at, cols), :] = turned[z * cols : (z + 1) * cols, :]
    same = (lax.broadcasted_iota(jnp.int32, (seqs, seqs), 0) == lax.broadcasted_iota(jnp.int32, (seqs, seqs), 1))
    out_ref[...] = dot_t(same.astype(f32).astype(bf16), part_ref[...].astype(bf16)).astype(bf16)
    fetch.wait()


def sum_in_order(piece_refs, line_ref):
    count = len(piece_refs)
    for shift, piece in enumerate(piece_refs):
        line_ref[(lax.axis_index("y") + count - shift) % count] = piece[...].astype(f32)
    total = line_ref[0]
    for n in range(1, count):
        total = total + line_ref[n]
    return total


def mid_kernel(p0, p1, p2, p3, x_ref, post_ref, ffn_ref, table_ref, middle_ref, rows_ref, line_ref):
    mix_sum = sum_in_order((p0, p1, p2, p3), line_ref)
    middle = (x_ref[...].astype(f32) + rms_scale(mix_sum, post_ref[...])).astype(bf16)
    middle_ref[...] = middle
    ffn_in = rms_scale(middle.astype(f32), ffn_ref[...]).astype(bf16)
    rows_ref[...] = dot(table_ref[...], ffn_in).reshape(rows_ref.shape).astype(bf16)


def fetch_kernel(gate_ref, up_ref, gate_out, up_out, sem_ref):
    copies = [
        pltpu.make_async_copy(gate_ref, gate_out, sem_ref.at[0]),
        pltpu.make_async_copy(up_ref, up_out, sem_ref.at[1]),
    ]
    for copy in copies:
        copy.start()
    for copy in copies:
        copy.wait()


def combine_kernel(back_ref, mixing_ref, out_ref):
    rows = back_ref[...].astype(f32).reshape(-1, back_ref.shape[2]).astype(bf16)
    both = dot(mixing_ref[...], rows)
    seqs = out_ref.shape[0]
    out_ref[...] = (both[0:seqs] + both[seqs:]).astype(bf16)


def expert_kernel(rows_ref, gate_ref, up_ref, down_ref, out_ref):
    rows = rows_ref[...].astype(f32).reshape(-1, rows_ref.shape[2]).astype(bf16)
    gate_cut = jnp.minimum(dot(rows, gate_ref[0]), clamp_limit)
    up_cut = jnp.clip(dot(rows, up_ref[0]), -clamp_limit, clamp_limit)
    hidden = ((up_cut + 1.0) * gate_cut * jax.nn.sigmoid(gate_alpha * gate_cut)).astype(bf16)
    out_ref[...] = dot(hidden, down_ref[0]).reshape(out_ref.shape).astype(bf16)


def last_kernel(p0, p1, p2, p3, middle_ref, gain_ref, out_ref, line_ref):
    moe_sum = sum_in_order((p0, p1, p2, p3), line_ref)
    out_ref[...] = (middle_ref[...].astype(f32) + rms_scale(moe_sum, gain_ref[...])).astype(bf16)


def local(
    layer_in,
    state_in,
    mix_gain,
    rec_weight,
    key_weight,
    val_weight,
    decay_down,
    decay_up,
    decay_base,
    rate_down,
    rate_up,
    rate_base,
    key_scale,
    group_gain,
    out_weight,
    post_gain,
    ffn_gain,
    routes,
    route_gates,
    expert_gate,
    expert_up,
    expert_down,
    out_gain,
):
    seqs, width = layer_in.shape
    heads = state_in.shape[1]
    local_cols = heads * HEAD_DIM
    nz, nx, nc, ny = (lax.axis_size(a) for a in ("z", "x", "c", "y"))
    nxc = nx * nc
    share = width // nz
    expert_total = nz * nxc
    slot_total = expert_total * CAPACITY
    shape = jax.ShapeDtypeStruct

    send, own, normed = pl.pallas_call(
        prep_kernel,
        out_shape=(
            pltpu.VMEM((nz, seqs // 2 + out_weight.shape[1], 2 * share), bf16),
            pltpu.VMEM((3 * rec_weight.shape[0], local_cols), bf16),
            pltpu.VMEM((seqs, width), bf16),
        ),
        name="prep",
    )(layer_in, mix_gain[None], out_weight.T, rec_weight, key_weight, val_weight)
    recv = lax.all_to_all(send, "z", split_axis=0, concat_axis=0, tiled=True)
    along_x = [own] + from_others(own, "x")
    pieces = along_x + [p for q in along_x for p in from_others(q, "c")]
    ow_own = recv[:, seqs // 2 :, :].reshape(nz * out_weight.shape[1], local_cols)
    ow_next, ow_last = shifted(ow_own, "x", 1), shifted(ow_own, "x", -1)
    decay_factor, learn_rate, dispatch_table, mixing = pl.pallas_call(
        rates_kernel,
        out_shape=(
            pltpu.VMEM((seqs, local_cols), f32),
            pltpu.VMEM((seqs, local_cols), f32),
            pltpu.VMEM((slot_total, seqs), bf16),
            pltpu.VMEM((2 * seqs, slot_total), bf16),
        ),
        name="rates",
        compiler_params=SMALL,
    )(
        on_chip(normed),
        off_chip(decay_down.T),
        off_chip(decay_up),
        off_chip(decay_base[None]),
        off_chip(rate_down.T),
        off_chip(rate_up),
        off_chip(rate_base[None]),
        off_chip(routes.T),
        off_chip(route_gates.T),
    )

    ow_next, ow_last, decay_factor = lax.optimization_barrier((ow_next, ow_last, decay_factor))
    half = ow_own.shape[0] // 2
    ow_low, ow_high = shifted(ow_last[:half], "x", -1), shifted(ow_next[half:], "x", 1)

    part = pl.pallas_call(
        proj_kernel,
        out_shape=pltpu.VMEM((nz, seqs, 3 * local_cols), bf16),
        in_specs=[ON_CHIP] * 9,
        scratch_shapes=[
            pltpu.VMEM((nz, seqs, share), f32),
        ],
        name="proj",
        compiler_params=SMALL,
    )(on_chip(recv), *[on_chip(p) for p in pieces])
    parts = lax.all_to_all(part, "z", split_axis=0, concat_axis=0, tiled=True)

    rows = seqs * heads
    lanes_total = state_in.shape[2]
    normed_out, new_state = pl.pallas_call(
        state_kernel,
        out_shape=(pltpu.VMEM((seqs, local_cols), bf16), shape((rows, lanes_total), f32)),
        in_specs=[ON_CHIP] * 5 + [HBM],
        out_specs=(ON_CHIP, HBM),
        scratch_shapes=[
            pltpu.VMEM((rows, lanes_total), f32),
            pltpu.VMEM((32 * (lanes_total // LANES), LANES), bf16),
            pltpu.VMEM((2, 32 * (lanes_total // LANES), LANES), f32),
            pltpu.VMEM((32 * (lanes_total // LANES), LANES), bf16),
            pltpu.VMEM((6, rows, LANES), f32),
            pltpu.SemaphoreType.DMA((rows // 32,)),
            pltpu.SemaphoreType.DMA((rows // 32,)),
        ],
        name="state",
        compiler_params=SMALL,
    )(
        on_chip(parts),
        on_chip(decay_factor),
        on_chip(learn_rate),
        off_chip(key_scale[None]),
        off_chip(group_gain[None]),
        off_chip(state_in.reshape(rows, lanes_total)),
    )
    normed_out, ow_low, ow_high = lax.optimization_barrier((normed_out, ow_low, ow_high))
    ow_pieces = [ow_own, ow_next, ow_last, ow_low, ow_high]
    ow_pieces = ow_pieces + [shifted(p, "c", 1) for p in ow_pieces]
    mix_part, down = pl.pallas_call(
        out_kernel,
        out_shape=(pltpu.VMEM((seqs, width), bf16), pltpu.VMEM(expert_down.shape, bf16)),
        in_specs=[ON_CHIP] * 11 + [HBM],
        out_specs=(ON_CHIP, ON_CHIP),
        scratch_shapes=[pltpu.VMEM((width, seqs), f32), pltpu.SemaphoreType.DMA((1,))],
        name="outproj",
        compiler_params=SMALL,
    )(on_chip(normed_out), *[on_chip(p) for p in ow_pieces], off_chip(expert_down))
    mix_part, *weights = lax.optimization_barrier((mix_part, expert_gate, expert_up))
    mix_parts = [mix_part] + from_others(mix_part, "y")
    weights = pl.pallas_call(
        fetch_kernel,
        out_shape=[pltpu.VMEM(w.shape, bf16) for w in weights],
        in_specs=[HBM] * 2,
        out_specs=[ON_CHIP] * 2,
        scratch_shapes=[pltpu.SemaphoreType.DMA((2,))],
        name="fetch",
        compiler_params=SMALL,
    )(*[off_chip(w) for w in weights])
    dispatch_table, *weights = lax.optimization_barrier((dispatch_table, *weights))

    middle, send_rows = pl.pallas_call(
        mid_kernel,
        out_shape=(pltpu.VMEM((seqs, width), bf16), pltpu.VMEM((expert_total, CAPACITY, width), bf16)),
        in_specs=[ON_CHIP] * 8,
        scratch_shapes=[pltpu.VMEM((ny, seqs, width), f32)],
        name="mid",
        compiler_params=SMALL,
    )(
        *[on_chip(p) for p in mix_parts],
        layer_in,
        post_gain[None],
        ffn_gain[None],
        on_chip(dispatch_table),
    )

    arrived = lax.all_to_all(send_rows, EP, split_axis=0, concat_axis=0, tiled=True)
    partial_value = pl.pallas_call(
        expert_kernel,
        out_shape=pltpu.VMEM((expert_total, CAPACITY, width), bf16),
        in_specs=[ON_CHIP] * 4,
        name="expert",
        compiler_params=SMALL,
    )(on_chip(arrived), *[on_chip(w) for w in weights], on_chip(down))
    back_rows = lax.all_to_all(partial_value, EP, split_axis=0, concat_axis=0, tiled=True)
    moe_part = pl.pallas_call(
        combine_kernel,
        out_shape=pltpu.VMEM((seqs, width), bf16),
        in_specs=[ON_CHIP] * 2,
        name="combine",
        compiler_params=SMALL,
    )(on_chip(back_rows), on_chip(mixing))
    layer_out = pl.pallas_call(
        last_kernel,
        out_shape=shape((seqs, width), bf16),
        in_specs=[ON_CHIP] * 6,
        scratch_shapes=[pltpu.VMEM((ny, seqs, width), f32)],
        name="last",
        compiler_params=SMALL,
    )(
        *[on_chip(p) for p in [moe_part] + from_others(moe_part, "y")],
        on_chip(middle),
        out_gain[None],
    )
    return layer_out, new_state.reshape(seqs, heads, lanes_total)


def solution(mesh):
    mesh = Mesh(mesh.devices.reshape(8, 4, 2, 4), ("z", "x", "c", "y"))
    in_specs = (
        P(EP, None),
        P(EP, "y", None),
        P(),
        P(EP, "y"),
        P(EP, "y"),
        P(EP, "y"),
        P(),
        P(None, "y"),
        P("y"),
        P(),
        P(None, "y"),
        P("y"),
        P("y"),
        P("y"),
        P("y", EP),
        P(),
        P(),
        P(EP, None),
        P(EP, None),
        P(EP, None, "y"),
        P(EP, None, "y"),
        P(EP, "y", None),
        P(),
    )
    out_specs = (P(EP, None), P(EP, "y", None))
    return jax.shard_map(local, mesh=mesh, in_specs=in_specs, out_specs=out_specs, check_vma=False)
```

```python
import math

import jax
import jax.numpy as jnp
from jax import lax
from jax.experimental import pallas as pl
from jax.experimental.pallas import tpu as pltpu
from jax.sharding import Mesh
from jax.sharding import PartitionSpec as P

HEAD_DIM = 64
CAPACITY = 2
LANES = 128
norm_eps = 1e-06
group_eps = 0.00064
clamp_limit = 7.0
gate_alpha = 1.702
f32 = jnp.float32
bf16 = jnp.bfloat16


EP = ("z", "x", "c")
HBM = pl.BlockSpec(memory_space=pl.ANY)
SMALL = pltpu.CompilerParams(vmem_limit_bytes=12 * 2**20)
ON_CHIP = pl.BlockSpec(memory_space=pltpu.VMEM)


def dot(a, b):
    return jnp.dot(a, b, preferred_element_type=f32)


def dot_t(a, b):
    return lax.dot_general(a, b, (((1,), (1,)), ((), ())), preferred_element_type=f32)


def on_chip(a):
    return pltpu.with_memory_space_constraint(a, pltpu.VMEM)


def off_chip(a):
    return pltpu.with_memory_space_constraint(a, pltpu.HBM)


def shifted(own, axis, by):
    size = lax.axis_size(axis)
    return lax.ppermute(own, axis, [(i, (i + by) % size) for i in range(size)])


def from_others(own, axis):
    return [shifted(own, axis, s) for s in range(1, lax.axis_size(axis))]


def rms_scale(values, scales):
    return values * lax.rsqrt(jnp.mean(values * values, axis=-1, keepdims=True) + norm_eps) * scales


def source_of(n):
    x_from = (lax.axis_index("x") + 4 - n % 4) % 4
    return x_from * 2 + (lax.axis_index("c") + n // 4) % 2


def prep_kernel(x_ref, gain_ref, ow_ref, rec_ref, key_ref, val_ref, send_ref, own_ref, normed_ref):
    for m, weight in enumerate((rec_ref, key_ref, val_ref)):
        own_ref[m * 32 : (m + 1) * 32, :] = weight[...]
    normed = rms_scale(x_ref[...].astype(f32), gain_ref[...]).astype(bf16)
    normed_ref[...] = normed
    nz, wide = send_ref.shape[0], send_ref.shape[2]
    seqs = normed.shape[0]
    width, half = wide // 2, seqs // 2
    at = lax.broadcasted_iota(jnp.int32, (width, width), 1)
    piece = at // 32
    x_from = (lax.axis_index("x") + 4 - piece % 4) % 4
    feature = (x_from * 2 + (lax.axis_index("c") + piece // 4) % 2) * 32 + at % 32
    order = (lax.broadcasted_iota(jnp.int32, (width, width), 0) == feature).astype(f32).astype(bf16)
    slices = jnp.concatenate([normed[:, z * width : (z + 1) * width] for z in range(nz)], axis=0)
    slices = dot(slices, order)
    for z in range(nz):
        send_ref[z, 0:half, 0:width] = slices[z * seqs : z * seqs + half].astype(bf16)
        send_ref[z, 0:half, width:wide] = slices[z * seqs + half : (z + 1) * seqs].astype(bf16)
        send_ref[z, half:, :] = ow_ref[...]


def rates_kernel(normed_ref, dd_ref, du_ref, db_ref, rd_ref, ru_ref, rb_ref, route_ref, gate_ref,
                 decay_ref, rate_ref, table_ref, mixing_ref):
    normed = normed_ref[...]
    decay_hidden = jnp.tanh(dot_t(normed, dd_ref[...])).astype(bf16)
    rate_hidden = dot_t(normed, rd_ref[...]).astype(bf16)
    decay_pre = db_ref[...] + dot(decay_hidden, du_ref[...])
    decay_ref[...] = jnp.exp(-math.exp(-0.5) * jax.nn.sigmoid(decay_pre))
    rate_ref[...] = jax.nn.sigmoid(rb_ref[...] + dot(rate_hidden, ru_ref[...]))

    seqs = normed.shape[0]
    top_count = route_ref.shape[0]
    slots = table_ref.shape[0]
    square = (seqs, seqs)
    row, col = (lax.broadcasted_iota(jnp.int32, square, d) for d in (0, 1))
    own, earlier = row == col, col < row

    def total(where, values, dim):
        return jnp.sum(jnp.where(where, values, 0.0), axis=dim, keepdims=True)

    along = [jnp.broadcast_to(route_ref[k : k + 1, :].astype(f32), square) for k in range(top_count)]
    down = [total(own, a, 1) for a in along]
    slot_of_row = lax.broadcasted_iota(jnp.int32, (slots, seqs), 0).astype(f32)
    slot_of_lane = lax.broadcasted_iota(jnp.int32, (seqs, slots), 1).astype(f32)
    table = jnp.zeros((slots, seqs), f32)
    mixing = jnp.zeros((seqs, slots), f32)
    for k in range(top_count):
        slot = down[k] * CAPACITY
        for other in along:
            slot = slot + total(earlier & (other == down[k]), 1.0, 1)
        table = table + (slot_of_row == total(own, slot, 0)).astype(f32)
        gate = total(own, jnp.broadcast_to(gate_ref[k : k + 1, :], square), 1)
        mixing = mixing + jnp.where(slot_of_lane == slot, gate, 0.0)
    table_ref[...] = table.astype(bf16)
    high = mixing.astype(bf16)
    mixing_ref[0:seqs, :] = high
    mixing_ref[seqs:, :] = (mixing - high.astype(f32)).astype(bf16)


def proj_kernel(recv_ref, *refs):
    pieces, (out_ref, tok_ref) = refs[:8], refs[8:]
    nz, seqs, width = recv_ref.shape[0], out_ref.shape[1], recv_ref.shape[2] // 2
    half = seqs // 2
    for z in range(nz):
        tok_ref[z, 0:half, :] = recv_ref[z, 0:half, 0:width].astype(f32)
        tok_ref[z, half:, :] = recv_ref[z, 0:half, width:].astype(f32)
    tokens = tok_ref[...].reshape(nz * seqs, width).astype(bf16)
    for m in range(3):
        weight = jnp.concatenate([piece[m * 32 : (m + 1) * 32, :] for piece in pieces], axis=0)
        part = dot(tokens, weight).astype(bf16)
        out_ref[:, :, m * 512 : (m + 1) * 512] = part.reshape(nz, seqs, 512)


def paired(a):
    return jnp.concatenate([a, a], axis=-1)


def state_kernel(parts_ref, decay_ref, rate_ref, scale_ref, gain_ref, state_ref, normed_ref, new_ref,
                 s_ref, p_ref, a_ref, v_ref, head_ref, in_sem):
    rows_total = state_ref.shape[0]
    chunk = 32
    chunks = rows_total // chunk
    blocks = state_ref.shape[1] // LANES
    heads = scale_ref.shape[1] // HEAD_DIM
    seqs = rows_total // heads

    def fetch(c):
        span = pl.ds(c * chunk, chunk)
        return pltpu.make_async_copy(state_ref.at[span, :], s_ref.at[span, :], in_sem.at[c])

    for c in range(chunks):
        fetch(c).start()

    total = parts_ref[0].astype(f32)
    for n in range(1, parts_ref.shape[0]):
        total = total + parts_ref[n].astype(f32)
    total = total.astype(bf16).astype(f32)
    local = heads * HEAD_DIM

    def by_head(slot, wide):
        for h in range(heads):
            head_ref[slot, pl.ds(h, seqs, stride=heads), :] = paired(wide[:, h * HEAD_DIM : (h + 1) * HEAD_DIM])

    def per_head(slot, gain_ref):
        by_head(slot, jnp.broadcast_to(gain_ref[...], (seqs, local)))
        return head_ref[slot]

    by_head(0, total[:, 0:local])
    by_head(1, total[:, local : 2 * local])
    by_head(2, total[:, 2 * local : 3 * local])
    by_head(3, decay_ref[...])
    by_head(4, rate_ref[...])
    keys = head_ref[1]
    rates = head_ref[4]
    scaled = keys * per_head(5, scale_ref)
    squares = jnp.sum((scaled * scaled)[:, 0:HEAD_DIM], axis=-1, keepdims=True)
    unit = scaled * lax.rsqrt(squares + norm_eps)
    head_ref[1] = unit
    head_ref[4] = unit * rates
    head_ref[5] = keys * rates

    def iota(shape, dim):
        return lax.broadcasted_iota(jnp.int32, shape, dim)

    square = (LANES, LANES)
    half_in = iota(square, 0) // HEAD_DIM
    spread = (half_in == iota(square, 1) // HEAD_DIM).astype(f32).astype(bf16)
    gathered = (half_in == iota(square, 1) % 2).astype(f32).astype(bf16)
    widen = (iota(square, 0) % 2 == iota(square, 1) // HEAD_DIM).astype(f32).astype(bf16)
    pair_of_lane = iota((chunk, LANES), 1) // 2

    def keep(k, values):
        p_ref[k * chunk : (k + 1) * chunk, :] = values.astype(bf16)

    for c in range(chunks):
        rows = pl.ds(c * chunk, chunk)
        fetch(c).wait()
        unit_c = head_ref[1, rows, :]
        val_c = head_ref[2, rows, :]
        for k in range(blocks):
            keep(k, s_ref[rows, k * LANES : (k + 1) * LANES] * unit_c)
            v_ref[k * chunk : (k + 1) * chunk, :] = jnp.where(pair_of_lane == k, val_c, 0.0).astype(bf16)
        a_ref[0] = dot(p_ref[...], spread)
        a_ref[1] = dot(v_ref[...], widen)
        rec_c = head_ref[0, rows, :]
        dec_c = head_ref[3, rows, :]
        corr_c = head_ref[4, rows, :]
        add_c = head_ref[5, rows, :]
        for k in range(blocks):
            lanes = slice(k * LANES, (k + 1) * LANES)
            here = slice(k * chunk, (k + 1) * chunk)
            new = s_ref[rows, lanes] * dec_c - a_ref[0, here, :] * corr_c + a_ref[1, here, :] * add_c
            new_ref[rows, lanes] = new
            keep(k, new * rec_c)
        a_ref[0] = dot(p_ref[...], gathered)
        read = jnp.zeros((chunk, LANES), f32)
        for k in range(blocks):
            read = jnp.where(pair_of_lane == k, a_ref[0, k * chunk : (k + 1) * chunk, :], read)
        head_ref[2, rows, :] = read

    read = head_ref[2][:, 0:HEAD_DIM]
    centred = read - jnp.mean(read, axis=-1, keepdims=True)
    normed = centred * lax.rsqrt(jnp.mean(centred * centred, axis=-1, keepdims=True) + group_eps)
    head_ref[2] = paired(normed) * per_head(5, gain_ref)
    for h in range(0, heads, 2):
        low = head_ref[2, pl.ds(h, seqs, stride=heads), :]
        high = head_ref[2, pl.ds(h + 1, seqs, stride=heads), :]
        both = jnp.concatenate([low[:, 0:HEAD_DIM], high[:, 0:HEAD_DIM]], axis=-1).astype(bf16)
        normed_ref[:, h * HEAD_DIM : (h + 2) * HEAD_DIM] = both


def out_kernel(tok_ref, *refs):
    pieces, (out_ref, part_ref) = refs[:10], refs[10:]
    tokens = tok_ref[...]
    groups, cols, seqs = 8, 32, tokens.shape[0]
    for n, piece in enumerate(pieces):
        shift, first_z = ((0, 0), (1, 0), (3, 0), (2, 0), (2, groups // 2))[n % 5]
        first = source_of(shift + n // 5 * 4) * cols
        turned = dot_t(piece[...], tokens)
        for z in range(piece.shape[0] // cols):
            at = pl.multiple_of(first + (z + first_z) * groups * cols, cols)
            part_ref[pl.ds(at, cols), :] = turned[z * cols : (z + 1) * cols, :]
    same = (lax.broadcasted_iota(jnp.int32, (seqs, seqs), 0) == lax.broadcasted_iota(jnp.int32, (seqs, seqs), 1))
    out_ref[...] = dot_t(same.astype(f32).astype(bf16), part_ref[...].astype(bf16)).astype(bf16)


def sum_in_order(piece_refs, line_ref):
    count = len(piece_refs)
    for shift, piece in enumerate(piece_refs):
        line_ref[(lax.axis_index("y") + count - shift) % count] = piece[...].astype(f32)
    total = line_ref[0]
    for n in range(1, count):
        total = total + line_ref[n]
    return total


def mid_kernel(p0, p1, p2, p3, x_ref, post_ref, ffn_ref, table_ref, middle_ref, rows_ref, line_ref):
    mix_sum = sum_in_order((p0, p1, p2, p3), line_ref)
    middle = (x_ref[...].astype(f32) + rms_scale(mix_sum, post_ref[...])).astype(bf16)
    middle_ref[...] = middle
    ffn_in = rms_scale(middle.astype(f32), ffn_ref[...]).astype(bf16)
    rows_ref[...] = dot(table_ref[...], ffn_in).reshape(rows_ref.shape).astype(bf16)


def move_kernel(*refs):
    count = len(refs) // 2
    sem_ref = refs[2 * count]
    copies = [pltpu.make_async_copy(refs[n], refs[count + n], sem_ref.at[n]) for n in range(count)]
    for copy in copies:
        copy.start()
    for copy in copies:
        copy.wait()


def bring_on_chip(arrays, name):
    return pl.pallas_call(
        move_kernel,
        out_shape=[pltpu.VMEM(a.shape, a.dtype) for a in arrays],
        in_specs=[HBM] * len(arrays),
        out_specs=[ON_CHIP] * len(arrays),
        scratch_shapes=[pltpu.SemaphoreType.DMA((len(arrays),))],
        name=name,
        compiler_params=SMALL,
    )(*[off_chip(a) for a in arrays])


def combine_kernel(back_ref, mixing_ref, out_ref):
    rows = back_ref[...].astype(f32).reshape(-1, back_ref.shape[2]).astype(bf16)
    both = dot(mixing_ref[...], rows)
    seqs = out_ref.shape[0]
    out_ref[...] = (both[0:seqs] + both[seqs:]).astype(bf16)


def expert_kernel(rows_ref, gate_ref, up_ref, down_ref, out_ref):
    rows = rows_ref[...].astype(f32).reshape(-1, rows_ref.shape[2]).astype(bf16)
    gate_cut = jnp.minimum(dot(rows, gate_ref[0]), clamp_limit)
    up_cut = jnp.clip(dot(rows, up_ref[0]), -clamp_limit, clamp_limit)
    hidden = ((up_cut + 1.0) * gate_cut * jax.nn.sigmoid(gate_alpha * gate_cut)).astype(bf16)
    out_ref[...] = dot(hidden, down_ref[0]).reshape(out_ref.shape).astype(bf16)


def last_kernel(p0, p1, p2, p3, middle_ref, gain_ref, out_ref, line_ref):
    moe_sum = sum_in_order((p0, p1, p2, p3), line_ref)
    out_ref[...] = (middle_ref[...].astype(f32) + rms_scale(moe_sum, gain_ref[...])).astype(bf16)


def local(
    layer_in,
    state_in,
    mix_gain,
    rec_weight,
    key_weight,
    val_weight,
    decay_down,
    decay_up,
    decay_base,
    rate_down,
    rate_up,
    rate_base,
    key_scale,
    group_gain,
    out_weight,
    post_gain,
    ffn_gain,
    routes,
    route_gates,
    expert_gate,
    expert_up,
    expert_down,
    out_gain,
):
    seqs, width = layer_in.shape
    heads = state_in.shape[1]
    local_cols = heads * HEAD_DIM
    nz, nx, nc, ny = (lax.axis_size(a) for a in ("z", "x", "c", "y"))
    nxc = nx * nc
    share = width // nz
    expert_total = nz * nxc
    slot_total = expert_total * CAPACITY
    shape = jax.ShapeDtypeStruct

    send, own, normed = pl.pallas_call(
        prep_kernel,
        out_shape=(
            pltpu.VMEM((nz, seqs // 2 + out_weight.shape[1], 2 * share), bf16),
            pltpu.VMEM((3 * rec_weight.shape[0], local_cols), bf16),
            pltpu.VMEM((seqs, width), bf16),
        ),
        name="prep",
    )(layer_in, mix_gain[None], out_weight.T, rec_weight, key_weight, val_weight)
    recv = lax.all_to_all(send, "z", split_axis=0, concat_axis=0, tiled=True)
    along_x = [own] + from_others(own, "x")
    pieces = along_x + [p for q in along_x for p in from_others(q, "c")]
    ow_own = recv[:, seqs // 2 :, :].reshape(nz * out_weight.shape[1], local_cols)
    ow_next, ow_last = shifted(ow_own, "x", 1), shifted(ow_own, "x", -1)
    decay_factor, learn_rate, dispatch_table, mixing = pl.pallas_call(
        rates_kernel,
        out_shape=(
            pltpu.VMEM((seqs, local_cols), f32),
            pltpu.VMEM((seqs, local_cols), f32),
            pltpu.VMEM((slot_total, seqs), bf16),
            pltpu.VMEM((2 * seqs, slot_total), bf16),
        ),
        name="rates",
        compiler_params=SMALL,
    )(
        on_chip(normed),
        off_chip(decay_down.T),
        off_chip(decay_up),
        off_chip(decay_base[None]),
        off_chip(rate_down.T),
        off_chip(rate_up),
        off_chip(rate_base[None]),
        off_chip(routes.T),
        off_chip(route_gates.T),
    )

    ow_next, ow_last, decay_factor = lax.optimization_barrier((ow_next, ow_last, decay_factor))
    half = ow_own.shape[0] // 2
    ow_low, ow_high = shifted(ow_last[:half], "x", -1), shifted(ow_next[half:], "x", 1)

    part = pl.pallas_call(
        proj_kernel,
        out_shape=pltpu.VMEM((nz, seqs, 3 * local_cols), bf16),
        in_specs=[ON_CHIP] * 9,
        scratch_shapes=[
            pltpu.VMEM((nz, seqs, share), f32),
        ],
        name="proj",
        compiler_params=SMALL,
    )(on_chip(recv), *[on_chip(p) for p in pieces])
    parts = lax.all_to_all(part, "z", split_axis=0, concat_axis=0, tiled=True)

    rows = seqs * heads
    lanes_total = state_in.shape[2]
    normed_out, new_state = pl.pallas_call(
        state_kernel,
        out_shape=(pltpu.VMEM((seqs, local_cols), bf16), pltpu.VMEM((rows, lanes_total), f32)),
        in_specs=[ON_CHIP] * 5 + [HBM],
        out_specs=(ON_CHIP, ON_CHIP),
        scratch_shapes=[
            pltpu.VMEM((rows, lanes_total), f32),
            pltpu.VMEM((32 * (lanes_total // LANES), LANES), bf16),
            pltpu.VMEM((2, 32 * (lanes_total // LANES), LANES), f32),
            pltpu.VMEM((32 * (lanes_total // LANES), LANES), bf16),
            pltpu.VMEM((6, rows, LANES), f32),
            pltpu.SemaphoreType.DMA((rows // 32,)),
        ],
        name="state",
        compiler_params=SMALL,
    )(
        on_chip(parts),
        on_chip(decay_factor),
        on_chip(learn_rate),
        off_chip(key_scale[None]),
        off_chip(group_gain[None]),
        off_chip(state_in.reshape(rows, lanes_total)),
    )
    normed_out, ow_low, ow_high, down = lax.optimization_barrier((normed_out, ow_low, ow_high, expert_down))
    (down,) = bring_on_chip([down], "fetch_down")
    ow_pieces = [ow_own, ow_next, ow_last, ow_low, ow_high]
    ow_pieces = ow_pieces + [shifted(p, "c", 1) for p in ow_pieces]
    normed_out, down = lax.optimization_barrier((normed_out, down))
    mix_part = pl.pallas_call(
        out_kernel,
        out_shape=pltpu.VMEM((seqs, width), bf16),
        in_specs=[ON_CHIP] * 11,
        scratch_shapes=[pltpu.VMEM((width, seqs), f32)],
        name="outproj",
        compiler_params=SMALL,
    )(on_chip(normed_out), *[on_chip(p) for p in ow_pieces])
    mix_part, *weights = lax.optimization_barrier((mix_part, expert_gate, expert_up))
    mix_parts = [mix_part] + from_others(mix_part, "y")
    weights = bring_on_chip(weights, "fetch")
    dispatch_table, *weights = lax.optimization_barrier((dispatch_table, *weights))

    middle, send_rows = pl.pallas_call(
        mid_kernel,
        out_shape=(pltpu.VMEM((seqs, width), bf16), pltpu.VMEM((expert_total, CAPACITY, width), bf16)),
        in_specs=[ON_CHIP] * 8,
        scratch_shapes=[pltpu.VMEM((ny, seqs, width), f32)],
        name="mid",
        compiler_params=SMALL,
    )(
        *[on_chip(p) for p in mix_parts],
        layer_in,
        post_gain[None],
        ffn_gain[None],
        on_chip(dispatch_table),
    )

    arrived = lax.all_to_all(send_rows, EP, split_axis=0, concat_axis=0, tiled=True)
    partial_value = pl.pallas_call(
        expert_kernel,
        out_shape=pltpu.VMEM((expert_total, CAPACITY, width), bf16),
        in_specs=[ON_CHIP] * 4,
        name="expert",
        compiler_params=SMALL,
    )(on_chip(arrived), *[on_chip(w) for w in weights], on_chip(down))
    back_rows = lax.all_to_all(partial_value, EP, split_axis=0, concat_axis=0, tiled=True)
    moe_part = pl.pallas_call(
        combine_kernel,
        out_shape=pltpu.VMEM((seqs, width), bf16),
        in_specs=[ON_CHIP] * 2,
        name="combine",
        compiler_params=SMALL,
    )(on_chip(back_rows), on_chip(mixing))
    moe_part, new_state = lax.optimization_barrier((moe_part, new_state))
    new_state = pl.pallas_call(
        move_kernel,
        out_shape=pltpu.HBM((rows, lanes_total), f32),
        in_specs=[ON_CHIP],
        out_specs=HBM,
        scratch_shapes=[pltpu.SemaphoreType.DMA((1,))],
        name="store",
        compiler_params=SMALL,
    )(on_chip(new_state))
    layer_out = pl.pallas_call(
        last_kernel,
        out_shape=shape((seqs, width), bf16),
        in_specs=[ON_CHIP] * 6,
        scratch_shapes=[pltpu.VMEM((ny, seqs, width), f32)],
        name="last",
        compiler_params=SMALL,
    )(
        *[on_chip(p) for p in [moe_part] + from_others(moe_part, "y")],
        on_chip(middle),
        out_gain[None],
    )
    return layer_out, new_state.reshape(seqs, heads, lanes_total)


def solution(mesh):
    mesh = Mesh(mesh.devices.reshape(8, 4, 2, 4), ("z", "x", "c", "y"))
    in_specs = (
        P(EP, None),
        P(EP, "y", None),
        P(),
        P(EP, "y"),
        P(EP, "y"),
        P(EP, "y"),
        P(),
        P(None, "y"),
        P("y"),
        P(),
        P(None, "y"),
        P("y"),
        P("y"),
        P("y"),
        P("y", EP),
        P(),
        P(),
        P(EP, None),
        P(EP, None),
        P(EP, None, "y"),
        P(EP, None, "y"),
        P(EP, "y", None),
        P(),
    )
    out_specs = (P(EP, None), P(EP, "y", None))
    return jax.shard_map(local, mesh=mesh, in_specs=in_specs, out_specs=out_specs, check_vma=False)
```

```python
import math

import jax
import jax.numpy as jnp
from jax import lax
from jax.experimental import pallas as pl
from jax.experimental.pallas import tpu as pltpu
from jax.sharding import Mesh
from jax.sharding import PartitionSpec as P

HEAD_DIM = 64
CAPACITY = 2
LANES = 128
norm_eps = 1e-06
group_eps = 0.00064
clamp_limit = 7.0
gate_alpha = 1.702
f32 = jnp.float32
bf16 = jnp.bfloat16


EP = ("z", "x", "c")
HBM = pl.BlockSpec(memory_space=pl.ANY)
SMALL = pltpu.CompilerParams(vmem_limit_bytes=12 * 2**20)
ON_CHIP = pl.BlockSpec(memory_space=pltpu.VMEM)


def dot(a, b):
    return jnp.dot(a, b, preferred_element_type=f32)


def dot_t(a, b):
    return lax.dot_general(a, b, (((1,), (1,)), ((), ())), preferred_element_type=f32)


def on_chip(a):
    return pltpu.with_memory_space_constraint(a, pltpu.VMEM)


def off_chip(a):
    return pltpu.with_memory_space_constraint(a, pltpu.HBM)


def shifted(own, axis, by):
    size = lax.axis_size(axis)
    return lax.ppermute(own, axis, [(i, (i + by) % size) for i in range(size)])


def from_others(own, axis):
    return [shifted(own, axis, s) for s in range(1, lax.axis_size(axis))]


def rms_scale(values, scales):
    return values * lax.rsqrt(jnp.mean(values * values, axis=-1, keepdims=True) + norm_eps) * scales


def source_of(n):
    x_from = (lax.axis_index("x") + 4 - n % 4) % 4
    return x_from * 2 + (lax.axis_index("c") + n // 4) % 2


def prep_kernel(x_ref, gain_ref, ow_ref, rec_ref, key_ref, val_ref, send_ref, own_ref, normed_ref):
    for m, weight in enumerate((rec_ref, key_ref, val_ref)):
        own_ref[m * 32 : (m + 1) * 32, :] = weight[...]
    normed = rms_scale(x_ref[...].astype(f32), gain_ref[...]).astype(bf16)
    normed_ref[...] = normed
    nz, wide = send_ref.shape[0], send_ref.shape[2]
    seqs = normed.shape[0]
    width, half = wide // 2, seqs // 2
    at = lax.broadcasted_iota(jnp.int32, (width, width), 1)
    piece = at // 32
    x_from = (lax.axis_index("x") + 4 - piece % 4) % 4
    feature = (x_from * 2 + (lax.axis_index("c") + piece // 4) % 2) * 32 + at % 32
    order = (lax.broadcasted_iota(jnp.int32, (width, width), 0) == feature).astype(f32).astype(bf16)
    slices = jnp.concatenate([normed[:, z * width : (z + 1) * width] for z in range(nz)], axis=0)
    slices = dot(slices, order)
    for z in range(nz):
        send_ref[z, 0:half, 0:width] = slices[z * seqs : z * seqs + half].astype(bf16)
        send_ref[z, 0:half, width:wide] = slices[z * seqs + half : (z + 1) * seqs].astype(bf16)
        send_ref[z, half:, :] = ow_ref[...]


def rates_kernel(normed_ref, dd_ref, du_ref, db_ref, rd_ref, ru_ref, rb_ref, route_ref, gate_ref,
                 decay_ref, rate_ref, table_ref, mixing_ref):
    normed = normed_ref[...]
    decay_hidden = jnp.tanh(dot_t(normed, dd_ref[...])).astype(bf16)
    rate_hidden = dot_t(normed, rd_ref[...]).astype(bf16)
    decay_pre = db_ref[...] + dot(decay_hidden, du_ref[...])
    decay_ref[...] = jnp.exp(-math.exp(-0.5) * jax.nn.sigmoid(decay_pre))
    rate_ref[...] = jax.nn.sigmoid(rb_ref[...] + dot(rate_hidden, ru_ref[...]))

    seqs = normed.shape[0]
    top_count = route_ref.shape[0]
    slots = table_ref.shape[0]
    square = (seqs, seqs)
    row, col = (lax.broadcasted_iota(jnp.int32, square, d) for d in (0, 1))
    own, earlier = row == col, col < row

    def total(where, values, dim):
        return jnp.sum(jnp.where(where, values, 0.0), axis=dim, keepdims=True)

    along = [jnp.broadcast_to(route_ref[k : k + 1, :].astype(f32), square) for k in range(top_count)]
    down = [total(own, a, 1) for a in along]
    slot_of_row = lax.broadcasted_iota(jnp.int32, (slots, seqs), 0).astype(f32)
    slot_of_lane = lax.broadcasted_iota(jnp.int32, (seqs, slots), 1).astype(f32)
    table = jnp.zeros((slots, seqs), f32)
    mixing = jnp.zeros((seqs, slots), f32)
    for k in range(top_count):
        slot = down[k] * CAPACITY
        for other in along:
            slot = slot + total(earlier & (other == down[k]), 1.0, 1)
        table = table + (slot_of_row == total(own, slot, 0)).astype(f32)
        gate = total(own, jnp.broadcast_to(gate_ref[k : k + 1, :], square), 1)
        mixing = mixing + jnp.where(slot_of_lane == slot, gate, 0.0)
    table_ref[...] = table.astype(bf16)
    high = mixing.astype(bf16)
    mixing_ref[0:seqs, :] = high
    mixing_ref[seqs:, :] = (mixing - high.astype(f32)).astype(bf16)


def proj_kernel(recv_ref, *refs):
    pieces, (out_ref, tok_ref) = refs[:8], refs[8:]
    nz, seqs, width = recv_ref.shape[0], out_ref.shape[1], recv_ref.shape[2] // 2
    half = seqs // 2
    for z in range(nz):
        tok_ref[z, 0:half, :] = recv_ref[z, 0:half, 0:width].astype(f32)
        tok_ref[z, half:, :] = recv_ref[z, 0:half, width:].astype(f32)
    tokens = tok_ref[...].reshape(nz * seqs, width).astype(bf16)
    for m in range(3):
        weight = jnp.concatenate([piece[m * 32 : (m + 1) * 32, :] for piece in pieces], axis=0)
        part = dot(tokens, weight).astype(bf16)
        out_ref[:, :, m * 512 : (m + 1) * 512] = part.reshape(nz, seqs, 512)


def paired(a):
    return jnp.concatenate([a, a], axis=-1)


def state_kernel(parts_ref, decay_ref, rate_ref, scale_ref, gain_ref, state_ref, normed_ref, new_ref,
                 s_ref, p_ref, a_ref, v_ref, head_ref, in_sem):
    rows_total = state_ref.shape[0]
    chunk = 32
    chunks = rows_total // chunk
    blocks = state_ref.shape[1] // LANES
    heads = scale_ref.shape[1] // HEAD_DIM
    seqs = rows_total // heads

    def fetch(c):
        span = pl.ds(c * chunk, chunk)
        return pltpu.make_async_copy(state_ref.at[span, :], s_ref.at[span, :], in_sem.at[c])

    for c in range(chunks):
        fetch(c).start()

    total = parts_ref[0].astype(f32)
    for n in range(1, parts_ref.shape[0]):
        total = total + parts_ref[n].astype(f32)
    total = total.astype(bf16).astype(f32)
    local = heads * HEAD_DIM

    def by_head(slot, wide):
        for h in range(heads):
            head_ref[slot, pl.ds(h, seqs, stride=heads), :] = paired(wide[:, h * HEAD_DIM : (h + 1) * HEAD_DIM])

    def per_head(slot, gain_ref):
        by_head(slot, jnp.broadcast_to(gain_ref[...], (seqs, local)))
        return head_ref[slot]

    by_head(0, total[:, 0:local])
    by_head(1, total[:, local : 2 * local])
    by_head(2, total[:, 2 * local : 3 * local])
    by_head(3, decay_ref[...])
    by_head(4, rate_ref[...])
    keys = head_ref[1]
    rates = head_ref[4]
    scaled = keys * per_head(5, scale_ref)
    squares = jnp.sum((scaled * scaled)[:, 0:HEAD_DIM], axis=-1, keepdims=True)
    unit = scaled * lax.rsqrt(squares + norm_eps)
    head_ref[1] = unit
    head_ref[4] = unit * rates
    head_ref[5] = keys * rates

    def iota(shape, dim):
        return lax.broadcasted_iota(jnp.int32, shape, dim)

    square = (LANES, LANES)
    half_in = iota(square, 0) // HEAD_DIM
    spread = (half_in == iota(square, 1) // HEAD_DIM).astype(f32).astype(bf16)
    gathered = (half_in == iota(square, 1) % 2).astype(f32).astype(bf16)
    widen = (iota(square, 0) % 2 == iota(square, 1) // HEAD_DIM).astype(f32).astype(bf16)
    pair_of_lane = iota((chunk, LANES), 1) // 2

    def keep(k, values):
        p_ref[k * chunk : (k + 1) * chunk, :] = values.astype(bf16)

    for c in range(chunks):
        rows = pl.ds(c * chunk, chunk)
        fetch(c).wait()
        unit_c = head_ref[1, rows, :]
        val_c = head_ref[2, rows, :]
        for k in range(blocks):
            keep(k, s_ref[rows, k * LANES : (k + 1) * LANES] * unit_c)
            v_ref[k * chunk : (k + 1) * chunk, :] = jnp.where(pair_of_lane == k, val_c, 0.0).astype(bf16)
        a_ref[0] = dot(p_ref[...], spread)
        a_ref[1] = dot(v_ref[...], widen)
        rec_c = head_ref[0, rows, :]
        dec_c = head_ref[3, rows, :]
        corr_c = head_ref[4, rows, :]
        add_c = head_ref[5, rows, :]
        for k in range(blocks):
            lanes = slice(k * LANES, (k + 1) * LANES)
            here = slice(k * chunk, (k + 1) * chunk)
            new = s_ref[rows, lanes] * dec_c - a_ref[0, here, :] * corr_c + a_ref[1, here, :] * add_c
            new_ref[rows, lanes] = new
            keep(k, new * rec_c)
        a_ref[0] = dot(p_ref[...], gathered)
        read = jnp.zeros((chunk, LANES), f32)
        for k in range(blocks):
            read = jnp.where(pair_of_lane == k, a_ref[0, k * chunk : (k + 1) * chunk, :], read)
        head_ref[2, rows, :] = read

    read = head_ref[2][:, 0:HEAD_DIM]
    centred = read - jnp.mean(read, axis=-1, keepdims=True)
    normed = centred * lax.rsqrt(jnp.mean(centred * centred, axis=-1, keepdims=True) + group_eps)
    head_ref[2] = paired(normed) * per_head(5, gain_ref)
    for h in range(0, heads, 2):
        low = head_ref[2, pl.ds(h, seqs, stride=heads), :]
        high = head_ref[2, pl.ds(h + 1, seqs, stride=heads), :]
        both = jnp.concatenate([low[:, 0:HEAD_DIM], high[:, 0:HEAD_DIM]], axis=-1).astype(bf16)
        normed_ref[:, h * HEAD_DIM : (h + 2) * HEAD_DIM] = both


def out_kernel(tok_ref, *refs):
    pieces, (out_ref, part_ref) = refs[:8], refs[8:]
    tokens = tok_ref[...]
    groups, cols, seqs = 8, 32, tokens.shape[0]
    for n, piece in enumerate(pieces):
        first = source_of(n) * cols
        turned = dot_t(piece[...], tokens)
        for z in range(groups):
            at = pl.multiple_of(first + z * groups * cols, cols)
            part_ref[pl.ds(at, cols), :] = turned[z * cols : (z + 1) * cols, :]
    same = (lax.broadcasted_iota(jnp.int32, (seqs, seqs), 0) == lax.broadcasted_iota(jnp.int32, (seqs, seqs), 1))
    out_ref[...] = dot_t(same.astype(f32).astype(bf16), part_ref[...].astype(bf16)).astype(bf16)


def sum_in_order(piece_refs, line_ref):
    count = len(piece_refs)
    for shift, piece in enumerate(piece_refs):
        line_ref[(lax.axis_index("y") + count - shift) % count] = piece[...].astype(f32)
    total = line_ref[0]
    for n in range(1, count):
        total = total + line_ref[n]
    return total


def mid_kernel(p0, p1, p2, p3, x_ref, post_ref, ffn_ref, table_ref, middle_ref, rows_ref, line_ref):
    mix_sum = sum_in_order((p0, p1, p2, p3), line_ref)
    middle = (x_ref[...].astype(f32) + rms_scale(mix_sum, post_ref[...])).astype(bf16)
    middle_ref[...] = middle
    ffn_in = rms_scale(middle.astype(f32), ffn_ref[...]).astype(bf16)
    rows_ref[...] = dot(table_ref[...], ffn_in).reshape(rows_ref.shape).astype(bf16)


def move_kernel(*refs):
    count = len(refs) // 2
    sem_ref = refs[2 * count]
    copies = [pltpu.make_async_copy(refs[n], refs[count + n], sem_ref.at[n]) for n in range(count)]
    for copy in copies:
        copy.start()
    for copy in copies:
        copy.wait()


def bring_on_chip(arrays, name):
    return pl.pallas_call(
        move_kernel,
        out_shape=[pltpu.VMEM(a.shape, a.dtype) for a in arrays],
        in_specs=[HBM] * len(arrays),
        out_specs=[ON_CHIP] * len(arrays),
        scratch_shapes=[pltpu.SemaphoreType.DMA((len(arrays),))],
        name=name,
        compiler_params=SMALL,
    )(*[off_chip(a) for a in arrays])


def combine_kernel(back_ref, mixing_ref, out_ref):
    rows = back_ref[...].astype(f32).reshape(-1, back_ref.shape[2]).astype(bf16)
    both = dot(mixing_ref[...], rows)
    seqs = out_ref.shape[0]
    out_ref[...] = (both[0:seqs] + both[seqs:]).astype(bf16)


def expert_kernel(rows_ref, gate_ref, up_ref, down_ref, out_ref):
    rows = rows_ref[...].astype(f32).reshape(-1, rows_ref.shape[2]).astype(bf16)
    gate_cut = jnp.minimum(dot(rows, gate_ref[0]), clamp_limit)
    up_cut = jnp.clip(dot(rows, up_ref[0]), -clamp_limit, clamp_limit)
    hidden = ((up_cut + 1.0) * gate_cut * jax.nn.sigmoid(gate_alpha * gate_cut)).astype(bf16)
    out_ref[...] = dot(hidden, down_ref[0]).reshape(out_ref.shape).astype(bf16)


def last_kernel(p0, p1, p2, p3, middle_ref, gain_ref, out_ref, line_ref):
    moe_sum = sum_in_order((p0, p1, p2, p3), line_ref)
    out_ref[...] = (middle_ref[...].astype(f32) + rms_scale(moe_sum, gain_ref[...])).astype(bf16)


def local(
    layer_in,
    state_in,
    mix_gain,
    rec_weight,
    key_weight,
    val_weight,
    decay_down,
    decay_up,
    decay_base,
    rate_down,
    rate_up,
    rate_base,
    key_scale,
    group_gain,
    out_weight,
    post_gain,
    ffn_gain,
    routes,
    route_gates,
    expert_gate,
    expert_up,
    expert_down,
    out_gain,
):
    seqs, width = layer_in.shape
    heads = state_in.shape[1]
    local_cols = heads * HEAD_DIM
    nz, nx, nc, ny = (lax.axis_size(a) for a in ("z", "x", "c", "y"))
    nxc = nx * nc
    share = width // nz
    expert_total = nz * nxc
    slot_total = expert_total * CAPACITY
    shape = jax.ShapeDtypeStruct

    send, own, normed = pl.pallas_call(
        prep_kernel,
        out_shape=(
            pltpu.VMEM((nz, seqs // 2 + out_weight.shape[1], 2 * share), bf16),
            pltpu.VMEM((3 * rec_weight.shape[0], local_cols), bf16),
            pltpu.VMEM((seqs, width), bf16),
        ),
        name="prep",
    )(layer_in, mix_gain[None], out_weight.T, rec_weight, key_weight, val_weight)
    recv = lax.all_to_all(send, "z", split_axis=0, concat_axis=0, tiled=True)
    along_x = [own] + from_others(own, "x")
    pieces = along_x + [p for q in along_x for p in from_others(q, "c")]
    ow_own = recv[:, seqs // 2 :, :].reshape(nz * out_weight.shape[1], local_cols)
    ow_far = from_others(ow_own, "x")
    decay_factor, learn_rate, dispatch_table, mixing = pl.pallas_call(
        rates_kernel,
        out_shape=(
            pltpu.VMEM((seqs, local_cols), f32),
            pltpu.VMEM((seqs, local_cols), f32),
            pltpu.VMEM((slot_total, seqs), bf16),
            pltpu.VMEM((2 * seqs, slot_total), bf16),
        ),
        name="rates",
        compiler_params=SMALL,
    )(
        on_chip(normed),
        off_chip(decay_down.T),
        off_chip(decay_up),
        off_chip(decay_base[None]),
        off_chip(rate_down.T),
        off_chip(rate_up),
        off_chip(rate_base[None]),
        off_chip(routes.T),
        off_chip(route_gates.T),
    )

    part = pl.pallas_call(
        proj_kernel,
        out_shape=pltpu.VMEM((nz, seqs, 3 * local_cols), bf16),
        in_specs=[ON_CHIP] * 9,
        scratch_shapes=[
            pltpu.VMEM((nz, seqs, share), f32),
        ],
        name="proj",
        compiler_params=SMALL,
    )(on_chip(recv), *[on_chip(p) for p in pieces])
    parts = lax.all_to_all(part, "z", split_axis=0, concat_axis=0, tiled=True)

    rows = seqs * heads
    lanes_total = state_in.shape[2]
    normed_out, new_state = pl.pallas_call(
        state_kernel,
        out_shape=(pltpu.VMEM((seqs, local_cols), bf16), pltpu.VMEM((rows, lanes_total), f32)),
        in_specs=[ON_CHIP] * 5 + [HBM],
        out_specs=(ON_CHIP, ON_CHIP),
        scratch_shapes=[
            pltpu.VMEM((rows, lanes_total), f32),
            pltpu.VMEM((32 * (lanes_total // LANES), LANES), bf16),
            pltpu.VMEM((2, 32 * (lanes_total // LANES), LANES), f32),
            pltpu.VMEM((32 * (lanes_total // LANES), LANES), bf16),
            pltpu.VMEM((6, rows, LANES), f32),
            pltpu.SemaphoreType.DMA((rows // 32,)),
        ],
        name="state",
        compiler_params=SMALL,
    )(
        on_chip(parts),
        on_chip(decay_factor),
        on_chip(learn_rate),
        off_chip(key_scale[None]),
        off_chip(group_gain[None]),
        off_chip(state_in.reshape(rows, lanes_total)),
    )
    ow_own_other = shifted(ow_own, "c", 1)
    normed_out, down, *ow_far = lax.optimization_barrier((normed_out, expert_down, *ow_far))
    (down,) = bring_on_chip([down], "fetch_down")
    ow_pieces = [ow_own, *ow_far, ow_own_other] + [shifted(p, "c", 1) for p in ow_far]
    normed_out, down = lax.optimization_barrier((normed_out, down))
    mix_part = pl.pallas_call(
        out_kernel,
        out_shape=pltpu.VMEM((seqs, width), bf16),
        in_specs=[ON_CHIP] * 9,
        scratch_shapes=[pltpu.VMEM((width, seqs), f32)],
        name="outproj",
        compiler_params=SMALL,
    )(on_chip(normed_out), *[on_chip(p) for p in ow_pieces])
    mix_part, *weights = lax.optimization_barrier((mix_part, expert_gate, expert_up))
    mix_parts = [mix_part] + from_others(mix_part, "y")
    weights = bring_on_chip(weights, "fetch")
    dispatch_table, *weights = lax.optimization_barrier((dispatch_table, *weights))

    middle, send_rows = pl.pallas_call(
        mid_kernel,
        out_shape=(pltpu.VMEM((seqs, width), bf16), pltpu.VMEM((expert_total, CAPACITY, width), bf16)),
        in_specs=[ON_CHIP] * 8,
        scratch_shapes=[pltpu.VMEM((ny, seqs, width), f32)],
        name="mid",
        compiler_params=SMALL,
    )(
        *[on_chip(p) for p in mix_parts],
        layer_in,
        post_gain[None],
        ffn_gain[None],
        on_chip(dispatch_table),
    )

    arrived = lax.all_to_all(send_rows, EP, split_axis=0, concat_axis=0, tiled=True)
    partial_value = pl.pallas_call(
        expert_kernel,
        out_shape=pltpu.VMEM((expert_total, CAPACITY, width), bf16),
        in_specs=[ON_CHIP] * 4,
        name="expert",
        compiler_params=SMALL,
    )(on_chip(arrived), *[on_chip(w) for w in weights], on_chip(down))
    back_rows = lax.all_to_all(partial_value, EP, split_axis=0, concat_axis=0, tiled=True)
    moe_part = pl.pallas_call(
        combine_kernel,
        out_shape=pltpu.VMEM((seqs, width), bf16),
        in_specs=[ON_CHIP] * 2,
        name="combine",
        compiler_params=SMALL,
    )(on_chip(back_rows), on_chip(mixing))
    moe_part, new_state = lax.optimization_barrier((moe_part, new_state))
    new_state = pl.pallas_call(
        move_kernel,
        out_shape=pltpu.HBM((rows, lanes_total), f32),
        in_specs=[ON_CHIP],
        out_specs=HBM,
        scratch_shapes=[pltpu.SemaphoreType.DMA((1,))],
        name="store",
        compiler_params=SMALL,
    )(on_chip(new_state))
    layer_out = pl.pallas_call(
        last_kernel,
        out_shape=shape((seqs, width), bf16),
        in_specs=[ON_CHIP] * 6,
        scratch_shapes=[pltpu.VMEM((ny, seqs, width), f32)],
        name="last",
        compiler_params=SMALL,
    )(
        *[on_chip(p) for p in [moe_part] + from_others(moe_part, "y")],
        on_chip(middle),
        out_gain[None],
    )
    return layer_out, new_state.reshape(seqs, heads, lanes_total)


def solution(mesh):
    mesh = Mesh(mesh.devices.reshape(8, 4, 2, 4), ("z", "x", "c", "y"))
    in_specs = (
        P(EP, None),
        P(EP, "y", None),
        P(),
        P(EP, "y"),
        P(EP, "y"),
        P(EP, "y"),
        P(),
        P(None, "y"),
        P("y"),
        P(),
        P(None, "y"),
        P("y"),
        P("y"),
        P("y"),
        P("y", EP),
        P(),
        P(),
        P(EP, None),
        P(EP, None),
        P(EP, None, "y"),
        P(EP, None, "y"),
        P(EP, "y", None),
        P(),
    )
    out_specs = (P(EP, None), P(EP, "y", None))
    return jax.shard_map(local, mesh=mesh, in_specs=in_specs, out_specs=out_specs, check_vma=False)
```

```python
import math

import jax
import jax.numpy as jnp
from jax import lax
from jax.experimental import pallas as pl
from jax.experimental.pallas import tpu as pltpu
from jax.sharding import Mesh
from jax.sharding import PartitionSpec as P

HEAD_DIM = 64
CAPACITY = 2
LANES = 128
norm_eps = 1e-06
group_eps = 0.00064
clamp_limit = 7.0
gate_alpha = 1.702
f32 = jnp.float32
bf16 = jnp.bfloat16


EP = ("z", "x", "c")
HBM = pl.BlockSpec(memory_space=pl.ANY)
SMALL = pltpu.CompilerParams(vmem_limit_bytes=12 * 2**20)
ON_CHIP = pl.BlockSpec(memory_space=pltpu.VMEM)


def dot(a, b):
    return jnp.dot(a, b, preferred_element_type=f32)


def dot_t(a, b):
    return lax.dot_general(a, b, (((1,), (1,)), ((), ())), preferred_element_type=f32)


def on_chip(a):
    return pltpu.with_memory_space_constraint(a, pltpu.VMEM)


def off_chip(a):
    return pltpu.with_memory_space_constraint(a, pltpu.HBM)


def shifted(own, axis, by):
    size = lax.axis_size(axis)
    return lax.ppermute(own, axis, [(i, (i + by) % size) for i in range(size)])


def from_others(own, axis):
    return [shifted(own, axis, s) for s in range(1, lax.axis_size(axis))]


def rms_scale(values, scales):
    return values * lax.rsqrt(jnp.mean(values * values, axis=-1, keepdims=True) + norm_eps) * scales


def source_of(n):
    x_from = (lax.axis_index("x") + 4 - n % 4) % 4
    return x_from * 2 + (lax.axis_index("c") + n // 4) % 2


def prep_kernel(x_ref, gain_ref, ow_ref, rec_ref, key_ref, val_ref, send_ref, own_ref, normed_ref):
    for m, weight in enumerate((rec_ref, key_ref, val_ref)):
        own_ref[m * 32 : (m + 1) * 32, :] = weight[...]
    normed = rms_scale(x_ref[...].astype(f32), gain_ref[...]).astype(bf16)
    normed_ref[...] = normed
    nz, wide = send_ref.shape[0], send_ref.shape[2]
    seqs = normed.shape[0]
    width, half = wide // 2, seqs // 2
    at = lax.broadcasted_iota(jnp.int32, (width, width), 1)
    piece = at // 32
    x_from = (lax.axis_index("x") + 4 - piece % 4) % 4
    feature = (x_from * 2 + (lax.axis_index("c") + piece // 4) % 2) * 32 + at % 32
    order = (lax.broadcasted_iota(jnp.int32, (width, width), 0) == feature).astype(f32).astype(bf16)
    slices = jnp.concatenate([normed[:, z * width : (z + 1) * width] for z in range(nz)], axis=0)
    slices = dot(slices, order)
    for z in range(nz):
        send_ref[z, 0:half, 0:width] = slices[z * seqs : z * seqs + half].astype(bf16)
        send_ref[z, 0:half, width:wide] = slices[z * seqs + half : (z + 1) * seqs].astype(bf16)
        send_ref[z, half:, :] = ow_ref[...]


def rates_kernel(normed_ref, dd_ref, du_ref, db_ref, rd_ref, ru_ref, rb_ref, route_ref, gate_ref, state_ref,
                 decay_ref, rate_ref, table_ref, mixing_ref, state_out, sem_ref):
    copy = pltpu.make_async_copy(state_ref.at[pl.ds(0, state_out.shape[0]), :], state_out, sem_ref.at[0])
    copy.start()
    normed = normed_ref[...]
    decay_hidden = jnp.tanh(dot_t(normed, dd_ref[...])).astype(bf16)
    rate_hidden = dot_t(normed, rd_ref[...]).astype(bf16)
    decay_pre = db_ref[...] + dot(decay_hidden, du_ref[...])
    decay_ref[...] = jnp.exp(-math.exp(-0.5) * jax.nn.sigmoid(decay_pre))
    rate_ref[...] = jax.nn.sigmoid(rb_ref[...] + dot(rate_hidden, ru_ref[...]))

    seqs = normed.shape[0]
    top_count = route_ref.shape[0]
    slots = table_ref.shape[0]
    square = (seqs, seqs)
    row, col = (lax.broadcasted_iota(jnp.int32, square, d) for d in (0, 1))
    own, earlier = row == col, col < row

    def total(where, values, dim):
        return jnp.sum(jnp.where(where, values, 0.0), axis=dim, keepdims=True)

    along = [jnp.broadcast_to(route_ref[k : k + 1, :].astype(f32), square) for k in range(top_count)]
    down = [total(own, a, 1) for a in along]
    slot_of_row = lax.broadcasted_iota(jnp.int32, (slots, seqs), 0).astype(f32)
    slot_of_lane = lax.broadcasted_iota(jnp.int32, (seqs, slots), 1).astype(f32)
    table = jnp.zeros((slots, seqs), f32)
    mixing = jnp.zeros((seqs, slots), f32)
    for k in range(top_count):
        slot = down[k] * CAPACITY
        for other in along:
            slot = slot + total(earlier & (other == down[k]), 1.0, 1)
        table = table + (slot_of_row == total(own, slot, 0)).astype(f32)
        gate = total(own, jnp.broadcast_to(gate_ref[k : k + 1, :], square), 1)
        mixing = mixing + jnp.where(slot_of_lane == slot, gate, 0.0)
    table_ref[...] = table.astype(bf16)
    high = mixing.astype(bf16)
    mixing_ref[0:seqs, :] = high
    mixing_ref[seqs:, :] = (mixing - high.astype(f32)).astype(bf16)
    copy.wait()


def proj_kernel(recv_ref, *refs):
    pieces, (out_ref, tok_ref) = refs[:8], refs[8:]
    nz, seqs, width = recv_ref.shape[0], out_ref.shape[1], recv_ref.shape[2] // 2
    half = seqs // 2
    for z in range(nz):
        tok_ref[z, 0:half, :] = recv_ref[z, 0:half, 0:width].astype(f32)
        tok_ref[z, half:, :] = recv_ref[z, 0:half, width:].astype(f32)
    tokens = tok_ref[...].reshape(nz * seqs, width).astype(bf16)
    for m in range(3):
        weight = jnp.concatenate([piece[m * 32 : (m + 1) * 32, :] for piece in pieces], axis=0)
        part = dot(tokens, weight).astype(bf16)
        out_ref[:, :, m * 512 : (m + 1) * 512] = part.reshape(nz, seqs, 512)


def paired(a):
    return jnp.concatenate([a, a], axis=-1)


def state_kernel(parts_ref, decay_ref, rate_ref, scale_ref, gain_ref, half_ref, state_ref, normed_ref, new_ref,
                 s_ref, p_ref, a_ref, v_ref, head_ref, in_sem):
    rows_total = state_ref.shape[0]
    chunk = 32
    chunks = rows_total // chunk
    blocks = state_ref.shape[1] // LANES
    heads = scale_ref.shape[1] // HEAD_DIM
    seqs = rows_total // heads

    here_chunks = half_ref.shape[0] // chunk

    def fetch(c):
        source, target = pl.ds(c * chunk, chunk), pl.ds((c - here_chunks) * chunk, chunk)
        return pltpu.make_async_copy(state_ref.at[source, :], s_ref.at[target, :], in_sem.at[c - here_chunks])

    for c in range(here_chunks, chunks):
        fetch(c).start()

    total = parts_ref[0].astype(f32)
    for n in range(1, parts_ref.shape[0]):
        total = total + parts_ref[n].astype(f32)
    total = total.astype(bf16).astype(f32)
    local = heads * HEAD_DIM

    def by_head(slot, wide):
        for h in range(heads):
            head_ref[slot, pl.ds(h, seqs, stride=heads), :] = paired(wide[:, h * HEAD_DIM : (h + 1) * HEAD_DIM])

    def per_head(slot, gain_ref):
        by_head(slot, jnp.broadcast_to(gain_ref[...], (seqs, local)))
        return head_ref[slot]

    by_head(0, total[:, 0:local])
    by_head(1, total[:, local : 2 * local])
    by_head(2, total[:, 2 * local : 3 * local])
    by_head(3, decay_ref[...])
    by_head(4, rate_ref[...])
    keys = head_ref[1]
    rates = head_ref[4]
    scaled = keys * per_head(5, scale_ref)
    squares = jnp.sum((scaled * scaled)[:, 0:HEAD_DIM], axis=-1, keepdims=True)
    unit = scaled * lax.rsqrt(squares + norm_eps)
    head_ref[1] = unit
    head_ref[4] = unit * rates
    head_ref[5] = keys * rates

    def iota(shape, dim):
        return lax.broadcasted_iota(jnp.int32, shape, dim)

    square = (LANES, LANES)
    half_in = iota(square, 0) // HEAD_DIM
    spread = (half_in == iota(square, 1) // HEAD_DIM).astype(f32).astype(bf16)
    gathered = (half_in == iota(square, 1) % 2).astype(f32).astype(bf16)
    widen = (iota(square, 0) % 2 == iota(square, 1) // HEAD_DIM).astype(f32).astype(bf16)
    pair_of_lane = iota((chunk, LANES), 1) // 2

    def keep(k, values):
        p_ref[k * chunk : (k + 1) * chunk, :] = values.astype(bf16)

    for c in range(chunks):
        rows = pl.ds(c * chunk, chunk)
        old_ref, old_rows = half_ref, rows
        if c >= here_chunks:
            fetch(c).wait()
            old_ref, old_rows = s_ref, pl.ds((c - here_chunks) * chunk, chunk)
        unit_c = head_ref[1, rows, :]
        val_c = head_ref[2, rows, :]
        for k in range(blocks):
            keep(k, old_ref[old_rows, k * LANES : (k + 1) * LANES] * unit_c)
            v_ref[k * chunk : (k + 1) * chunk, :] = jnp.where(pair_of_lane == k, val_c, 0.0).astype(bf16)
        a_ref[0] = dot(p_ref[...], spread)
        a_ref[1] = dot(v_ref[...], widen)
        rec_c = head_ref[0, rows, :]
        dec_c = head_ref[3, rows, :]
        corr_c = head_ref[4, rows, :]
        add_c = head_ref[5, rows, :]
        for k in range(blocks):
            lanes = slice(k * LANES, (k + 1) * LANES)
            here = slice(k * chunk, (k + 1) * chunk)
            new = old_ref[old_rows, lanes] * dec_c - a_ref[0, here, :] * corr_c + a_ref[1, here, :] * add_c
            new_ref[rows, lanes] = new
            keep(k, new * rec_c)
        a_ref[0] = dot(p_ref[...], gathered)
        read = jnp.zeros((chunk, LANES), f32)
        for k in range(blocks):
            read = jnp.where(pair_of_lane == k, a_ref[0, k * chunk : (k + 1) * chunk, :], read)
        head_ref[2, rows, :] = read

    read = head_ref[2][:, 0:HEAD_DIM]
    centred = read - jnp.mean(read, axis=-1, keepdims=True)
    normed = centred * lax.rsqrt(jnp.mean(centred * centred, axis=-1, keepdims=True) + group_eps)
    head_ref[2] = paired(normed) * per_head(5, gain_ref)
    for h in range(0, heads, 2):
        low = head_ref[2, pl.ds(h, seqs, stride=heads), :]
        high = head_ref[2, pl.ds(h + 1, seqs, stride=heads), :]
        both = jnp.concatenate([low[:, 0:HEAD_DIM], high[:, 0:HEAD_DIM]], axis=-1).astype(bf16)
        normed_ref[:, h * HEAD_DIM : (h + 2) * HEAD_DIM] = both


def out_kernel(tok_ref, *refs):
    pieces, (out_ref, part_ref) = refs[:10], refs[10:]
    tokens = tok_ref[...]
    groups, cols, seqs = 8, 32, tokens.shape[0]
    for n, piece in enumerate(pieces):
        shift, first_z = ((0, 0), (1, 0), (3, 0), (2, 0), (2, groups // 2))[n % 5]
        first = source_of(shift + n // 5 * 4) * cols
        turned = dot_t(piece[...], tokens)
        for z in range(piece.shape[0] // cols):
            at = pl.multiple_of(first + (z + first_z) * groups * cols, cols)
            part_ref[pl.ds(at, cols), :] = turned[z * cols : (z + 1) * cols, :]
    same = (lax.broadcasted_iota(jnp.int32, (seqs, seqs), 0) == lax.broadcasted_iota(jnp.int32, (seqs, seqs), 1))
    out_ref[...] = dot_t(same.astype(f32).astype(bf16), part_ref[...].astype(bf16)).astype(bf16)


def sum_in_order(piece_refs, line_ref):
    count = len(piece_refs)
    for shift, piece in enumerate(piece_refs):
        line_ref[(lax.axis_index("y") + count - shift) % count] = piece[...].astype(f32)
    total = line_ref[0]
    for n in range(1, count):
        total = total + line_ref[n]
    return total


def mid_kernel(p0, p1, p2, p3, x_ref, post_ref, ffn_ref, table_ref, middle_ref, rows_ref, line_ref):
    mix_sum = sum_in_order((p0, p1, p2, p3), line_ref)
    middle = (x_ref[...].astype(f32) + rms_scale(mix_sum, post_ref[...])).astype(bf16)
    middle_ref[...] = middle
    ffn_in = rms_scale(middle.astype(f32), ffn_ref[...]).astype(bf16)
    rows_ref[...] = dot(table_ref[...], ffn_in).reshape(rows_ref.shape).astype(bf16)


def move_kernel(*refs):
    count = len(refs) // 2
    sem_ref = refs[2 * count]
    copies = [pltpu.make_async_copy(refs[n], refs[count + n], sem_ref.at[n]) for n in range(count)]
    for copy in copies:
        copy.start()
    for copy in copies:
        copy.wait()


def bring_on_chip(arrays, name):
    return pl.pallas_call(
        move_kernel,
        out_shape=[pltpu.VMEM(a.shape, a.dtype) for a in arrays],
        in_specs=[HBM] * len(arrays),
        out_specs=[ON_CHIP] * len(arrays),
        scratch_shapes=[pltpu.SemaphoreType.DMA((len(arrays),))],
        name=name,
        compiler_params=SMALL,
    )(*[off_chip(a) for a in arrays])


def combine_kernel(back_ref, mixing_ref, out_ref):
    rows = back_ref[...].astype(f32).reshape(-1, back_ref.shape[2]).astype(bf16)
    both = dot(mixing_ref[...], rows)
    seqs = out_ref.shape[0]
    out_ref[...] = (both[0:seqs] + both[seqs:]).astype(bf16)


def expert_kernel(rows_ref, gate_ref, up_ref, down_ref, out_ref):
    rows = rows_ref[...].astype(f32).reshape(-1, rows_ref.shape[2]).astype(bf16)
    gate_cut = jnp.minimum(dot(rows, gate_ref[0]), clamp_limit)
    up_cut = jnp.clip(dot(rows, up_ref[0]), -clamp_limit, clamp_limit)
    hidden = ((up_cut + 1.0) * gate_cut * jax.nn.sigmoid(gate_alpha * gate_cut)).astype(bf16)
    out_ref[...] = dot(hidden, down_ref[0]).reshape(out_ref.shape).astype(bf16)


def last_kernel(p0, p1, p2, p3, middle_ref, gain_ref, out_ref, line_ref):
    moe_sum = sum_in_order((p0, p1, p2, p3), line_ref)
    out_ref[...] = (middle_ref[...].astype(f32) + rms_scale(moe_sum, gain_ref[...])).astype(bf16)


def local(
    layer_in,
    state_in,
    mix_gain,
    rec_weight,
    key_weight,
    val_weight,
    decay_down,
    decay_up,
    decay_base,
    rate_down,
    rate_up,
    rate_base,
    key_scale,
    group_gain,
    out_weight,
    post_gain,
    ffn_gain,
    routes,
    route_gates,
    expert_gate,
    expert_up,
    expert_down,
    out_gain,
):
    seqs, width = layer_in.shape
    heads = state_in.shape[1]
    local_cols = heads * HEAD_DIM
    nz, nx, nc, ny = (lax.axis_size(a) for a in ("z", "x", "c", "y"))
    nxc = nx * nc
    share = width // nz
    expert_total = nz * nxc
    slot_total = expert_total * CAPACITY
    shape = jax.ShapeDtypeStruct

    send, own, normed = pl.pallas_call(
        prep_kernel,
        out_shape=(
            pltpu.VMEM((nz, seqs // 2 + out_weight.shape[1], 2 * share), bf16),
            pltpu.VMEM((3 * rec_weight.shape[0], local_cols), bf16),
            pltpu.VMEM((seqs, width), bf16),
        ),
        name="prep",
    )(layer_in, mix_gain[None], out_weight.T, rec_weight, key_weight, val_weight)
    recv = lax.all_to_all(send, "z", split_axis=0, concat_axis=0, tiled=True)
    along_x = [own] + from_others(own, "x")
    pieces = along_x + [p for q in along_x for p in from_others(q, "c")]
    ow_own = recv[:, seqs // 2 :, :].reshape(nz * out_weight.shape[1], local_cols)
    half = ow_own.shape[0] // 2
    ow_last, ow_next, ow_low = shifted(ow_own, "x", -1), shifted(ow_own, "x", 1), shifted(ow_own[:half], "x", 2)
    rows, lanes_total = seqs * heads, state_in.shape[2]
    state_flat = off_chip(state_in.reshape(rows, lanes_total))
    decay_factor, learn_rate, dispatch_table, mixing, state_half = pl.pallas_call(
        rates_kernel,
        out_shape=(
            pltpu.VMEM((seqs, local_cols), f32),
            pltpu.VMEM((seqs, local_cols), f32),
            pltpu.VMEM((slot_total, seqs), bf16),
            pltpu.VMEM((2 * seqs, slot_total), bf16),
            pltpu.VMEM((rows // 2, lanes_total), f32),
        ),
        in_specs=[ON_CHIP] + [pl.BlockSpec()] * 8 + [HBM],
        scratch_shapes=[pltpu.SemaphoreType.DMA((1,))],
        name="rates",
        compiler_params=SMALL,
    )(
        on_chip(normed),
        off_chip(decay_down.T),
        off_chip(decay_up),
        off_chip(decay_base[None]),
        off_chip(rate_down.T),
        off_chip(rate_up),
        off_chip(rate_base[None]),
        off_chip(routes.T),
        off_chip(route_gates.T),
        state_flat,
    )

    ow_last, decay_factor = lax.optimization_barrier((ow_last, decay_factor))
    ow_high = shifted(ow_last[half:], "x", -1)

    part = pl.pallas_call(
        proj_kernel,
        out_shape=pltpu.VMEM((nz, seqs, 3 * local_cols), bf16),
        in_specs=[ON_CHIP] * 9,
        scratch_shapes=[
            pltpu.VMEM((nz, seqs, share), f32),
        ],
        name="proj",
        compiler_params=SMALL,
    )(on_chip(recv), *[on_chip(p) for p in pieces])
    parts = lax.all_to_all(part, "z", split_axis=0, concat_axis=0, tiled=True)

    normed_out, new_state = pl.pallas_call(
        state_kernel,
        out_shape=(pltpu.VMEM((seqs, local_cols), bf16), pltpu.VMEM((rows, lanes_total), f32)),
        in_specs=[ON_CHIP] * 6 + [HBM],
        out_specs=(ON_CHIP, ON_CHIP),
        scratch_shapes=[
            pltpu.VMEM((rows // 2, lanes_total), f32),
            pltpu.VMEM((32 * (lanes_total // LANES), LANES), bf16),
            pltpu.VMEM((2, 32 * (lanes_total // LANES), LANES), f32),
            pltpu.VMEM((32 * (lanes_total // LANES), LANES), bf16),
            pltpu.VMEM((6, rows, LANES), f32),
            pltpu.SemaphoreType.DMA((rows // 64,)),
        ],
        name="state",
        compiler_params=SMALL,
    )(
        on_chip(parts),
        on_chip(decay_factor),
        on_chip(learn_rate),
        off_chip(key_scale[None]),
        off_chip(group_gain[None]),
        on_chip(state_half),
        state_flat,
    )
    ow_early = [shifted(ow_own, "c", 1), shifted(ow_last, "c", 1)]
    normed_out, down, ow_next, ow_low, ow_high = lax.optimization_barrier(
        (normed_out, expert_down, ow_next, ow_low, ow_high)
    )
    (down,) = bring_on_chip([down], "fetch_down")
    ow_next_other, ow_low_other, ow_high_other = (shifted(p, "c", 1) for p in (ow_next, ow_low, ow_high))
    ow_pieces = [ow_own, ow_next, ow_last, ow_low, ow_high]
    ow_pieces = ow_pieces + [ow_early[0], ow_next_other, ow_early[1], ow_low_other, ow_high_other]
    normed_out, down = lax.optimization_barrier((normed_out, down))
    mix_part = pl.pallas_call(
        out_kernel,
        out_shape=pltpu.VMEM((seqs, width), bf16),
        in_specs=[ON_CHIP] * 11,
        scratch_shapes=[pltpu.VMEM((width, seqs), f32)],
        name="outproj",
        compiler_params=SMALL,
    )(on_chip(normed_out), *[on_chip(p) for p in ow_pieces])
    mix_part, *weights = lax.optimization_barrier((mix_part, expert_gate, expert_up))
    mix_parts = [mix_part] + from_others(mix_part, "y")
    weights = bring_on_chip(weights, "fetch")
    dispatch_table, *weights = lax.optimization_barrier((dispatch_table, *weights))

    middle, send_rows = pl.pallas_call(
        mid_kernel,
        out_shape=(pltpu.VMEM((seqs, width), bf16), pltpu.VMEM((expert_total, CAPACITY, width), bf16)),
        in_specs=[ON_CHIP] * 8,
        scratch_shapes=[pltpu.VMEM((ny, seqs, width), f32)],
        name="mid",
        compiler_params=SMALL,
    )(
        *[on_chip(p) for p in mix_parts],
        layer_in,
        post_gain[None],
        ffn_gain[None],
        on_chip(dispatch_table),
    )

    arrived = lax.all_to_all(send_rows, EP, split_axis=0, concat_axis=0, tiled=True)
    partial_value = pl.pallas_call(
        expert_kernel,
        out_shape=pltpu.VMEM((expert_total, CAPACITY, width), bf16),
        in_specs=[ON_CHIP] * 4,
        name="expert",
        compiler_params=SMALL,
    )(on_chip(arrived), *[on_chip(w) for w in weights], on_chip(down))
    back_rows = lax.all_to_all(partial_value, EP, split_axis=0, concat_axis=0, tiled=True)
    moe_part = pl.pallas_call(
        combine_kernel,
        out_shape=pltpu.VMEM((seqs, width), bf16),
        in_specs=[ON_CHIP] * 2,
        name="combine",
        compiler_params=SMALL,
    )(on_chip(back_rows), on_chip(mixing))
    moe_part, new_state = lax.optimization_barrier((moe_part, new_state))
    new_state = pl.pallas_call(
        move_kernel,
        out_shape=pltpu.HBM((rows, lanes_total), f32),
        in_specs=[ON_CHIP],
        out_specs=HBM,
        scratch_shapes=[pltpu.SemaphoreType.DMA((1,))],
        name="store",
        compiler_params=SMALL,
    )(on_chip(new_state))
    layer_out = pl.pallas_call(
        last_kernel,
        out_shape=shape((seqs, width), bf16),
        in_specs=[ON_CHIP] * 6,
        scratch_shapes=[pltpu.VMEM((ny, seqs, width), f32)],
        name="last",
        compiler_params=SMALL,
    )(
        *[on_chip(p) for p in [moe_part] + from_others(moe_part, "y")],
        on_chip(middle),
        out_gain[None],
    )
    return layer_out, new_state.reshape(seqs, heads, lanes_total)


def solution(mesh):
    mesh = Mesh(mesh.devices.reshape(8, 4, 2, 4), ("z", "x", "c", "y"))
    in_specs = (
        P(EP, None),
        P(EP, "y", None),
        P(),
        P(EP, "y"),
        P(EP, "y"),
        P(EP, "y"),
        P(),
        P(None, "y"),
        P("y"),
        P(),
        P(None, "y"),
        P("y"),
        P("y"),
        P("y"),
        P("y", EP),
        P(),
        P(),
        P(EP, None),
        P(EP, None),
        P(EP, None, "y"),
        P(EP, None, "y"),
        P(EP, "y", None),
        P(),
    )
    out_specs = (P(EP, None), P(EP, "y", None))
    return jax.shard_map(local, mesh=mesh, in_specs=in_specs, out_specs=out_specs, check_vma=False)
```

```python
import math

import jax
import jax.numpy as jnp
from jax import lax
from jax.experimental import pallas as pl
from jax.experimental.pallas import tpu as pltpu
from jax.sharding import Mesh
from jax.sharding import PartitionSpec as P

HEAD_DIM = 64
CAPACITY = 2
LANES = 128
norm_eps = 1e-06
group_eps = 0.00064
clamp_limit = 7.0
gate_alpha = 1.702
f32 = jnp.float32
bf16 = jnp.bfloat16


EP = ("z", "x", "c")
HBM = pl.BlockSpec(memory_space=pl.ANY)
SMALL = pltpu.CompilerParams(vmem_limit_bytes=12 * 2**20)
ON_CHIP = pl.BlockSpec(memory_space=pltpu.VMEM)


def dot(a, b):
    return jnp.dot(a, b, preferred_element_type=f32)


def dot_t(a, b):
    return lax.dot_general(a, b, (((1,), (1,)), ((), ())), preferred_element_type=f32)


def on_chip(a):
    return pltpu.with_memory_space_constraint(a, pltpu.VMEM)


def off_chip(a):
    return pltpu.with_memory_space_constraint(a, pltpu.HBM)


def shifted(own, axis, by):
    size = lax.axis_size(axis)
    return lax.ppermute(own, axis, [(i, (i + by) % size) for i in range(size)])


def from_others(own, axis):
    return [shifted(own, axis, s) for s in range(1, lax.axis_size(axis))]


def rms_scale(values, scales):
    return values * lax.rsqrt(jnp.mean(values * values, axis=-1, keepdims=True) + norm_eps) * scales


def source_of(n):
    x_from = (lax.axis_index("x") + 4 - n % 4) % 4
    return x_from * 2 + (lax.axis_index("c") + n // 4) % 2


def prep_kernel(x_ref, gain_ref, ow_ref, rec_ref, key_ref, val_ref, send_ref, own_ref, normed_ref):
    for m, weight in enumerate((rec_ref, key_ref, val_ref)):
        own_ref[m * 32 : (m + 1) * 32, :] = weight[...]
    normed = rms_scale(x_ref[...].astype(f32), gain_ref[...]).astype(bf16)
    normed_ref[...] = normed
    nz, wide = send_ref.shape[0], send_ref.shape[2]
    seqs = normed.shape[0]
    width, half = wide // 2, seqs // 2
    at = lax.broadcasted_iota(jnp.int32, (width, width), 1)
    piece = at // 32
    x_from = (lax.axis_index("x") + 4 - piece % 4) % 4
    feature = (x_from * 2 + (lax.axis_index("c") + piece // 4) % 2) * 32 + at % 32
    order = (lax.broadcasted_iota(jnp.int32, (width, width), 0) == feature).astype(f32).astype(bf16)
    slices = jnp.concatenate([normed[:, z * width : (z + 1) * width] for z in range(nz)], axis=0)
    slices = dot(slices, order)
    for z in range(nz):
        send_ref[z, 0:half, 0:width] = slices[z * seqs : z * seqs + half].astype(bf16)
        send_ref[z, 0:half, width:wide] = slices[z * seqs + half : (z + 1) * seqs].astype(bf16)
        send_ref[z, half:, :] = ow_ref[...]


def rates_kernel(normed_ref, dd_ref, du_ref, db_ref, rd_ref, ru_ref, rb_ref, route_ref, gate_ref, state_ref,
                 decay_ref, rate_ref, table_ref, mixing_ref, state_out, sem_ref):
    copy = pltpu.make_async_copy(state_ref.at[pl.ds(0, state_out.shape[0]), :], state_out, sem_ref.at[0])
    copy.start()
    normed = normed_ref[...]
    decay_hidden = jnp.tanh(dot_t(normed, dd_ref[...])).astype(bf16)
    rate_hidden = dot_t(normed, rd_ref[...]).astype(bf16)
    decay_pre = db_ref[...] + dot(decay_hidden, du_ref[...])
    decay_ref[...] = jnp.exp(-math.exp(-0.5) * jax.nn.sigmoid(decay_pre))
    rate_ref[...] = jax.nn.sigmoid(rb_ref[...] + dot(rate_hidden, ru_ref[...]))

    seqs = normed.shape[0]
    top_count = route_ref.shape[0]
    slots = table_ref.shape[0]
    square = (seqs, seqs)
    row, col = (lax.broadcasted_iota(jnp.int32, square, d) for d in (0, 1))
    own, earlier = row == col, col < row

    def total(where, values, dim):
        return jnp.sum(jnp.where(where, values, 0.0), axis=dim, keepdims=True)

    along = [jnp.broadcast_to(route_ref[k : k + 1, :].astype(f32), square) for k in range(top_count)]
    down = [total(own, a, 1) for a in along]
    slot_of_row = lax.broadcasted_iota(jnp.int32, (slots, seqs), 0).astype(f32)
    slot_of_lane = lax.broadcasted_iota(jnp.int32, (seqs, slots), 1).astype(f32)
    table = jnp.zeros((slots, seqs), f32)
    mixing = jnp.zeros((seqs, slots), f32)
    for k in range(top_count):
        slot = down[k] * CAPACITY
        for other in along:
            slot = slot + total(earlier & (other == down[k]), 1.0, 1)
        table = table + (slot_of_row == total(own, slot, 0)).astype(f32)
        gate = total(own, jnp.broadcast_to(gate_ref[k : k + 1, :], square), 1)
        mixing = mixing + jnp.where(slot_of_lane == slot, gate, 0.0)
    table_ref[...] = table.astype(bf16)
    high = mixing.astype(bf16)
    mixing_ref[0:seqs, :] = high
    mixing_ref[seqs:, :] = (mixing - high.astype(f32)).astype(bf16)
    copy.wait()


def proj_kernel(recv_ref, *refs):
    pieces, (out_ref, tok_ref) = refs[:8], refs[8:]
    nz, seqs, width = recv_ref.shape[0], out_ref.shape[1], recv_ref.shape[2] // 2
    half = seqs // 2
    for z in range(nz):
        tok_ref[z, 0:half, :] = recv_ref[z, 0:half, 0:width].astype(f32)
        tok_ref[z, half:, :] = recv_ref[z, 0:half, width:].astype(f32)
    tokens = tok_ref[...].reshape(nz * seqs, width).astype(bf16)
    for m in range(3):
        weight = jnp.concatenate([piece[m * 32 : (m + 1) * 32, :] for piece in pieces], axis=0)
        part = dot(tokens, weight).astype(bf16)
        out_ref[:, :, m * 512 : (m + 1) * 512] = part.reshape(nz, seqs, 512)


def paired(a):
    return jnp.concatenate([a, a], axis=-1)


def state_kernel(parts_ref, decay_ref, rate_ref, scale_ref, gain_ref, half_ref, state_ref, gate_ref, normed_ref, new_ref,
                 gate_out,
                 s_ref, p_ref, a_ref, v_ref, head_ref, in_sem, gate_sem):
    rows_total = state_ref.shape[0]
    chunk = 32
    chunks = rows_total // chunk
    blocks = state_ref.shape[1] // LANES
    heads = scale_ref.shape[1] // HEAD_DIM
    seqs = rows_total // heads

    here_chunks = half_ref.shape[0] // chunk

    def fetch(c):
        source, target = pl.ds(c * chunk, chunk), pl.ds((c - here_chunks) * chunk, chunk)
        return pltpu.make_async_copy(state_ref.at[source, :], s_ref.at[target, :], in_sem.at[c - here_chunks])

    for c in range(here_chunks, chunks):
        fetch(c).start()
    gate_copy = pltpu.make_async_copy(gate_ref, gate_out, gate_sem.at[0])
    gate_copy.start()

    total = parts_ref[0].astype(f32)
    for n in range(1, parts_ref.shape[0]):
        total = total + parts_ref[n].astype(f32)
    total = total.astype(bf16).astype(f32)
    local = heads * HEAD_DIM

    def by_head(slot, wide):
        for h in range(heads):
            head_ref[slot, pl.ds(h, seqs, stride=heads), :] = paired(wide[:, h * HEAD_DIM : (h + 1) * HEAD_DIM])

    def per_head(slot, gain_ref):
        by_head(slot, jnp.broadcast_to(gain_ref[...], (seqs, local)))
        return head_ref[slot]

    by_head(0, total[:, 0:local])
    by_head(1, total[:, local : 2 * local])
    by_head(2, total[:, 2 * local : 3 * local])
    by_head(3, decay_ref[...])
    by_head(4, rate_ref[...])
    keys = head_ref[1]
    rates = head_ref[4]
    scaled = keys * per_head(5, scale_ref)
    squares = jnp.sum((scaled * scaled)[:, 0:HEAD_DIM], axis=-1, keepdims=True)
    unit = scaled * lax.rsqrt(squares + norm_eps)
    head_ref[1] = unit
    head_ref[4] = unit * rates
    head_ref[5] = keys * rates

    def iota(shape, dim):
        return lax.broadcasted_iota(jnp.int32, shape, dim)

    square = (LANES, LANES)
    half_in = iota(square, 0) // HEAD_DIM
    spread = (half_in == iota(square, 1) // HEAD_DIM).astype(f32).astype(bf16)
    gathered = (half_in == iota(square, 1) % 2).astype(f32).astype(bf16)
    widen = (iota(square, 0) % 2 == iota(square, 1) // HEAD_DIM).astype(f32).astype(bf16)
    pair_of_lane = iota((chunk, LANES), 1) // 2

    def keep(k, values):
        p_ref[k * chunk : (k + 1) * chunk, :] = values.astype(bf16)

    for c in range(chunks):
        rows = pl.ds(c * chunk, chunk)
        old_ref, old_rows = half_ref, rows
        if c >= here_chunks:
            fetch(c).wait()
            old_ref, old_rows = s_ref, pl.ds((c - here_chunks) * chunk, chunk)
        unit_c = head_ref[1, rows, :]
        val_c = head_ref[2, rows, :]
        for k in range(blocks):
            keep(k, old_ref[old_rows, k * LANES : (k + 1) * LANES] * unit_c)
            v_ref[k * chunk : (k + 1) * chunk, :] = jnp.where(pair_of_lane == k, val_c, 0.0).astype(bf16)
        a_ref[0] = dot(p_ref[...], spread)
        a_ref[1] = dot(v_ref[...], widen)
        rec_c = head_ref[0, rows, :]
        dec_c = head_ref[3, rows, :]
        corr_c = head_ref[4, rows, :]
        add_c = head_ref[5, rows, :]
        for k in range(blocks):
            lanes = slice(k * LANES, (k + 1) * LANES)
            here = slice(k * chunk, (k + 1) * chunk)
            new = old_ref[old_rows, lanes] * dec_c - a_ref[0, here, :] * corr_c + a_ref[1, here, :] * add_c
            new_ref[rows, lanes] = new
            keep(k, new * rec_c)
        a_ref[0] = dot(p_ref[...], gathered)
        read = jnp.zeros((chunk, LANES), f32)
        for k in range(blocks):
            read = jnp.where(pair_of_lane == k, a_ref[0, k * chunk : (k + 1) * chunk, :], read)
        head_ref[2, rows, :] = read

    read = head_ref[2][:, 0:HEAD_DIM]
    centred = read - jnp.mean(read, axis=-1, keepdims=True)
    normed = centred * lax.rsqrt(jnp.mean(centred * centred, axis=-1, keepdims=True) + group_eps)
    head_ref[2] = paired(normed) * per_head(5, gain_ref)
    for h in range(0, heads, 2):
        low = head_ref[2, pl.ds(h, seqs, stride=heads), :]
        high = head_ref[2, pl.ds(h + 1, seqs, stride=heads), :]
        both = jnp.concatenate([low[:, 0:HEAD_DIM], high[:, 0:HEAD_DIM]], axis=-1).astype(bf16)
        normed_ref[:, h * HEAD_DIM : (h + 2) * HEAD_DIM] = both
    gate_copy.wait()


def out_kernel(tok_ref, *refs):
    pieces, (out_ref, part_ref) = refs[:10], refs[10:]
    tokens = tok_ref[...]
    groups, cols, seqs = 8, 32, tokens.shape[0]
    for n, piece in enumerate(pieces):
        shift, first_z = ((0, 0), (1, 0), (3, 0), (2, 0), (2, groups // 2))[n % 5]
        first = source_of(shift + n // 5 * 4) * cols
        turned = dot_t(piece[...], tokens)
        for z in range(piece.shape[0] // cols):
            at = pl.multiple_of(first + (z + first_z) * groups * cols, cols)
            part_ref[pl.ds(at, cols), :] = turned[z * cols : (z + 1) * cols, :]
    same = (lax.broadcasted_iota(jnp.int32, (seqs, seqs), 0) == lax.broadcasted_iota(jnp.int32, (seqs, seqs), 1))
    out_ref[...] = dot_t(same.astype(f32).astype(bf16), part_ref[...].astype(bf16)).astype(bf16)


def sum_in_order(piece_refs, line_ref):
    count = len(piece_refs)
    for shift, piece in enumerate(piece_refs):
        line_ref[(lax.axis_index("y") + count - shift) % count] = piece[...].astype(f32)
    total = line_ref[0]
    for n in range(1, count):
        total = total + line_ref[n]
    return total


def mid_kernel(p0, p1, p2, p3, x_ref, post_ref, ffn_ref, table_ref, middle_ref, rows_ref, line_ref):
    mix_sum = sum_in_order((p0, p1, p2, p3), line_ref)
    middle = (x_ref[...].astype(f32) + rms_scale(mix_sum, post_ref[...])).astype(bf16)
    middle_ref[...] = middle
    ffn_in = rms_scale(middle.astype(f32), ffn_ref[...]).astype(bf16)
    rows_ref[...] = dot(table_ref[...], ffn_in).reshape(rows_ref.shape).astype(bf16)


def move_kernel(*refs):
    count = len(refs) // 2
    sem_ref = refs[2 * count]
    copies = [pltpu.make_async_copy(refs[n], refs[count + n], sem_ref.at[n]) for n in range(count)]
    for copy in copies:
        copy.start()
    for copy in copies:
        copy.wait()


def bring_on_chip(arrays, name):
    return pl.pallas_call(
        move_kernel,
        out_shape=[pltpu.VMEM(a.shape, a.dtype) for a in arrays],
        in_specs=[HBM] * len(arrays),
        out_specs=[ON_CHIP] * len(arrays),
        scratch_shapes=[pltpu.SemaphoreType.DMA((len(arrays),))],
        name=name,
        compiler_params=SMALL,
    )(*[off_chip(a) for a in arrays])


def combine_kernel(back_ref, mixing_ref, out_ref):
    rows = back_ref[...].astype(f32).reshape(-1, back_ref.shape[2]).astype(bf16)
    both = dot(mixing_ref[...], rows)
    seqs = out_ref.shape[0]
    out_ref[...] = (both[0:seqs] + both[seqs:]).astype(bf16)


def expert_kernel(rows_ref, gate_ref, up_ref, down_ref, out_ref):
    rows = rows_ref[...].astype(f32).reshape(-1, rows_ref.shape[2]).astype(bf16)
    gate_cut = jnp.minimum(dot(rows, gate_ref[0]), clamp_limit)
    up_cut = jnp.clip(dot(rows, up_ref[0]), -clamp_limit, clamp_limit)
    hidden = ((up_cut + 1.0) * gate_cut * jax.nn.sigmoid(gate_alpha * gate_cut)).astype(bf16)
    out_ref[...] = dot(hidden, down_ref[0]).reshape(out_ref.shape).astype(bf16)


def last_kernel(p0, p1, p2, p3, middle_ref, gain_ref, out_ref, line_ref):
    moe_sum = sum_in_order((p0, p1, p2, p3), line_ref)
    out_ref[...] = (middle_ref[...].astype(f32) + rms_scale(moe_sum, gain_ref[...])).astype(bf16)


def local(
    layer_in,
    state_in,
    mix_gain,
    rec_weight,
    key_weight,
    val_weight,
    decay_down,
    decay_up,
    decay_base,
    rate_down,
    rate_up,
    rate_base,
    key_scale,
    group_gain,
    out_weight,
    post_gain,
    ffn_gain,
    routes,
    route_gates,
    expert_gate,
    expert_up,
    expert_down,
    out_gain,
):
    seqs, width = layer_in.shape
    heads = state_in.shape[1]
    local_cols = heads * HEAD_DIM
    nz, nx, nc, ny = (lax.axis_size(a) for a in ("z", "x", "c", "y"))
    nxc = nx * nc
    share = width // nz
    expert_total = nz * nxc
    slot_total = expert_total * CAPACITY
    shape = jax.ShapeDtypeStruct

    send, own, normed = pl.pallas_call(
        prep_kernel,
        out_shape=(
            pltpu.VMEM((nz, seqs // 2 + out_weight.shape[1], 2 * share), bf16),
            pltpu.VMEM((3 * rec_weight.shape[0], local_cols), bf16),
            pltpu.VMEM((seqs, width), bf16),
        ),
        name="prep",
    )(layer_in, mix_gain[None], out_weight.T, rec_weight, key_weight, val_weight)
    recv = lax.all_to_all(send, "z", split_axis=0, concat_axis=0, tiled=True)
    along_x = [own] + from_others(own, "x")
    pieces = along_x + [p for q in along_x for p in from_others(q, "c")]
    ow_own = recv[:, seqs // 2 :, :].reshape(nz * out_weight.shape[1], local_cols)
    half = ow_own.shape[0] // 2
    ow_last, ow_next, ow_low = shifted(ow_own, "x", -1), shifted(ow_own, "x", 1), shifted(ow_own[:half], "x", 2)
    rows, lanes_total = seqs * heads, state_in.shape[2]
    state_flat = off_chip(state_in.reshape(rows, lanes_total))
    decay_factor, learn_rate, dispatch_table, mixing, state_half = pl.pallas_call(
        rates_kernel,
        out_shape=(
            pltpu.VMEM((seqs, local_cols), f32),
            pltpu.VMEM((seqs, local_cols), f32),
            pltpu.VMEM((slot_total, seqs), bf16),
            pltpu.VMEM((2 * seqs, slot_total), bf16),
            pltpu.VMEM((rows // 2, lanes_total), f32),
        ),
        in_specs=[ON_CHIP] + [pl.BlockSpec()] * 8 + [HBM],
        scratch_shapes=[pltpu.SemaphoreType.DMA((1,))],
        name="rates",
        compiler_params=SMALL,
    )(
        on_chip(normed),
        off_chip(decay_down.T),
        off_chip(decay_up),
        off_chip(decay_base[None]),
        off_chip(rate_down.T),
        off_chip(rate_up),
        off_chip(rate_base[None]),
        off_chip(routes.T),
        off_chip(route_gates.T),
        state_flat,
    )

    ow_last, decay_factor = lax.optimization_barrier((ow_last, decay_factor))
    ow_high = shifted(ow_last[half:], "x", -1)

    part = pl.pallas_call(
        proj_kernel,
        out_shape=pltpu.VMEM((nz, seqs, 3 * local_cols), bf16),
        in_specs=[ON_CHIP] * 9,
        scratch_shapes=[
            pltpu.VMEM((nz, seqs, share), f32),
        ],
        name="proj",
        compiler_params=SMALL,
    )(on_chip(recv), *[on_chip(p) for p in pieces])
    parts = lax.all_to_all(part, "z", split_axis=0, concat_axis=0, tiled=True)

    normed_out, new_state, gate = pl.pallas_call(
        state_kernel,
        out_shape=(
            pltpu.VMEM((seqs, local_cols), bf16),
            pltpu.VMEM((rows, lanes_total), f32),
            pltpu.VMEM(expert_gate.shape, bf16),
        ),
        in_specs=[ON_CHIP] * 6 + [HBM] * 2,
        out_specs=(ON_CHIP,) * 3,
        scratch_shapes=[
            pltpu.VMEM((rows // 2, lanes_total), f32),
            pltpu.VMEM((32 * (lanes_total // LANES), LANES), bf16),
            pltpu.VMEM((2, 32 * (lanes_total // LANES), LANES), f32),
            pltpu.VMEM((32 * (lanes_total // LANES), LANES), bf16),
            pltpu.VMEM((6, rows, LANES), f32),
            pltpu.SemaphoreType.DMA((rows // 64,)),
            pltpu.SemaphoreType.DMA((1,)),
        ],
        name="state",
        compiler_params=SMALL,
    )(
        on_chip(parts),
        on_chip(decay_factor),
        on_chip(learn_rate),
        off_chip(key_scale[None]),
        off_chip(group_gain[None]),
        on_chip(state_half),
        state_flat,
        off_chip(expert_gate),
    )
    ow_early = [shifted(ow_own, "c", 1), shifted(ow_last, "c", 1)]
    normed_out, down, ow_next, ow_low, ow_high = lax.optimization_barrier(
        (normed_out, expert_down, ow_next, ow_low, ow_high)
    )
    (down,) = bring_on_chip([down], "fetch_down")
    ow_next_other, ow_low_other, ow_high_other = (shifted(p, "c", 1) for p in (ow_next, ow_low, ow_high))
    ow_pieces = [ow_own, ow_next, ow_last, ow_low, ow_high]
    ow_pieces = ow_pieces + [ow_early[0], ow_next_other, ow_early[1], ow_low_other, ow_high_other]
    normed_out, down = lax.optimization_barrier((normed_out, down))
    mix_part = pl.pallas_call(
        out_kernel,
        out_shape=pltpu.VMEM((seqs, width), bf16),
        in_specs=[ON_CHIP] * 11,
        scratch_shapes=[pltpu.VMEM((width, seqs), f32)],
        name="outproj",
        compiler_params=SMALL,
    )(on_chip(normed_out), *[on_chip(p) for p in ow_pieces])
    mix_part, up = lax.optimization_barrier((mix_part, expert_up))
    mix_parts = [mix_part] + from_others(mix_part, "y")
    (up,) = bring_on_chip([up], "fetch")
    dispatch_table, up = lax.optimization_barrier((dispatch_table, up))

    middle, send_rows = pl.pallas_call(
        mid_kernel,
        out_shape=(pltpu.VMEM((seqs, width), bf16), pltpu.VMEM((expert_total, CAPACITY, width), bf16)),
        in_specs=[ON_CHIP] * 8,
        scratch_shapes=[pltpu.VMEM((ny, seqs, width), f32)],
        name="mid",
        compiler_params=SMALL,
    )(
        *[on_chip(p) for p in mix_parts],
        layer_in,
        post_gain[None],
        ffn_gain[None],
        on_chip(dispatch_table),
    )

    arrived = lax.all_to_all(send_rows, EP, split_axis=0, concat_axis=0, tiled=True)
    partial_value = pl.pallas_call(
        expert_kernel,
        out_shape=pltpu.VMEM((expert_total, CAPACITY, width), bf16),
        in_specs=[ON_CHIP] * 4,
        name="expert",
        compiler_params=SMALL,
    )(on_chip(arrived), on_chip(gate), on_chip(up), on_chip(down))
    back_rows = lax.all_to_all(partial_value, EP, split_axis=0, concat_axis=0, tiled=True)
    moe_part = pl.pallas_call(
        combine_kernel,
        out_shape=pltpu.VMEM((seqs, width), bf16),
        in_specs=[ON_CHIP] * 2,
        name="combine",
        compiler_params=SMALL,
    )(on_chip(back_rows), on_chip(mixing))
    moe_part, new_state = lax.optimization_barrier((moe_part, new_state))
    new_state = pl.pallas_call(
        move_kernel,
        out_shape=pltpu.HBM((rows, lanes_total), f32),
        in_specs=[ON_CHIP],
        out_specs=HBM,
        scratch_shapes=[pltpu.SemaphoreType.DMA((1,))],
        name="store",
        compiler_params=SMALL,
    )(on_chip(new_state))
    layer_out = pl.pallas_call(
        last_kernel,
        out_shape=shape((seqs, width), bf16),
        in_specs=[ON_CHIP] * 6,
        scratch_shapes=[pltpu.VMEM((ny, seqs, width), f32)],
        name="last",
        compiler_params=SMALL,
    )(
        *[on_chip(p) for p in [moe_part] + from_others(moe_part, "y")],
        on_chip(middle),
        out_gain[None],
    )
    return layer_out, new_state.reshape(seqs, heads, lanes_total)


def solution(mesh):
    mesh = Mesh(mesh.devices.reshape(8, 4, 2, 4), ("z", "x", "c", "y"))
    in_specs = (
        P(EP, None),
        P(EP, "y", None),
        P(),
        P(EP, "y"),
        P(EP, "y"),
        P(EP, "y"),
        P(),
        P(None, "y"),
        P("y"),
        P(),
        P(None, "y"),
        P("y"),
        P("y"),
        P("y"),
        P("y", EP),
        P(),
        P(),
        P(EP, None),
        P(EP, None),
        P(EP, None, "y"),
        P(EP, None, "y"),
        P(EP, "y", None),
        P(),
    )
    out_specs = (P(EP, None), P(EP, "y", None))
    return jax.shard_map(local, mesh=mesh, in_specs=in_specs, out_specs=out_specs, check_vma=False)
```

```python
import math

import jax
import jax.numpy as jnp
from jax import lax
from jax.experimental import pallas as pl
from jax.experimental.pallas import tpu as pltpu
from jax.sharding import Mesh
from jax.sharding import PartitionSpec as P

HEAD_DIM = 64
CAPACITY = 2
LANES = 128
norm_eps = 1e-06
group_eps = 0.00064
clamp_limit = 7.0
gate_alpha = 1.702
f32 = jnp.float32
bf16 = jnp.bfloat16


EP = ("z", "x", "c")
HBM = pl.BlockSpec(memory_space=pl.ANY)
SMALL = pltpu.CompilerParams(vmem_limit_bytes=12 * 2**20)
ON_CHIP = pl.BlockSpec(memory_space=pltpu.VMEM)


def dot(a, b):
    return jnp.dot(a, b, preferred_element_type=f32)


def dot_t(a, b):
    return lax.dot_general(a, b, (((1,), (1,)), ((), ())), preferred_element_type=f32)


def on_chip(a):
    return pltpu.with_memory_space_constraint(a, pltpu.VMEM)


def off_chip(a):
    return pltpu.with_memory_space_constraint(a, pltpu.HBM)


def shifted(own, axis, by):
    size = lax.axis_size(axis)
    return lax.ppermute(own, axis, [(i, (i + by) % size) for i in range(size)])


def from_others(own, axis):
    return [shifted(own, axis, s) for s in range(1, lax.axis_size(axis))]


def rms_scale(values, scales):
    return values * lax.rsqrt(jnp.mean(values * values, axis=-1, keepdims=True) + norm_eps) * scales


def source_of(n):
    x_from = (lax.axis_index("x") + 4 - n % 4) % 4
    return x_from * 2 + (lax.axis_index("c") + n // 4) % 2


def prep_kernel(x_ref, gain_ref, ow_ref, rec_ref, key_ref, val_ref, send_ref, own_ref, normed_ref):
    for m, weight in enumerate((rec_ref, key_ref, val_ref)):
        own_ref[m * 32 : (m + 1) * 32, :] = weight[...]
    normed = rms_scale(x_ref[...].astype(f32), gain_ref[...]).astype(bf16)
    normed_ref[...] = normed
    nz, wide = send_ref.shape[0], send_ref.shape[2]
    seqs = normed.shape[0]
    width, half = wide // 2, seqs // 2
    at = lax.broadcasted_iota(jnp.int32, (width, width), 1)
    piece = at // 32
    x_from = (lax.axis_index("x") + 4 - piece % 4) % 4
    feature = (x_from * 2 + (lax.axis_index("c") + piece // 4) % 2) * 32 + at % 32
    order = (lax.broadcasted_iota(jnp.int32, (width, width), 0) == feature).astype(f32).astype(bf16)
    slices = jnp.concatenate([normed[:, z * width : (z + 1) * width] for z in range(nz)], axis=0)
    slices = dot(slices, order)
    for z in range(nz):
        send_ref[z, 0:half, 0:width] = slices[z * seqs : z * seqs + half].astype(bf16)
        send_ref[z, 0:half, width:wide] = slices[z * seqs + half : (z + 1) * seqs].astype(bf16)
        send_ref[z, half:, :] = ow_ref[...]


def rates_kernel(normed_ref, dd_ref, du_ref, db_ref, rd_ref, ru_ref, rb_ref, route_ref, gate_ref, state_ref,
                 decay_ref, rate_ref, table_ref, mixing_ref, state_out, sem_ref):
    copy = pltpu.make_async_copy(state_ref.at[pl.ds(0, state_out.shape[0]), :], state_out, sem_ref.at[0])
    copy.start()
    normed = normed_ref[...]
    decay_hidden = jnp.tanh(dot_t(normed, dd_ref[...])).astype(bf16)
    rate_hidden = dot_t(normed, rd_ref[...]).astype(bf16)
    decay_pre = db_ref[...] + dot(decay_hidden, du_ref[...])
    decay_ref[...] = jnp.exp(-math.exp(-0.5) * jax.nn.sigmoid(decay_pre))
    rate_ref[...] = jax.nn.sigmoid(rb_ref[...] + dot(rate_hidden, ru_ref[...]))

    seqs = normed.shape[0]
    top_count = route_ref.shape[0]
    slots = table_ref.shape[0]
    square = (seqs, seqs)
    row, col = (lax.broadcasted_iota(jnp.int32, square, d) for d in (0, 1))
    own, earlier = row == col, col < row

    def total(where, values, dim):
        return jnp.sum(jnp.where(where, values, 0.0), axis=dim, keepdims=True)

    along = [jnp.broadcast_to(route_ref[k : k + 1, :].astype(f32), square) for k in range(top_count)]
    down = [total(own, a, 1) for a in along]
    slot_of_row = lax.broadcasted_iota(jnp.int32, (slots, seqs), 0).astype(f32)
    slot_of_lane = lax.broadcasted_iota(jnp.int32, (seqs, slots), 1).astype(f32)
    table = jnp.zeros((slots, seqs), f32)
    mixing = jnp.zeros((seqs, slots), f32)
    for k in range(top_count):
        slot = down[k] * CAPACITY
        for other in along:
            slot = slot + total(earlier & (other == down[k]), 1.0, 1)
        table = table + (slot_of_row == total(own, slot, 0)).astype(f32)
        gate = total(own, jnp.broadcast_to(gate_ref[k : k + 1, :], square), 1)
        mixing = mixing + jnp.where(slot_of_lane == slot, gate, 0.0)
    table_ref[...] = table.astype(bf16)
    high = mixing.astype(bf16)
    mixing_ref[0:seqs, :] = high
    mixing_ref[seqs:, :] = (mixing - high.astype(f32)).astype(bf16)
    copy.wait()


def proj_kernel(recv_ref, *refs):
    pieces, (out_ref, tok_ref) = refs[:8], refs[8:]
    nz, seqs, width = recv_ref.shape[0], out_ref.shape[1], recv_ref.shape[2] // 2
    half = seqs // 2
    for z in range(nz):
        tok_ref[z, 0:half, :] = recv_ref[z, 0:half, 0:width].astype(f32)
        tok_ref[z, half:, :] = recv_ref[z, 0:half, width:].astype(f32)
    tokens = tok_ref[...].reshape(nz * seqs, width).astype(bf16)
    for m in range(3):
        weight = jnp.concatenate([piece[m * 32 : (m + 1) * 32, :] for piece in pieces], axis=0)
        part = dot(tokens, weight).astype(bf16)
        out_ref[:, :, m * 512 : (m + 1) * 512] = part.reshape(nz, seqs, 512)


def paired(a):
    return jnp.concatenate([a, a], axis=-1)


def state_kernel(parts_ref, decay_ref, rate_ref, scale_ref, gain_ref, half_ref, state_ref, normed_ref, new_ref,
                 s_ref, p_ref, a_ref, v_ref, head_ref, in_sem):
    rows_total = state_ref.shape[0]
    chunk = 32
    chunks = rows_total // chunk
    blocks = state_ref.shape[1] // LANES
    heads = scale_ref.shape[1] // HEAD_DIM
    seqs = rows_total // heads

    here_chunks = half_ref.shape[0] // chunk

    def fetch(c):
        source, target = pl.ds(c * chunk, chunk), pl.ds((c - here_chunks) * chunk, chunk)
        return pltpu.make_async_copy(state_ref.at[source, :], s_ref.at[target, :], in_sem.at[c - here_chunks])

    for c in range(here_chunks, chunks):
        fetch(c).start()

    total = parts_ref[0].astype(f32)
    for n in range(1, parts_ref.shape[0]):
        total = total + parts_ref[n].astype(f32)
    total = total.astype(bf16).astype(f32)
    local = heads * HEAD_DIM

    def by_head(slot, wide):
        for h in range(heads):
            head_ref[slot, pl.ds(h, seqs, stride=heads), :] = paired(wide[:, h * HEAD_DIM : (h + 1) * HEAD_DIM])

    def per_head(slot, gain_ref):
        by_head(slot, jnp.broadcast_to(gain_ref[...], (seqs, local)))
        return head_ref[slot]

    by_head(0, total[:, 0:local])
    by_head(1, total[:, local : 2 * local])
    by_head(2, total[:, 2 * local : 3 * local])
    by_head(3, decay_ref[...])
    by_head(4, rate_ref[...])
    keys = head_ref[1]
    rates = head_ref[4]
    scaled = keys * per_head(5, scale_ref)
    squares = jnp.sum((scaled * scaled)[:, 0:HEAD_DIM], axis=-1, keepdims=True)
    unit = scaled * lax.rsqrt(squares + norm_eps)
    head_ref[1] = unit
    head_ref[4] = unit * rates
    head_ref[5] = keys * rates

    def iota(shape, dim):
        return lax.broadcasted_iota(jnp.int32, shape, dim)

    square = (LANES, LANES)
    half_in = iota(square, 0) // HEAD_DIM
    spread = (half_in == iota(square, 1) // HEAD_DIM).astype(f32).astype(bf16)
    gathered = (half_in == iota(square, 1) % 2).astype(f32).astype(bf16)
    widen = (iota(square, 0) % 2 == iota(square, 1) // HEAD_DIM).astype(f32).astype(bf16)
    pair_of_lane = iota((chunk, LANES), 1) // 2

    def keep(k, values):
        p_ref[k * chunk : (k + 1) * chunk, :] = values.astype(bf16)

    for c in range(chunks):
        rows = pl.ds(c * chunk, chunk)
        old_ref, old_rows = half_ref, rows
        if c >= here_chunks:
            fetch(c).wait()
            old_ref, old_rows = s_ref, pl.ds((c - here_chunks) * chunk, chunk)
        unit_c = head_ref[1, rows, :]
        val_c = head_ref[2, rows, :]
        for k in range(blocks):
            keep(k, old_ref[old_rows, k * LANES : (k + 1) * LANES] * unit_c)
            v_ref[k * chunk : (k + 1) * chunk, :] = jnp.where(pair_of_lane == k, val_c, 0.0).astype(bf16)
        a_ref[0] = dot(p_ref[...], spread)
        a_ref[1] = dot(v_ref[...], widen)
        rec_c = head_ref[0, rows, :]
        dec_c = head_ref[3, rows, :]
        corr_c = head_ref[4, rows, :]
        add_c = head_ref[5, rows, :]
        for k in range(blocks):
            lanes = slice(k * LANES, (k + 1) * LANES)
            here = slice(k * chunk, (k + 1) * chunk)
            new = old_ref[old_rows, lanes] * dec_c - a_ref[0, here, :] * corr_c + a_ref[1, here, :] * add_c
            new_ref[rows, lanes] = new
            keep(k, new * rec_c)
        a_ref[0] = dot(p_ref[...], gathered)
        read = jnp.zeros((chunk, LANES), f32)
        for k in range(blocks):
            read = jnp.where(pair_of_lane == k, a_ref[0, k * chunk : (k + 1) * chunk, :], read)
        head_ref[2, rows, :] = read

    read = head_ref[2][:, 0:HEAD_DIM]
    centred = read - jnp.mean(read, axis=-1, keepdims=True)
    normed = centred * lax.rsqrt(jnp.mean(centred * centred, axis=-1, keepdims=True) + group_eps)
    head_ref[2] = paired(normed) * per_head(5, gain_ref)
    for h in range(0, heads, 2):
        low = head_ref[2, pl.ds(h, seqs, stride=heads), :]
        high = head_ref[2, pl.ds(h + 1, seqs, stride=heads), :]
        both = jnp.concatenate([low[:, 0:HEAD_DIM], high[:, 0:HEAD_DIM]], axis=-1).astype(bf16)
        normed_ref[:, h * HEAD_DIM : (h + 2) * HEAD_DIM] = both


def out_kernel(tok_ref, *refs):
    pieces, (out_ref, part_ref) = refs[:10], refs[10:]
    tokens = tok_ref[...]
    groups, cols, seqs = 8, 32, tokens.shape[0]
    for n, piece in enumerate(pieces):
        shift, first_z = ((0, 0), (1, 0), (3, 0), (2, 0), (2, groups // 2))[n % 5]
        first = source_of(shift + n // 5 * 4) * cols
        turned = dot_t(piece[...], tokens)
        for z in range(piece.shape[0] // cols):
            at = pl.multiple_of(first + (z + first_z) * groups * cols, cols)
            part_ref[pl.ds(at, cols), :] = turned[z * cols : (z + 1) * cols, :]
    same = (lax.broadcasted_iota(jnp.int32, (seqs, seqs), 0) == lax.broadcasted_iota(jnp.int32, (seqs, seqs), 1))
    out_ref[...] = dot_t(same.astype(f32).astype(bf16), part_ref[...].astype(bf16)).astype(bf16)


def sum_in_order(piece_refs, line_ref):
    count = len(piece_refs)
    for shift, piece in enumerate(piece_refs):
        line_ref[(lax.axis_index("y") + count - shift) % count] = piece[...].astype(f32)
    total = line_ref[0]
    for n in range(1, count):
        total = total + line_ref[n]
    return total


def mid_kernel(p0, p1, p2, p3, x_ref, post_ref, ffn_ref, table_ref, middle_ref, rows_ref, line_ref):
    mix_sum = sum_in_order((p0, p1, p2, p3), line_ref)
    middle = (x_ref[...].astype(f32) + rms_scale(mix_sum, post_ref[...])).astype(bf16)
    middle_ref[...] = middle
    ffn_in = rms_scale(middle.astype(f32), ffn_ref[...]).astype(bf16)
    rows_ref[...] = dot(table_ref[...], ffn_in).reshape(rows_ref.shape).astype(bf16)


def move_kernel(*refs):
    count = len(refs) // 2
    sem_ref = refs[2 * count]
    copies = [pltpu.make_async_copy(refs[n], refs[count + n], sem_ref.at[n]) for n in range(count)]
    for copy in copies:
        copy.start()
    for copy in copies:
        copy.wait()


def bring_on_chip(arrays, name):
    return pl.pallas_call(
        move_kernel,
        out_shape=[pltpu.VMEM(a.shape, a.dtype) for a in arrays],
        in_specs=[HBM] * len(arrays),
        out_specs=[ON_CHIP] * len(arrays),
        scratch_shapes=[pltpu.SemaphoreType.DMA((len(arrays),))],
        name=name,
        compiler_params=SMALL,
    )(*[off_chip(a) for a in arrays])


def combine_kernel(back_ref, mixing_ref, out_ref):
    rows = back_ref[...].astype(f32).reshape(-1, back_ref.shape[2]).astype(bf16)
    both = dot(mixing_ref[...], rows)
    seqs = out_ref.shape[0]
    out_ref[...] = (both[0:seqs] + both[seqs:]).astype(bf16)


def expert_kernel(rows_ref, gate_ref, up_ref, down_ref, out_ref):
    rows = rows_ref[...].astype(f32).reshape(-1, rows_ref.shape[2]).astype(bf16)
    gate_cut = jnp.minimum(dot(rows, gate_ref[0]), clamp_limit)
    up_cut = jnp.clip(dot(rows, up_ref[0]), -clamp_limit, clamp_limit)
    hidden = ((up_cut + 1.0) * gate_cut * jax.nn.sigmoid(gate_alpha * gate_cut)).astype(bf16)
    out_ref[...] = dot(hidden, down_ref[0]).reshape(out_ref.shape).astype(bf16)


def last_kernel(p0, p1, p2, p3, middle_ref, gain_ref, out_ref, line_ref):
    moe_sum = sum_in_order((p0, p1, p2, p3), line_ref)
    out_ref[...] = (middle_ref[...].astype(f32) + rms_scale(moe_sum, gain_ref[...])).astype(bf16)


def local(
    layer_in,
    state_in,
    mix_gain,
    rec_weight,
    key_weight,
    val_weight,
    decay_down,
    decay_up,
    decay_base,
    rate_down,
    rate_up,
    rate_base,
    key_scale,
    group_gain,
    out_weight,
    post_gain,
    ffn_gain,
    routes,
    route_gates,
    expert_gate,
    expert_up,
    expert_down,
    out_gain,
):
    seqs, width = layer_in.shape
    heads = state_in.shape[1]
    local_cols = heads * HEAD_DIM
    nz, nx, nc, ny = (lax.axis_size(a) for a in ("z", "x", "c", "y"))
    nxc = nx * nc
    share = width // nz
    expert_total = nz * nxc
    slot_total = expert_total * CAPACITY
    shape = jax.ShapeDtypeStruct

    send, own, normed = pl.pallas_call(
        prep_kernel,
        out_shape=(
            pltpu.VMEM((nz, seqs // 2 + out_weight.shape[1], 2 * share), bf16),
            pltpu.VMEM((3 * rec_weight.shape[0], local_cols), bf16),
            pltpu.VMEM((seqs, width), bf16),
        ),
        name="prep",
    )(layer_in, mix_gain[None], out_weight.T, rec_weight, key_weight, val_weight)
    recv = lax.all_to_all(send, "z", split_axis=0, concat_axis=0, tiled=True)
    along_x = [own] + from_others(own, "x")
    pieces = along_x + [p for q in along_x for p in from_others(q, "c")]
    rows, lanes_total = seqs * heads, state_in.shape[2]
    state_flat = off_chip(state_in.reshape(rows, lanes_total))
    decay_factor, learn_rate, dispatch_table, mixing, state_half = pl.pallas_call(
        rates_kernel,
        out_shape=(
            pltpu.VMEM((seqs, local_cols), f32),
            pltpu.VMEM((seqs, local_cols), f32),
            pltpu.VMEM((slot_total, seqs), bf16),
            pltpu.VMEM((2 * seqs, slot_total), bf16),
            pltpu.VMEM((rows // 2, lanes_total), f32),
        ),
        in_specs=[ON_CHIP] + [pl.BlockSpec()] * 8 + [HBM],
        scratch_shapes=[pltpu.SemaphoreType.DMA((1,))],
        name="rates",
        compiler_params=SMALL,
    )(
        on_chip(normed),
        off_chip(decay_down.T),
        off_chip(decay_up),
        off_chip(decay_base[None]),
        off_chip(rate_down.T),
        off_chip(rate_up),
        off_chip(rate_base[None]),
        off_chip(routes.T),
        off_chip(route_gates.T),
        state_flat,
    )
    recv, decay_factor = lax.optimization_barrier((recv, decay_factor))

    ow_own = recv[:, seqs // 2 :, :].reshape(nz * out_weight.shape[1], local_cols)
    half = ow_own.shape[0] // 2
    ow_last, ow_next, ow_low = shifted(ow_own, "x", -1), shifted(ow_own, "x", 1), shifted(ow_own[:half], "x", 2)
    ow_high = shifted(ow_last[half:], "x", -1)

    part = pl.pallas_call(
        proj_kernel,
        out_shape=pltpu.VMEM((nz, seqs, 3 * local_cols), bf16),
        in_specs=[ON_CHIP] * 9,
        scratch_shapes=[
            pltpu.VMEM((nz, seqs, share), f32),
        ],
        name="proj",
        compiler_params=SMALL,
    )(on_chip(recv), *[on_chip(p) for p in pieces])
    parts = lax.all_to_all(part, "z", split_axis=0, concat_axis=0, tiled=True)

    normed_out, new_state = pl.pallas_call(
        state_kernel,
        out_shape=(pltpu.VMEM((seqs, local_cols), bf16), pltpu.VMEM((rows, lanes_total), f32)),
        in_specs=[ON_CHIP] * 6 + [HBM],
        out_specs=(ON_CHIP, ON_CHIP),
        scratch_shapes=[
            pltpu.VMEM((rows // 2, lanes_total), f32),
            pltpu.VMEM((32 * (lanes_total // LANES), LANES), bf16),
            pltpu.VMEM((2, 32 * (lanes_total // LANES), LANES), f32),
            pltpu.VMEM((32 * (lanes_total // LANES), LANES), bf16),
            pltpu.VMEM((6, rows, LANES), f32),
            pltpu.SemaphoreType.DMA((rows // 64,)),
        ],
        name="state",
        compiler_params=SMALL,
    )(
        on_chip(parts),
        on_chip(decay_factor),
        on_chip(learn_rate),
        off_chip(key_scale[None]),
        off_chip(group_gain[None]),
        on_chip(state_half),
        state_flat,
    )
    ow_early = [shifted(ow_own, "c", 1), shifted(ow_last, "c", 1)]
    normed_out, down, ow_next, ow_low, ow_high = lax.optimization_barrier(
        (normed_out, expert_down, ow_next, ow_low, ow_high)
    )
    (down,) = bring_on_chip([down], "fetch_down")
    ow_next_other, ow_low_other, ow_high_other = (shifted(p, "c", 1) for p in (ow_next, ow_low, ow_high))
    ow_pieces = [ow_own, ow_next, ow_last, ow_low, ow_high]
    ow_pieces = ow_pieces + [ow_early[0], ow_next_other, ow_early[1], ow_low_other, ow_high_other]
    normed_out, down = lax.optimization_barrier((normed_out, down))
    mix_part = pl.pallas_call(
        out_kernel,
        out_shape=pltpu.VMEM((seqs, width), bf16),
        in_specs=[ON_CHIP] * 11,
        scratch_shapes=[pltpu.VMEM((width, seqs), f32)],
        name="outproj",
        compiler_params=SMALL,
    )(on_chip(normed_out), *[on_chip(p) for p in ow_pieces])
    mix_part, *weights = lax.optimization_barrier((mix_part, expert_gate, expert_up))
    mix_parts = [mix_part] + from_others(mix_part, "y")
    weights = bring_on_chip(weights, "fetch")
    dispatch_table, *weights = lax.optimization_barrier((dispatch_table, *weights))

    middle, send_rows = pl.pallas_call(
        mid_kernel,
        out_shape=(pltpu.VMEM((seqs, width), bf16), pltpu.VMEM((expert_total, CAPACITY, width), bf16)),
        in_specs=[ON_CHIP] * 8,
        scratch_shapes=[pltpu.VMEM((ny, seqs, width), f32)],
        name="mid",
        compiler_params=SMALL,
    )(
        *[on_chip(p) for p in mix_parts],
        layer_in,
        post_gain[None],
        ffn_gain[None],
        on_chip(dispatch_table),
    )

    arrived = lax.all_to_all(send_rows, EP, split_axis=0, concat_axis=0, tiled=True)
    partial_value = pl.pallas_call(
        expert_kernel,
        out_shape=pltpu.VMEM((expert_total, CAPACITY, width), bf16),
        in_specs=[ON_CHIP] * 4,
        name="expert",
        compiler_params=SMALL,
    )(on_chip(arrived), *[on_chip(w) for w in weights], on_chip(down))
    back_rows = lax.all_to_all(partial_value, EP, split_axis=0, concat_axis=0, tiled=True)
    moe_part = pl.pallas_call(
        combine_kernel,
        out_shape=pltpu.VMEM((seqs, width), bf16),
        in_specs=[ON_CHIP] * 2,
        name="combine",
        compiler_params=SMALL,
    )(on_chip(back_rows), on_chip(mixing))
    moe_part, new_state = lax.optimization_barrier((moe_part, new_state))
    new_state = pl.pallas_call(
        move_kernel,
        out_shape=pltpu.HBM((rows, lanes_total), f32),
        in_specs=[ON_CHIP],
        out_specs=HBM,
        scratch_shapes=[pltpu.SemaphoreType.DMA((1,))],
        name="store",
        compiler_params=SMALL,
    )(on_chip(new_state))
    layer_out = pl.pallas_call(
        last_kernel,
        out_shape=shape((seqs, width), bf16),
        in_specs=[ON_CHIP] * 6,
        scratch_shapes=[pltpu.VMEM((ny, seqs, width), f32)],
        name="last",
        compiler_params=SMALL,
    )(
        *[on_chip(p) for p in [moe_part] + from_others(moe_part, "y")],
        on_chip(middle),
        out_gain[None],
    )
    return layer_out, new_state.reshape(seqs, heads, lanes_total)


def solution(mesh):
    mesh = Mesh(mesh.devices.reshape(8, 4, 2, 4), ("z", "x", "c", "y"))
    in_specs = (
        P(EP, None),
        P(EP, "y", None),
        P(),
        P(EP, "y"),
        P(EP, "y"),
        P(EP, "y"),
        P(),
        P(None, "y"),
        P("y"),
        P(),
        P(None, "y"),
        P("y"),
        P("y"),
        P("y"),
        P("y", EP),
        P(),
        P(),
        P(EP, None),
        P(EP, None),
        P(EP, None, "y"),
        P(EP, None, "y"),
        P(EP, "y", None),
        P(),
    )
    out_specs = (P(EP, None), P(EP, "y", None))
    return jax.shard_map(local, mesh=mesh, in_specs=in_specs, out_specs=out_specs, check_vma=False)
```
